128 devices in a mesh: fs: 16 (over z, y), tp: 8 (over x, core).
Axes of the slice: x: 4, y: 4, z: 4, core: 2. Of those that a mesh axis runs over, the one named last changes fastest.
Arguments:
- resid: bfloat16 [24576, 2048], P(('fs', 'tp')), may hold values from -6 to 6
- norm1_gain: float32 [2048], replicated, may hold values from 0.1 to 1.9
- w_value: float32 [2048, 2048], P('fs', 'tp'), may hold values from -0.125 to 0.125
- w_gate: float32 [2048, 2048], P('fs', 'tp'), may hold values from -0.125 to 0.125
- value_scale: float32 [2048], replicated, may hold values from 0.3 to 3
- gate_scale: float32 [2048], replicated, may hold values from 0.5 to 3
- conv_taps: float32 [31, 2048], replicated, may hold values from -1 to 1
- conv_gain: float32 [2048], replicated, may hold values from 0.1 to 1.9
- w_point: float32 [2048, 2048], P('tp', 'fs'), may hold values from -0.125 to 0.125
- point_scale: float32 [2048], P('fs'), may hold values from 0.5 to 3
- norm2_gain: float32 [2048], replicated, may hold values from 0.1 to 1.9
- w_up: float32 [2048, 8192], P('fs', 'tp'), may hold values from -0.125 to 0.125
- up_scale: float32 [8192], P('tp'), may hold values from 0.5 to 1.5
- w_down: float32 [8192, 2048], P('tp', 'fs'), may hold values from -0.0625 to 0.0625
- down_scale: float32 [2048], P('fs'), may hold values from 0.3 to 1
Outputs:
- layer_out: bfloat16 [24576, 2048], P(('fs', 'tp'))
The draws below stay inside these ranges and needn't reach their ends.
All inputs are finite; a program needn't handle non-finite values.
Results may differ from the reference program's by a relative error of at most 0.015.
Values may be sent and summed in bfloat16 or wider, within the bound.
A program may use at most 128 MiB of HBM per device.

```python
import math
import jax
import jax.numpy as jnp
from jax import lax

D = 2048
CH = 2048
FF = 8192
KERNEL = 31
GROUPS = 4
LEN = 1536
TOKENS = 24576
N_TP = 8


def levels(stream_key, extent, shards, low, top_value):
    level = 1.0
    for position, shards_of in shards:
        heights = jax.random.uniform(jax.random.fold_in(jax.random.fold_in(stream_key, 6), position), (shards_of,), jnp.float32, low / len(shards), top_value / len(shards))
        level = level * jnp.repeat(jnp.exp(heights), extent[position] // shards_of).reshape((-1,) + (1,) * (len(extent) - 1 - position))
    return level


def noise(own_key, extent, scale, most, pieces=(), kind=jnp.bfloat16):
    entries = scale * jax.random.normal(own_key, extent, jnp.float32)
    if pieces:
        entries = entries * levels(own_key, extent, pieces, -0.22, 0.18)
    return jnp.clip(entries, -most, most).astype(kind)


def setup_inputs(seed: int = 0) -> dict:
    key_list = jax.random.split(jax.random.key(seed), 16)
    return {
        "resid": noise(key_list[0], (TOKENS, D), 1.0, 6.0, ((0, 128),)),
        "norm1_gain": jnp.clip(1.0 + 0.18 * jax.random.normal(key_list[1], (D,), jnp.float32), 0.1, 1.9),
        "w_value": noise(key_list[2], (D, CH), D ** -0.5, 0.125, ((0, 16), (1, 8)), jnp.float32),
        "w_gate": noise(key_list[3], (D, CH), D ** -0.5, 0.125, ((0, 16), (1, 8)), jnp.float32),
        "value_scale": jnp.clip(jnp.exp(jax.random.uniform(key_list[4], (CH,), jnp.float32, math.log(0.3), math.log(3.0))), 0.3, 3.0),
        "gate_scale": jnp.clip(jnp.exp(jax.random.uniform(key_list[5], (CH,), jnp.float32, math.log(0.5), math.log(3.0))), 0.5, 3.0),
        "conv_taps": noise(key_list[6], (KERNEL, CH), KERNEL ** -0.5, 1.0, (), jnp.float32),
        "conv_gain": jnp.clip(1.0 + 0.18 * jax.random.normal(key_list[7], (CH,), jnp.float32), 0.1, 1.9),
        "w_point": noise(key_list[8], (CH, D), CH ** -0.5, 0.125, ((0, 8), (1, 16)), jnp.float32),
        "point_scale": jnp.clip(jnp.exp(math.log(3.0) - 1.7917595 * jax.random.uniform(key_list[9], (D,), jnp.float32) ** levels(key_list[9], (D,), ((0, 16),), -0.2, 0.2)), 0.5, 3.0),
        "norm2_gain": jnp.clip(1.0 + 0.18 * jax.random.normal(key_list[10], (D,), jnp.float32), 0.1, 1.9),
        "w_up": noise(key_list[11], (D, FF), D ** -0.5, 0.125, ((0, 16), (1, 8)), jnp.float32),
        "up_scale": jnp.clip(jnp.exp(math.log(1.5) - 1.0986123 * jax.random.uniform(key_list[12], (FF,), jnp.float32) ** levels(key_list[12], (FF,), ((0, 8),), -0.2, 0.2)), 0.5, 1.5),
        "w_down": noise(key_list[13], (FF, D), FF ** -0.5, 0.0625, ((0, 8), (1, 16)), jnp.float32),
        "down_scale": jnp.clip(jnp.exp(math.log(1.0) - 1.2039728 * jax.random.uniform(key_list[14], (D,), jnp.float32) ** levels(key_list[14], (D,), ((0, 16),), -0.2, 0.2)), 0.3, 1.0),
    }


def rms_scaled(values, gain):
    data = values.astype(jnp.float32)
    return data * lax.rsqrt(lax.optimization_barrier(jnp.mean(data * data, axis=-1, keepdims=True)) + 1e-06) * gain

def reference(resid, norm1_gain, w_value, w_gate, value_scale, gate_scale, conv_taps, conv_gain, w_point, point_scale, norm2_gain, w_up, up_scale, w_down, down_scale):
    value_bf = w_value.astype(jnp.bfloat16)
    gate_bf = w_gate.astype(jnp.bfloat16)
    point_bf = w_point.astype(jnp.bfloat16)
    up_bf = w_up.astype(jnp.bfloat16)
    down_bf = w_down.astype(jnp.bfloat16)
    normed = rms_scaled(resid, norm1_gain).astype(jnp.bfloat16)
    value = jnp.dot(normed, value_bf, preferred_element_type=jnp.float32) * value_scale
    gate = jnp.dot(normed, gate_bf, preferred_element_type=jnp.float32) * gate_scale
    glu = (value * jax.nn.sigmoid(gate)).astype(jnp.bfloat16)
    reach = KERNEL // 2
    seqs = glu.reshape(-1, LEN, CH).astype(jnp.float32)
    padded = jnp.pad(seqs, ((0, 0), (reach, reach), (0, 0)))
    conv = jnp.zeros(seqs.shape, jnp.float32)
    for offset in range(KERNEL):
        conv = conv + conv_taps[offset] * padded[:, offset:offset + LEN]
    grouped = conv.reshape(-1, CH // GROUPS, GROUPS)
    gmean = lax.optimization_barrier(jnp.mean(grouped, axis=-2, keepdims=True))
    gsquare = lax.optimization_barrier(jnp.mean(grouped * grouped, axis=-2, keepdims=True))
    scaled = ((grouped - gmean) * lax.rsqrt(gsquare - gmean * gmean + 1e-05)).reshape(-1, CH) * conv_gain
    act = jax.nn.silu(scaled).astype(jnp.bfloat16)
    mixed = jnp.dot(act, point_bf, preferred_element_type=jnp.float32) * point_scale
    middle = (resid.astype(jnp.float32) + mixed).astype(jnp.bfloat16)
    normed2 = rms_scaled(middle, norm2_gain).astype(jnp.bfloat16)
    upper = jnp.dot(normed2, up_bf, preferred_element_type=jnp.float32) * up_scale
    hidden = jnp.square(jax.nn.relu(upper)).astype(jnp.bfloat16)
    block = FF // N_TP
    hid_blocks = jnp.transpose(hidden.reshape(hidden.shape[0], N_TP, block), (1, 0, 2))
    down_blocks = down_bf.reshape(N_TP, block, D)

    def add_block(total, pair):
        hid_block, down_block = pair
        partial_value = (jnp.dot(hid_block, down_block, preferred_element_type=jnp.float32) * down_scale).astype(jnp.bfloat16)
        partial_value = lax.optimization_barrier(partial_value)
        return (total + partial_value.astype(jnp.float32), None)
    total, _ = lax.scan(add_block, jnp.zeros((hidden.shape[0], D), jnp.float32), (hid_blocks, down_blocks))
    return (middle.astype(jnp.float32) + total).astype(jnp.bfloat16)
```

```python
import functools

import jax
import jax.numpy as jnp
from jax import lax
from jax.experimental import pallas as pl
from jax.experimental.pallas import tpu as pltpu
from jax.sharding import PartitionSpec as P

BF = jnp.bfloat16
F32 = jnp.float32
MESH = pl.DeviceIdType.MESH

RB = 192
HB = 96
CB = 384
SEQ = 1536
D = 2048
CW = 256
HALO = 16
KERNEL = 31
GROUP_WIDTH = 512.0
N_SEM = 120


def dot(a, b):
    return jnp.dot(a, b, preferred_element_type=F32)


class Copies:
    def __init__(self, send, recv):
        self.send, self.recv, self.used, self.started = send, recv, 0, []

    def take(self, count=1):
        at = self.used
        self.used += count
        assert self.used <= N_SEM
        return at

    def copy(self, src, dst, device, at=None):
        at = self.take() if at is None else at
        return pltpu.make_async_remote_copy(
            src_ref=src,
            dst_ref=dst,
            send_sem=self.send.at[at],
            recv_sem=self.recv.at[at],
            device_id=device,
            device_id_type=MESH,
        )

    def start(self, src, dst, device):
        made = self.copy(src, dst, device)
        made.start()
        self.started.append(made)
        return made

    def finish(self):
        for made in self.started:
            made.wait_send()


def kernel(
    resid,
    gain1,
    w_value,
    w_gate,
    value_scale,
    gate_scale,
    taps,
    conv_gain,
    w_point,
    point_scale,
    gain2,
    w_up,
    up_scale,
    w_down,
    down_scale,
    out,
    x1,
    x2,
    vg,
    pp,
    uu,
    dd,
    glu,
    cin,
    cv,
    st,
    st_in,
    act,
    mix_out,
    mix_in,
    mix,
    mid,
    hid,
    par_out,
    par_in,
    par,
    rel_in,
    fin_in,
    send_sem,
    recv_sem,
):
    fs = lax.axis_index("fs")
    tp = lax.axis_index("tp")
    z, y = fs // 4, fs % 4
    x, c = tp // 2, tp % 2
    xp, xm, xf = (x + 1) % 4, (x + 3) % 4, (x + 2) % 4
    yp, ym = (y + 1) % 4, (y + 3) % 4
    zp, zm = (z + 1) % 4, (z + 3) % 4
    to_xp, to_xm, to_xf = ({"tp": v * 2 + c} for v in (xp, xm, xf))
    to_pair = {"tp": x * 2 + 1 - c}
    to_yp, to_ym = ({"fs": z * 4 + v} for v in (yp, ym))
    to_zp, to_zm = ({"fs": v * 4 + y} for v in (zp, zm))
    cp = Copies(send_sem, recv_sem)

    barrier = pltpu.get_barrier_semaphore()
    for peer in (to_pair, to_xp, to_xm, to_xf, to_yp, to_ym, to_zp, to_zm):
        pl.semaphore_signal(barrier, inc=1, device_id=peer, device_id_type=MESH)

    vg[0, z, y] = w_value[...].astype(BF)
    vg[1, z, y] = w_gate[...].astype(BF)
    own_point = pp.at[x // 2, z, y, pl.ds(pl.multiple_of((x % 2) * 256, 256), 256)]
    own_point[...] = (w_point[...] * point_scale[...]).astype(BF)
    for half in range(2):
        uu[half, z, y] = w_up[:, half * 512 : half * 512 + 512].astype(BF)
        dd[half, z, y] = (w_down[half * 512 : half * 512 + 512, :] * down_scale[...]).astype(BF)

    def norm_rows(source, gain, target, base):
        def step(i, carry):
            rows = pl.multiple_of(i * 16, 16)
            v = source[pl.ds(rows, 16), :].astype(F32)
            scale = lax.rsqrt(jnp.mean(v * v, axis=-1, keepdims=True) + 1e-06)
            at = pl.multiple_of(base + i * 16, 16)
            target[pl.ds(at, 16), :] = (v * scale * gain[...]).astype(BF)
            return carry

        lax.fori_loop(0, RB // 16, step, 0)

    norm_rows(resid, gain1, x1, tp * RB)
    pl.semaphore_wait(barrier, 8)

    class Ring:
        def __init__(self, buf):
            self.buf = buf

        def at(self, v, core, first, count):
            return self.buf.at[pl.ds(pl.multiple_of(v * CB + core * RB + first, 16), count)]

        def own(self):
            lo, hi = self.at(x, c, 0, HB), self.at(x, c, HB, HB)
            whole = self.at(x, c, 0, RB)
            self.p0 = cp.start(lo, lo, to_xp)
            self.m1 = cp.start(hi, hi, to_xm)
            self.p1 = cp.start(hi, hi, to_xp)
            self.m0 = cp.start(lo, lo, to_xm)
            self.d0 = cp.start(whole, whole, to_pair)

        def relay(self):
            self.p0.wait_recv()
            lo = self.at(xm, c, 0, HB)
            self.rp = cp.start(lo, lo, to_xp)
            self.d1 = cp.start(lo, lo, to_pair)
            self.m1.wait_recv()
            hi = self.at(xp, c, HB, HB)
            self.rm = cp.start(hi, hi, to_xm)
            self.d2 = cp.start(hi, hi, to_pair)

        def near(self):
            self.p1.wait_recv()
            hi = self.at(xm, c, HB, HB)
            self.d3 = cp.start(hi, hi, to_pair)
            self.m0.wait_recv()
            lo = self.at(xp, c, 0, HB)
            self.d4 = cp.start(lo, lo, to_pair)

        def near_wait(self):
            for made in (self.d1, self.d2, self.d3, self.d4):
                made.wait_recv()

        def far(self):
            self.rp.wait_recv()
            lo = self.at(xf, c, 0, HB)
            self.d5 = cp.start(lo, lo, to_pair)
            self.rm.wait_recv()
            hi = self.at(xf, c, HB, HB)
            self.d6 = cp.start(hi, hi, to_pair)

        def far_wait(self):
            self.d5.wait_recv()
            self.d6.wait_recv()

    class Weights:
        def __init__(self, buf):
            self.buf, self.deep = buf, buf.shape[3]

        def s0(self):
            a, b = self.buf.at[0, z, y], self.buf.at[1, z, y]
            self.first = [
                cp.start(a, a, to_yp),
                cp.start(b, b, to_zp),
                cp.start(a, a, to_ym),
                cp.start(b, b, to_zm),
            ]

        def s1(self):
            half = self.deep // 2
            lo, hi = pl.ds(0, half), pl.ds(half, half)
            plan = (
                (self.buf.at[0, z, ym, lo], to_yp),
                (self.buf.at[1, zm, y, lo], to_zp),
                (self.buf.at[0, z, yp, hi], to_ym),
                (self.buf.at[1, zp, y, hi], to_zm),
            )
            self.second = []
            for made, (ref, peer) in zip(self.first, plan):
                made.wait_recv()
                self.second.append(cp.start(ref, ref, peer))

        def s2(self):
            for made in self.second:
                made.wait_recv()
            a, b = self.buf.at[0, z], self.buf.at[1, :, y]
            self.third = [
                cp.start(a, a, to_zp),
                cp.start(b, b, to_yp),
                cp.start(a, a, to_zm),
                cp.start(b, b, to_ym),
            ]

        def s3(self):
            lo, hi = pl.ds(0, 2), pl.ds(2, 2)
            plan = (
                (self.buf.at[0, zm, lo], to_zp),
                (self.buf.at[1, lo, ym], to_yp),
                (self.buf.at[0, zp, hi], to_zm),
                (self.buf.at[1, hi, yp], to_ym),
            )
            self.fourth = []
            for made, (ref, peer) in zip(self.third, plan):
                made.wait_recv()
                self.fourth.append(cp.start(ref, ref, peer))

        def s4(self):
            for made in self.fourth:
                made.wait_recv()

    ring1, ring2 = Ring(x1), Ring(x2)
    gv, gp, gu, gd = Weights(vg), Weights(pp), Weights(uu), Weights(dd)

    gv.s0()
    point_x = [cp.start(own_point, own_point, peer) for peer in (to_xp, to_xm, to_xf)]
    ring1.own()
    gv.s1()
    gv.s2()
    for made in point_x:
        made.wait_recv()
    gp.s0()

    glu[0:HALO, :] = jnp.zeros((HALO, CW), BF)
    glu[HALO + SEQ : HALO + SEQ + HALO, :] = jnp.zeros((HALO, CW), BF)
    st[...] = jnp.zeros(st.shape, F32)

    ring1.relay()
    gp.s1()
    gv.s3()
    gp.s2()
    gu.s0()

    own_cols = pl.ds(pl.multiple_of(tp * CW, CW), CW)

    def gated(v):
        rows = pl.multiple_of(v * CB, CB)
        block = x1[pl.ds(rows, CB), :]
        value = dot(block, vg[0].reshape(D, CW)) * value_scale[:, own_cols]
        gate = dot(block, vg[1].reshape(D, CW)) * gate_scale[:, own_cols]
        glu[pl.ds(pl.multiple_of(rows + HALO, 16), CB), :] = (value * jax.nn.sigmoid(gate)).astype(BF)

    ring1.d0.wait_recv()
    gv.s4()
    gated(x)
    ring1.near()
    ring1.near_wait()
    gated(xp)
    gated(xm)
    ring1.far()
    ring1.far_wait()
    gated(xf)

    def glu_for(v):
        return glu.at[pl.ds(pl.multiple_of(v * CB, CB), CB + 2 * HALO)]

    sent_glu = [cp.start(glu_for(v), cin.at[x], peer) for v, peer in ((xf, to_xf), (xp, to_xp), (xm, to_xm))]
    cin[x] = glu_for(x)[...]

    def convolve(v):
        def step(i, carry):
            part, chunk = i % 2, i // 2
            lane = pl.multiple_of(part * 128, 128)
            row = pl.multiple_of(chunk * 64, 64)
            col = pl.multiple_of((2 * v + c) * CW + part * 128, 128)
            data = cin[v, pl.ds(row, 96), pl.ds(lane, 128)].astype(F32)
            total = jnp.zeros((64, 128), F32)
            for b in range(8):
                turned = data if b == 0 else pltpu.roll(data, 96 - b, 0)
                for a in range(4):
                    k = 8 * a + b
                    if k:
                        tap = taps[k - 1 : k, pl.ds(col, 128)]
                        total = total + tap * turned[8 * a : 8 * a + 64]
            cv[v, pl.ds(row, 64), pl.ds(lane, 128)] = total
            st[0, pl.ds(row, 64), :] += total
            st[1, pl.ds(row, 64), :] += total * total
            return carry

        lax.fori_loop(0, 12, step, 0)

    convolve(x)
    gp.s3()
    gu.s1()
    sent_glu[1].wait_recv()
    convolve(xm)
    sent_glu[2].wait_recv()
    convolve(xp)
    sent_glu[0].wait_recv()
    convolve(xf)

    for kind in range(2):
        total = st[kind]
        for shift in (4, 8, 16, 32, 64):
            total = total + pltpu.roll(total, shift, 1)
        st[kind] = total
    sent_stats = cp.start(st, st_in, to_pair)
    gp.s4()
    gu.s2()
    gd.s0()
    sent_stats.wait_recv()

    def activate(i, carry):
        rows = pl.ds(pl.multiple_of(i * 32, 32), 32)
        gmean = (st[0, rows, :] + st_in[0, rows, :]) / GROUP_WIDTH
        gsquare = (st[1, rows, :] + st_in[1, rows, :]) / GROUP_WIDTH
        inv = lax.rsqrt(gsquare - gmean * gmean + 1e-05)
        for v in range(4):
            for part in range(2):
                col = pl.multiple_of((2 * v + c) * CW + part * 128, 128)
                lane = part * 128
                s = (cv[v, rows, lane : lane + 128] - gmean) * inv * conv_gain[:, pl.ds(col, 128)]
                act[rows, v * CW + lane : v * CW + lane + 128] = (s / (1.0 + jnp.exp(-s))).astype(BF)
        return carry

    lax.fori_loop(0, CB // 32, activate, 0)

    pair_rows = pl.ds(pl.multiple_of((1 - c) * RB, RB), RB)
    own_rows = pl.ds(pl.multiple_of(c * RB, RB), RB)
    mix_at = cp.take(8)

    def mix_copy(n):
        return cp.copy(mix_out.at[n], mix_in.at[n], to_pair, mix_at + n)

    def columns(buf, half, n):
        two = buf[half, n // 2, pl.ds((n % 2) * 2, 2)]
        return jnp.concatenate([two[0], two[1]], axis=1)

    def point(n, carry):
        left = jnp.concatenate([act[pair_rows, 0:512], act[own_rows, 0:512]], axis=0)
        right = jnp.concatenate([act[pair_rows, 512:1024], act[own_rows, 512:1024]], axis=0)
        both = dot(left, columns(pp, 0, n)) + dot(right, columns(pp, 1, n))
        mix_out[n] = both[:RB].astype(BF)
        mix_copy(n).start()
        mix[:, pl.ds(pl.multiple_of(n * 256, 256), 256)] = both[RB:]
        return carry

    lax.fori_loop(0, 8, point, 0)

    def add_mixed(n, carry):
        mix_copy(n).wait_recv()
        cols = pl.ds(pl.multiple_of(n * 256, 256), 256)
        mixed = mix[:, cols] + mix_in[n].astype(F32)
        mid[:, cols] = (resid[:, cols].astype(F32) + mixed).astype(BF)
        return carry

    lax.fori_loop(0, 8, add_mixed, 0)
    norm_rows(mid, gain2, x2, tp * RB)
    ring2.own()
    gu.s3()
    gd.s1()

    def up(v):
        rows = pl.ds(pl.multiple_of(v * CB, CB), CB)

        def step(n, carry):
            weight = uu[n // 2, :, :, :, pl.ds(pl.multiple_of((n % 2) * 256, 256), 256)].reshape(D, 256)
            cols = pl.ds(pl.multiple_of(n * 256, 256), 256)
            upper = jnp.maximum(dot(x2[rows, :], weight) * up_scale[:, cols], 0.0)
            hid[rows, cols] = (upper * upper).astype(BF)
            return carry

        lax.fori_loop(0, 4, step, 0)

    ring2.relay()
    gu.s4()
    gd.s2()
    ring2.d0.wait_recv()
    up(x)
    ring2.near()
    ring2.near_wait()
    up(xp)
    up(xm)
    ring2.far()
    gd.s3()
    ring2.far_wait()
    up(xf)
    gd.s4()

    def down(v):
        pair_at = pl.ds(pl.multiple_of(v * CB + (1 - c) * RB, RB), RB)
        own_at = pl.ds(pl.multiple_of(v * CB + c * RB, RB), RB)

        def step(n, carry):
            left = jnp.concatenate([hid[pair_at, 0:512], hid[own_at, 0:512]], axis=0)
            right = jnp.concatenate([hid[pair_at, 512:1024], hid[own_at, 512:1024]], axis=0)
            both = dot(left, columns(dd, 0, n)) + dot(right, columns(dd, 1, n))
            cols = pl.ds(pl.multiple_of(n * 256, 256), 256)
            par_out[v, :, cols] = both[:RB].astype(BF)
            par[v, :, cols] = both[RB:].astype(BF)
            return carry

        lax.fori_loop(0, 8, step, 0)
        return cp.start(par_out.at[v], par_in.at[v], to_pair)

    def add_pair(v, made, first=0, count=RB):
        made.wait_recv()

        def step(i, carry):
            rows = pl.ds(pl.multiple_of(i * 32, 32), 32)
            par[v, rows, :] = (par[v, rows, :].astype(F32) + par_in[v, rows, :].astype(F32)).astype(BF)
            return carry

        lax.fori_loop(0, RB // 32, step, 0)

    lo, hi = pl.ds(0, HB), pl.ds(HB, HB)
    made_f = down(xf)
    made_p = down(xp)
    add_pair(xf, made_f)
    relay_p = cp.start(par.at[xf, lo], rel_in.at[0], to_xp)
    relay_m = cp.start(par.at[xf, hi], rel_in.at[1], to_xm)
    made_m = down(xm)
    add_pair(xp, made_p)
    plain_p = cp.start(par.at[xp, hi], fin_in.at[0, hi], to_xp)
    add_pair(xm, made_m)
    plain_m = cp.start(par.at[xm, lo], fin_in.at[1, lo], to_xm)
    made_x = down(x)

    def add_relay(v, slot, first):
        def step(i, carry):
            rows = pl.ds(pl.multiple_of(first + i * 32, 32), 32)
            here = pl.ds(pl.multiple_of(i * 32, 32), 32)
            par[v, rows, :] = (par[v, rows, :].astype(F32) + rel_in[slot, here, :].astype(F32)).astype(BF)
            return carry

        lax.fori_loop(0, HB // 32, step, 0)

    relay_p.wait_recv()
    add_relay(xp, 0, 0)
    last_p = cp.start(par.at[xp, lo], fin_in.at[0, lo], to_xp)
    relay_m.wait_recv()
    add_relay(xm, 1, HB)
    last_m = cp.start(par.at[xm, hi], fin_in.at[1, hi], to_xm)

    made_x.wait_recv()

    def add_own(i, carry):
        rows = pl.ds(pl.multiple_of(i * 16, 16), 16)
        mix[rows, :] = mid[rows, :].astype(F32) + (par[x, rows, :].astype(F32) + par_in[x, rows, :].astype(F32))
        return carry

    lax.fori_loop(0, RB // 16, add_own, 0)
    for made in (plain_p, plain_m, last_p, last_m):
        made.wait_recv()

    def finish(i, carry):
        rows = pl.ds(pl.multiple_of(i * 16, 16), 16)
        total = fin_in[0, rows, :].astype(F32) + fin_in[1, rows, :].astype(F32)
        out[rows, :] = (mix[rows, :] + total).astype(BF)
        return carry

    lax.fori_loop(0, RB // 16, finish, 0)
    cp.finish()

    def mix_sent(n, carry):
        mix_copy(n).wait_send()
        return carry

    lax.fori_loop(0, 8, mix_sent, 0)


SCRATCH = (
    ((SEQ, D), BF),
    ((SEQ, D), BF),
    ((2, 4, 4, 128, 256), BF),
    ((2, 4, 4, 512, 128), BF),
    ((2, 4, 4, 128, 512), BF),
    ((2, 4, 4, 512, 128), BF),
    ((SEQ + 2 * HALO, CW), BF),
    ((4, CB + 2 * HALO, CW), BF),
    ((4, CB, CW), F32),
    ((2, CB, 128), F32),
    ((2, CB, 128), F32),
    ((CB, 4 * CW), BF),
    ((8, RB, 256), BF),
    ((8, RB, 256), BF),
    ((RB, D), F32),
    ((RB, D), BF),
    ((SEQ, 1024), BF),
    ((4, RB, D), BF),
    ((4, RB, D), BF),
    ((4, RB, D), BF),
    ((2, HB, D), BF),
    ((2, RB, D), BF),
)


def shards(*arrays):
    flat = [a.reshape(1, -1) if a.ndim == 1 else a for a in arrays]
    return pl.pallas_call(
        kernel,
        out_shape=jax.ShapeDtypeStruct((RB, D), BF),
        in_specs=[pl.BlockSpec(memory_space=pltpu.VMEM)] * len(flat),
        out_specs=pl.BlockSpec(memory_space=pltpu.VMEM),
        scratch_shapes=[pltpu.VMEM(shape, kind) for shape, kind in SCRATCH]
        + [pltpu.SemaphoreType.DMA((N_SEM,)), pltpu.SemaphoreType.DMA((N_SEM,))],
        compiler_params=pltpu.CompilerParams(
            collective_id=0, has_side_effects=True, vmem_limit_bytes=66 * 1000 * 1000
        ),
        name="layer",
    )(*flat)


def solution(mesh):
    in_specs = (
        P(("fs", "tp"), None),
        P(),
        P("fs", "tp"),
        P("fs", "tp"),
        P(),
        P(),
        P(),
        P(),
        P("tp", "fs"),
        P("fs"),
        P(),
        P("fs", "tp"),
        P("tp"),
        P("tp", "fs"),
        P("fs"),
    )
    out_specs = P(("fs", "tp"), None)
    return jax.shard_map(shards, mesh=mesh, in_specs=in_specs, out_specs=out_specs, check_vma=False)
```

```python
import functools

import jax
import jax.numpy as jnp
from jax import lax
from jax.experimental import pallas as pl
from jax.experimental.pallas import tpu as pltpu
from jax.sharding import PartitionSpec as P

BF = jnp.bfloat16
F32 = jnp.float32
MESH = pl.DeviceIdType.MESH

RB = 192
QB = 48
CB = 384
SEQ = 1536
D = 2048
CW = 256
HALO = 16
FAR = 208
KERNEL = 31
GROUP_WIDTH = 512.0
N_SEM = 260

ORDER = (
    "V.s0", "D.s0", "px.0", "R1.oa", "c.init", "px.1", "V.s1", "R1.ob", "U.s0", "V.s2", "R1.oc", "U.s1",
    "R1.ra", "px.2", "V.s3", "P.s0", "R1.rb", "V.s4", "R1.nr", "P.s1", "D.s1", "c.gx", "P.s2", "R1.nw",
    "c.gp", "R1.fa", "c.sp", "c.gm", "R1.fb", "R1.fw", "c.gf", "P.s3", "c.cx", "c.fr", "U.s2", "c.cm", "c.cp",
    "c.cf", "c.st", "P.s4", "c.ac", "c.pt", "c.nm", "R2.oa", "U.s3", "R2.ob", "R2.oc", "D.s2", "R2.ra",
    "D.s3", "U.s4", "c.ux", "R2.rb", "R2.nr", "R2.nw", "c.up", "R2.fa", "c.um", "D.s4", "d.pl", "R2.fb",
    "R2.fw", "c.uf", "d.fa", "d.la", "d.sl", "d.xx", "d.fn",
)


def dot(a, b):
    return jnp.dot(a, b, preferred_element_type=F32)


class Copies:
    def __init__(self, send, recv):
        self.send, self.recv, self.used, self.started = send, recv, 0, []

    def take(self, count=1):
        at = self.used
        self.used += count
        assert self.used <= N_SEM
        return at

    def copy(self, src, dst, device, at=None):
        at = self.take() if at is None else at
        return pltpu.make_async_remote_copy(
            src_ref=src,
            dst_ref=dst,
            send_sem=self.send.at[at],
            recv_sem=self.recv.at[at],
            device_id=device,
            device_id_type=MESH,
        )

    def start(self, src, dst, device):
        made = self.copy(src, dst, device)
        made.start()
        self.started.append(made)
        return made

    def finish(self):
        for made in self.started:
            made.wait_send()


def kernel(
    resid,
    gain1,
    w_value,
    w_gate,
    value_scale,
    gate_scale,
    taps,
    conv_gain,
    w_point,
    point_scale,
    gain2,
    w_up,
    up_scale,
    w_down,
    down_scale,
    out,
    x1,
    x2,
    vg,
    pp,
    uu,
    dd,
    glu,
    cin,
    cv,
    st,
    st_in,
    act,
    mix_out,
    mix_in,
    mix,
    mid,
    hid,
    par_out,
    par_in,
    par,
    rel_in,
    fin_in,
    far_in,
    out_buf,
    send_sem,
    recv_sem,
):
    fs = lax.axis_index("fs")
    tp = lax.axis_index("tp")
    z, y = fs // 4, fs % 4
    x, c = tp // 2, tp % 2
    xp, xm, xf = (x + 1) % 4, (x + 3) % 4, (x + 2) % 4
    yp, ym = (y + 1) % 4, (y + 3) % 4
    zp, zm = (z + 1) % 4, (z + 3) % 4
    to_xp, to_xm, to_xf = ({"tp": v * 2 + c} for v in (xp, xm, xf))
    to_pair = {"tp": x * 2 + 1 - c}
    to_yp, to_ym = ({"fs": z * 4 + v} for v in (yp, ym))
    to_zp, to_zm = ({"fs": v * 4 + y} for v in (zp, zm))
    cp = Copies(send_sem, recv_sem)

    barrier = pltpu.get_barrier_semaphore()
    for peer in (to_pair, to_xp, to_xm, to_xf, to_yp, to_ym, to_zp, to_zm):
        pl.semaphore_signal(barrier, inc=1, device_id=peer, device_id_type=MESH)

    vg[0, z, y] = w_value[...].astype(BF)
    vg[1, z, y] = w_gate[...].astype(BF)
    own_point = pp.at[x // 2, z, y, pl.ds(pl.multiple_of((x % 2) * 256, 256), 256)]
    own_point[...] = (w_point[...] * point_scale[...]).astype(BF)
    for half in range(2):
        uu[half, z, y] = w_up[:, half * 512 : half * 512 + 512].astype(BF)
        dd[half, z, y] = (w_down[half * 512 : half * 512 + 512, :] * down_scale[...]).astype(BF)

    def norm_rows(source, gain, target, base):
        def step(i, carry):
            rows = pl.multiple_of(i * 16, 16)
            v = source[pl.ds(rows, 16), :].astype(F32)
            scale = lax.rsqrt(jnp.mean(v * v, axis=-1, keepdims=True) + 1e-06)
            at = pl.multiple_of(base + i * 16, 16)
            target[pl.ds(at, 16), :] = (v * scale * gain[...]).astype(BF)
            return carry

        lax.fori_loop(0, RB // 16, step, 0)

    norm_rows(resid, gain1, x1, tp * RB)
    pl.semaphore_wait(barrier, 8)

    class Ring:
        def __init__(self, buf):
            self.buf = buf

        def at(self, v, first, count):
            return self.buf.at[pl.ds(pl.multiple_of(v * CB + c * RB + first * QB, 16), count * QB)]

        def both(self, up, down):
            pair = []
            for (v, first, count), peer in ((up, to_xp), (down, to_xm)):
                ref = self.at(v, first, count)
                pair.append(cp.start(ref, ref, peer))
            return pair

        def share(self, waits, blocks):
            made = []
            for wait, (v, first, count) in zip(waits, blocks):
                wait.wait_recv()
                ref = self.at(v, first, count)
                made.append(cp.start(ref, ref, to_pair))
            return made

        def oa(self):
            self.a = self.both((x, 0, 1), (x, 2, 1))

        def ob(self):
            self.b = self.both((x, 1, 1), (x, 3, 1))
            whole = self.at(x, 0, 4)
            self.d0 = cp.start(whole, whole, to_pair)

        def oc(self):
            self.c = self.both((x, 2, 2), (x, 0, 2))

        def relay(self, waits, up, down):
            pair = []
            for wait, (v, first, count), peer in zip(waits, (up, down), (to_xp, to_xm)):
                wait.wait_recv()
                ref = self.at(v, first, count)
                pair.append(cp.start(ref, ref, peer))
                self.near.append(cp.start(ref, ref, to_pair))
            return pair

        def ra(self):
            self.near = []
            self.ra_made = self.relay(self.a, (xm, 0, 1), (xp, 2, 1))

        def rb(self):
            self.rb_made = self.relay(self.b, (xm, 1, 1), (xp, 3, 1))

        def nr(self):
            self.near += self.share(self.c, ((xm, 2, 2), (xp, 0, 2)))

        def nw(self):
            for made in self.near:
                made.wait_recv()

        def fa(self):
            self.far = self.share(self.ra_made, ((xf, 0, 1), (xf, 2, 1)))

        def fb(self):
            self.far += self.share(self.rb_made, ((xf, 1, 1), (xf, 3, 1)))

        def fw(self):
            for made in self.far:
                made.wait_recv()

    class Weights:
        def __init__(self, buf):
            self.buf, self.deep = buf, buf.shape[3]

        def s0(self):
            half = self.deep // 2
            parts = pl.ds(0, half), pl.ds(half, half)
            self.first = []
            for turn in range(2):
                lo, hi = parts[turn], parts[1 - turn]
                plan = (
                    (self.buf.at[0, z, y, lo], to_yp),
                    (self.buf.at[1, z, y, lo], to_zp),
                    (self.buf.at[0, z, y, hi], to_ym),
                    (self.buf.at[1, z, y, hi], to_zm),
                )
                self.first += [cp.start(ref, ref, peer) for ref, peer in plan]

        def s1(self):
            half = self.deep // 2
            lo, hi = pl.ds(0, half), pl.ds(half, half)
            plan = (
                (self.buf.at[0, z, ym, lo], to_yp),
                (self.buf.at[1, zm, y, lo], to_zp),
                (self.buf.at[0, z, yp, hi], to_ym),
                (self.buf.at[1, zp, y, hi], to_zm),
            )
            self.second = []
            for made, (ref, peer) in zip(self.first, plan):
                made.wait_recv()
                self.second.append(cp.start(ref, ref, peer))

        def s2(self):
            for made in self.first[4:] + self.second:
                made.wait_recv()
            parts = pl.ds(0, 2), pl.ds(2, 2)
            self.third = []
            for turn in range(2):
                lo, hi = parts[turn], parts[1 - turn]
                plan = (
                    (self.buf.at[0, z, lo], to_zp),
                    (self.buf.at[1, lo, y], to_yp),
                    (self.buf.at[0, z, hi], to_zm),
                    (self.buf.at[1, hi, y], to_ym),
                )
                self.third += [cp.start(ref, ref, peer) for ref, peer in plan]

        def s3(self):
            lo, hi = pl.ds(0, 2), pl.ds(2, 2)
            plan = (
                (self.buf.at[0, zm, lo], to_zp),
                (self.buf.at[1, lo, ym], to_yp),
                (self.buf.at[0, zp, hi], to_zm),
                (self.buf.at[1, hi, yp], to_ym),
            )
            self.fourth = []
            for made, (ref, peer) in zip(self.third, plan):
                made.wait_recv()
                self.fourth.append(cp.start(ref, ref, peer))

        def s4(self):
            for made in self.third[4:] + self.fourth:
                made.wait_recv()

    ring1, ring2 = Ring(x1), Ring(x2)
    gv, gp, gu, gd = Weights(vg), Weights(pp), Weights(uu), Weights(dd)

    def point_rows(v, first, count):
        rows = pl.ds(pl.multiple_of((v % 2) * 256 + first, 128), count)
        return pp.at[v // 2, z, y, rows]

    steps = {}
    made = {}

    def step_named(name):
        def keep(body):
            steps[name] = body
            return body

        return keep

    for name, chain in (("V", gv), ("P", gp), ("U", gu), ("D", gd)):
        for part in ("s0", "s1", "s2", "s3", "s4"):
            steps[name + "." + part] = getattr(chain, part)
    for name, chain in (("R1", ring1), ("R2", ring2)):
        for part in ("oa", "ob", "oc", "ra", "rb", "nr", "nw", "fa", "fb", "fw"):
            steps[name + "." + part] = getattr(chain, part)

    def wait(*names):
        for name in names:
            made[name].wait_recv()

    def send_point(name, v, first, count, peer):
        ref = pp.at[v // 2, z, y, pl.ds(pl.multiple_of((v % 2) * 256 + first, 128), count)]
        made[name] = cp.start(ref, ref, peer)

    @step_named("px.0")
    def _():
        send_point("pxp", x, 0, 256, to_xp)
        send_point("pxm", x, 0, 256, to_xm)

    @step_named("px.1")
    def _():
        wait("pxp")
        send_point("pxl", xm, 0, 128, to_xp)
        wait("pxm")
        send_point("pxh", xp, 128, 128, to_xm)

    steps["px.2"] = lambda: wait("pxl", "pxh")

    @step_named("c.init")
    def _():
        glu[0:HALO, :] = jnp.zeros((HALO, CW), BF)
        glu[HALO + SEQ : HALO + SEQ + HALO, :] = jnp.zeros((HALO, CW), BF)
        st[...] = jnp.zeros(st.shape, F32)

    own_cols = pl.ds(pl.multiple_of(tp * CW, CW), CW)

    def gated(v):
        rows = pl.multiple_of(v * CB, CB)
        block = x1[pl.ds(rows, CB), :]
        value = dot(block, vg[0].reshape(D, CW)) * value_scale[:, own_cols]
        gate = dot(block, vg[1].reshape(D, CW)) * gate_scale[:, own_cols]
        glu[pl.ds(pl.multiple_of(rows + HALO, 16), CB), :] = (value * jax.nn.sigmoid(gate)).astype(BF)

    @step_named("c.gx")
    def _():
        ring1.d0.wait_recv()
        gated(x)

    steps["c.gp"] = lambda: gated(xp)

    def send_glu(name, v, first, count, peer):
        rows = pl.ds(pl.multiple_of(v * CB + first, 16), count)
        made[name] = cp.start(glu.at[rows], cin.at[x, pl.ds(first, count)], peer)

    def send_far(name, first, slot, peer):
        rows = pl.ds(pl.multiple_of(xf * CB + first, 16), FAR)
        made[name] = cp.start(glu.at[rows], far_in.at[slot], peer)

    steps["c.sp"] = lambda: send_glu("gp", xp, 0, CB + HALO, to_xp)

    @step_named("c.gm")
    def _():
        gated(xm)
        send_glu("gm", xm, HALO, CB + HALO, to_xm)

    @step_named("c.gf")
    def _():
        gated(xf)
        send_far("fl", 0, 0, to_xp)
        send_far("fh", FAR, 1, to_xm)
        send_glu("ep", xp, CB + HALO, HALO, to_xp)
        send_glu("em", xm, 0, HALO, to_xm)

    def convolve(v):
        def step(i, carry):
            part, chunk = i % 2, i // 2
            lane = pl.multiple_of(part * 128, 128)
            row = pl.multiple_of(chunk * 64, 64)
            col = pl.multiple_of((2 * v + c) * CW + part * 128, 128)
            data = cin[v, pl.ds(row, 96), pl.ds(lane, 128)].astype(F32)
            total = jnp.zeros((64, 128), F32)
            for b in range(8):
                turned = data if b == 0 else pltpu.roll(data, 96 - b, 0)
                for a in range(4):
                    k = 8 * a + b
                    if k:
                        tap = taps[k - 1 : k, pl.ds(col, 128)]
                        total = total + tap * turned[8 * a : 8 * a + 64]
            cv[v, pl.ds(row, 64), pl.ds(lane, 128)] = total
            st[0, pl.ds(row, 64), :] += total
            st[1, pl.ds(row, 64), :] += total * total
            return carry

        lax.fori_loop(0, 12, step, 0)

    @step_named("c.cx")
    def _():
        cin[x] = glu[pl.ds(pl.multiple_of(x * CB, CB), CB + 2 * HALO), :]
        convolve(x)

    @step_named("c.fr")
    def _():
        wait("fl")
        made["l2"] = cp.start(far_in.at[0], cin.at[xm, pl.ds(0, FAR)], to_xp)
        wait("fh")
        made["h2"] = cp.start(far_in.at[1], cin.at[xp, pl.ds(FAR, FAR)], to_xm)

    @step_named("c.cm")
    def _():
        wait("gp", "ep")
        convolve(xm)

    @step_named("c.cp")
    def _():
        wait("gm", "em")
        convolve(xp)

    @step_named("c.cf")
    def _():
        wait("l2", "h2")
        convolve(xf)

    @step_named("c.st")
    def _():
        for kind in range(2):
            total = st[kind]
            for shift in (4, 8, 16, 32, 64):
                total = total + pltpu.roll(total, shift, 1)
            st[kind] = total
        made["st"] = cp.start(st, st_in, to_pair)

    def activate(i, carry):
        rows = pl.ds(pl.multiple_of(i * 32, 32), 32)
        gmean = (st[0, rows, :] + st_in[0, rows, :]) / GROUP_WIDTH
        gsquare = (st[1, rows, :] + st_in[1, rows, :]) / GROUP_WIDTH
        inv = lax.rsqrt(gsquare - gmean * gmean + 1e-05)
        for v in range(4):
            for part in range(2):
                col = pl.multiple_of((2 * v + c) * CW + part * 128, 128)
                lane = part * 128
                s = (cv[v, rows, lane : lane + 128] - gmean) * inv * conv_gain[:, pl.ds(col, 128)]
                act[rows, v * CW + lane : v * CW + lane + 128] = (s / (1.0 + jnp.exp(-s))).astype(BF)
        return carry

    @step_named("c.ac")
    def _():
        wait("st")
        lax.fori_loop(0, CB // 32, activate, 0)

    pair_rows = pl.ds(pl.multiple_of((1 - c) * RB, RB), RB)
    own_rows = pl.ds(pl.multiple_of(c * RB, RB), RB)
    mix_at = cp.take(8)

    def mix_copy(n):
        return cp.copy(mix_out.at[n], mix_in.at[n], to_pair, mix_at + n)

    def columns(buf, half, n):
        two = buf[half, n // 2, pl.ds((n % 2) * 2, 2)]
        return jnp.concatenate([two[0], two[1]], axis=1)

    def point(n, carry):
        left = jnp.concatenate([act[pair_rows, 0:512], act[own_rows, 0:512]], axis=0)
        right = jnp.concatenate([act[pair_rows, 512:1024], act[own_rows, 512:1024]], axis=0)
        both = dot(left, columns(pp, 0, n)) + dot(right, columns(pp, 1, n))
        mix_out[n] = both[:RB].astype(BF)
        mix_copy(n).start()
        mix[:, pl.ds(pl.multiple_of(n * 256, 256), 256)] = both[RB:]
        return carry

    steps["c.pt"] = lambda: lax.fori_loop(0, 8, point, 0)

    def add_mixed(n, carry):
        mix_copy(n).wait_recv()
        cols = pl.ds(pl.multiple_of(n * 256, 256), 256)
        mixed = mix[:, cols] + mix_in[n].astype(F32)
        mid[:, cols] = (resid[:, cols].astype(F32) + mixed).astype(BF)
        return carry

    @step_named("c.nm")
    def _():
        lax.fori_loop(0, 8, add_mixed, 0)
        norm_rows(mid, gain2, x2, tp * RB)

    def up(v):
        rows = pl.ds(pl.multiple_of(v * CB, CB), CB)

        def step(n, carry):
            weight = uu[n // 2, :, :, :, pl.ds(pl.multiple_of((n % 2) * 256, 256), 256)].reshape(D, 256)
            cols = pl.ds(pl.multiple_of(n * 256, 256), 256)
            upper = jnp.maximum(dot(x2[rows, :], weight) * up_scale[:, cols], 0.0)
            hid[rows, cols] = (upper * upper).astype(BF)
            return carry

        lax.fori_loop(0, 4, step, 0)

    @step_named("c.ux")
    def _():
        ring2.d0.wait_recv()
        up(x)

    steps["c.up"] = lambda: up(xp)
    steps["c.um"] = lambda: up(xm)
    steps["c.uf"] = lambda: up(xf)

    pair_at, last_at, out_at = cp.take(32), cp.take(24), cp.take(8)

    def to_other(v, n):
        return cp.copy(par_out.at[v, n], par_in.at[v, n], to_pair, pair_at + v * 8 + n)

    def down(v, n):
        pair_rows = pl.ds(pl.multiple_of(v * CB + (1 - c) * RB, RB), RB)
        own_rows = pl.ds(pl.multiple_of(v * CB + c * RB, RB), RB)
        left = jnp.concatenate([hid[pair_rows, 0:512], hid[own_rows, 0:512]], axis=0)
        right = jnp.concatenate([hid[pair_rows, 512:1024], hid[own_rows, 512:1024]], axis=0)
        both = dot(left, columns(dd, 0, n)) + dot(right, columns(dd, 1, n))
        par_out[v, n] = both[:RB].astype(BF)
        to_other(v, n).start()
        par[v, n] = both[RB:].astype(BF)

    def add_pair(v, n):
        to_other(v, n).wait_recv()
        par[v, n] = (par[v, n].astype(F32) + par_in[v, n].astype(F32)).astype(BF)

    def relay(side, k):
        n = k + 4 * side
        return cp.copy(par.at[xf, n], rel_in.at[side, k], to_xm if side else to_xp, last_at + n)

    def plain(side, k):
        n = k + 4 * (1 - side)
        to, peer = (xm, to_xm) if side else (xp, to_xp)
        return cp.copy(par.at[to, n], fin_in.at[side, n], peer, last_at + 8 + side * 4 + k)

    def last(side, k):
        n = k + 4 * side
        to, peer = (xm, to_xm) if side else (xp, to_xp)
        return cp.copy(par.at[to, n], fin_in.at[side, n], peer, last_at + 16 + side * 4 + k)

    def each(count, body):
        def step(i, carry):
            body(i)
            return carry

        lax.fori_loop(0, count, step, 0)

    def relay_chunk(j):
        add_pair(xf, (j % 2) * 4 + j // 2)

        @pl.when(j % 2 == 0)
        def _():
            relay(0, j // 2).start()

        @pl.when(j % 2 == 1)
        def _():
            relay(1, j // 2).start()

    @step_named("d.fa")
    def _():
        def far_step(i):
            down(xf, (i % 2) * 4 + i // 2)

            @pl.when(i >= 3)
            def _():
                relay_chunk(i - 3)

        each(8, far_step)
        each(3, lambda i: relay_chunk(i + 5))

    @step_named("d.pl")
    def _():
        def plain_chunk(k):
            add_pair(xp, k + 4)
            plain(0, k).start()
            add_pair(xm, k)
            plain(1, k).start()

        def near_step(k):
            down(xp, k + 4)
            down(xm, k)

            @pl.when(k >= 1)
            def _():
                plain_chunk(k - 1)

        each(4, near_step)
        plain_chunk(3)

    @step_named("d.la")
    def _():
        def last_step(k):
            down(xp, k)
            down(xm, k + 4)

        each(4, last_step)

    @step_named("d.sl")
    def _():
        def send_last(k):
            for side, v in ((0, xp), (1, xm)):
                n = k + 4 * side
                to_other(v, n).wait_recv()
                relay(side, k).wait_recv()
                total = par[v, n].astype(F32) + par_in[v, n].astype(F32) + rel_in[side, k].astype(F32)
                par[v, n] = total.astype(BF)
                last(side, k).start()

        each(4, send_last)

    @step_named("d.xx")
    def _():
        each(8, lambda n: down(x, n))

        def own_step(n):
            to_other(x, n).wait_recv()
            cols = pl.ds(pl.multiple_of(n * 256, 256), 256)
            mix[:, cols] = mid[:, cols].astype(F32) + (par[x, n].astype(F32) + par_in[x, n].astype(F32))

        each(8, own_step)

    def out_copy(n):
        cols = pl.ds(pl.multiple_of(n * 256, 256), 256)
        return pltpu.make_async_copy(out_buf.at[n], out.at[:, cols], recv_sem.at[out_at + n])

    def finish(k):
        for n, near, far in ((k, last(0, k), plain(1, k)), (k + 4, plain(0, k), last(1, k))):
            near.wait_recv()
            far.wait_recv()
            cols = pl.ds(pl.multiple_of(n * 256, 256), 256)
            total = fin_in[0, n].astype(F32) + fin_in[1, n].astype(F32)
            out_buf[n] = (mix[:, cols] + total).astype(BF)
            out_copy(n).start()

    steps["d.fn"] = lambda: each(4, finish)
    for name in ORDER:
        with jax.named_scope(name):
            steps[name]()
    assert len(ORDER) == len(set(ORDER)) == len(steps)
    cp.finish()

    def sent(n):
        mix_copy(n).wait_send()
        for v in range(4):
            to_other(v, n).wait_send()
        out_copy(n).wait()

    each(8, sent)

    def sent_last(k):
        for side in range(2):
            for made in (relay(side, k), plain(side, k), last(side, k)):
                made.wait_send()

    each(4, sent_last)


SCRATCH = (
    ((SEQ, D), BF),
    ((SEQ, D), BF),
    ((2, 4, 4, 128, 256), BF),
    ((2, 4, 4, 512, 128), BF),
    ((2, 4, 4, 128, 512), BF),
    ((2, 4, 4, 512, 128), BF),
    ((SEQ + 2 * HALO, CW), BF),
    ((4, CB + 2 * HALO, CW), BF),
    ((4, CB, CW), F32),
    ((2, CB, 128), F32),
    ((2, CB, 128), F32),
    ((CB, 4 * CW), BF),
    ((8, RB, 256), BF),
    ((8, RB, 256), BF),
    ((RB, D), F32),
    ((RB, D), BF),
    ((SEQ, 1024), BF),
    ((4, 8, RB, 256), BF),
    ((4, 8, RB, 256), BF),
    ((4, 8, RB, 256), BF),
    ((2, 4, RB, 256), BF),
    ((2, 8, RB, 256), BF),
    ((2, FAR, CW), BF),
    ((8, RB, 256), BF),
)


def shards(*arrays):
    flat = [a.reshape(1, -1) if a.ndim == 1 else a for a in arrays]
    return pl.pallas_call(
        kernel,
        out_shape=jax.ShapeDtypeStruct((RB, D), BF),
        in_specs=[pl.BlockSpec(memory_space=pltpu.VMEM)] * len(flat),
        out_specs=pl.BlockSpec(memory_space=pl.ANY),
        scratch_shapes=[pltpu.VMEM(shape, kind) for shape, kind in SCRATCH]
        + [pltpu.SemaphoreType.DMA((N_SEM,)), pltpu.SemaphoreType.DMA((N_SEM,))],
        compiler_params=pltpu.CompilerParams(
            collective_id=0, has_side_effects=True, vmem_limit_bytes=66 * 1000 * 1000
        ),
        name="layer",
    )(*flat)


def solution(mesh):
    in_specs = (
        P(("fs", "tp"), None),
        P(),
        P("fs", "tp"),
        P("fs", "tp"),
        P(),
        P(),
        P(),
        P(),
        P("tp", "fs"),
        P("fs"),
        P(),
        P("fs", "tp"),
        P("tp"),
        P("tp", "fs"),
        P("fs"),
    )
    out_specs = P(("fs", "tp"), None)
    return jax.shard_map(shards, mesh=mesh, in_specs=in_specs, out_specs=out_specs, check_vma=False)
```

```python
import functools

import jax
import jax.numpy as jnp
from jax import lax
from jax.experimental import pallas as pl
from jax.experimental.pallas import tpu as pltpu
from jax.sharding import PartitionSpec as P

BF = jnp.bfloat16
F32 = jnp.float32
MESH = pl.DeviceIdType.MESH

RB = 192
QB = 48
CB = 384
SEQ = 1536
D = 2048
CW = 256
HALO = 16
FAR = 208
KERNEL = 31
GROUP_WIDTH = 512.0
N_SEND, N_RECV = 12, 112

ORDER = (
    "V.s0", "px.0", "c.n1", "R1.oa", "c.ld", "D.s0", "px.1", "V.s1", "R1.ob", "U.s0", "c.init", "V.s2",
    "R1.oc", "U.s1", "px.2", "P.s0", "R1.ra", "V.s3", "R1.rb", "P.s1", "V.s4", "R1.nr", "D.s1", "c.gx",
    "P.s2", "R1.nw", "c.gp", "R1.fa", "c.sp", "c.gm", "R1.fb", "R1.fw", "c.gf", "P.s3", "c.cx", "c.fr",
    "U.s2", "c.cm", "c.cp", "c.cf", "c.st", "P.s4", "c.ac", "c.pt", "c.nm", "R2.oa", "U.s3", "R2.ob", "R2.oc",
    "D.s2", "R2.ra", "D.s3", "U.s4", "c.ux", "R2.rb", "R2.nr", "R2.nw", "c.up", "R2.fa", "c.um", "D.s4",
    "d.pl", "R2.fb", "R2.fw", "c.uf", "d.fa", "d.la", "d.sl", "d.xx", "d.fn",
)


def dot(a, b):
    return jnp.dot(a, b, preferred_element_type=F32)


class Copies:
    def __init__(self, send, recv, peer):
        self.send, self.recv, self.peer = send, recv, peer
        self.sends, self.recvs, self.finals = 0, 0, []

    def take(self, count=1):
        at = self.recvs
        self.recvs += count
        assert self.recvs <= N_RECV
        return at

    def take_send(self, total):
        at = self.sends
        self.sends += 1
        assert self.sends <= N_SEND
        self.finals.append((total, at))
        return at

    def copy(self, src, dst, device, recv, send):
        return pltpu.make_async_remote_copy(
            src_ref=src,
            dst_ref=dst,
            send_sem=self.send.at[send],
            recv_sem=self.recv.at[recv],
            device_id=device,
            device_id_type=MESH,
        )

    def start(self, ref, device, recv, send):
        self.copy(ref, ref, device, recv, send).start()

    def arrived(self, total, recv):
        self.copy(total, total, self.peer, recv, 0).wait_recv()

    def finish(self):
        for total, at in self.finals:
            self.copy(total, total, self.peer, 0, at).wait_send()


def kernel(*refs):
    hbm, out, local, refs = refs[:15], refs[15], refs[16:31], refs[31:]
    x1, x2, vg, pp, uu, dd, glu, cin, cv, st, st_in, act, mix_out, mix_in, mix, mid, hid = refs[:17]
    par_out, par_in, par, rel_in, fin_in, far_in, out_buf, send_sem, recv_sem, load_sem, out_sem = refs[17:]
    resid, gain1, w_value, w_gate, value_scale, gate_scale, taps, conv_gain = local[:8]
    w_point, point_scale, gain2, w_up, up_scale, w_down, down_scale = local[8:]

    fs = lax.axis_index("fs")
    tp = lax.axis_index("tp")
    z, y = fs // 4, fs % 4
    x, c = tp // 2, tp % 2
    xp, xm, xf = (x + 1) % 4, (x + 3) % 4, (x + 2) % 4
    yp, ym = (y + 1) % 4, (y + 3) % 4
    zp, zm = (z + 1) % 4, (z + 3) % 4
    to_xp, to_xm = ({"tp": v * 2 + c} for v in (xp, xm))
    to_pair = {"tp": x * 2 + 1 - c}
    to_yp, to_ym = ({"fs": z * 4 + v} for v in (yp, ym))
    to_zp, to_zm = ({"fs": v * 4 + y} for v in (zp, zm))
    cp = Copies(send_sem, recv_sem, to_pair)

    barrier = pltpu.get_barrier_semaphore()
    for peer in (to_pair, to_xp, to_xm, to_yp, to_ym, to_zp, to_zm):
        pl.semaphore_signal(barrier, inc=1, device_id=peer, device_id_type=MESH)

    loads = [pltpu.make_async_copy(a, b, load_sem.at[i]) for i, (a, b) in enumerate(zip(hbm, local))]
    for i in (2, 3, 8, 9, 0, 1, 13, 14, 11, 4, 5, 6, 7, 10, 12):
        loads[i].start()

    for i in (2, 3, 8, 9):
        loads[i].wait()
    vg[0, z, y] = w_value[...].astype(BF)
    vg[1, z, y] = w_gate[...].astype(BF)
    own_point = pp.at[x // 2, z, y, pl.ds(pl.multiple_of((x % 2) * 256, 256), 256)]
    own_point[...] = (w_point[...] * point_scale[...]).astype(BF)

    def norm_rows(source, gain, target, base):
        def step(i, carry):
            rows = pl.multiple_of(i * 16, 16)
            v = source[pl.ds(rows, 16), :].astype(F32)
            scale = lax.rsqrt(jnp.mean(v * v, axis=-1, keepdims=True) + 1e-06)
            at = pl.multiple_of(base + i * 16, 16)
            target[pl.ds(at, 16), :] = (v * scale * gain[...]).astype(BF)
            return carry

        lax.fori_loop(0, RB // 16, step, 0)

    class Ring:
        def __init__(self, buf):
            self.buf = buf
            self.sem = {name: cp.take() for name in ("a", "b", "c", "d", "ra", "rb", "near", "far")}
            self.send = cp.take_send(buf.at[0 : 28 * QB])

        def at(self, v, first, count):
            return self.buf.at[pl.ds(pl.multiple_of(v * CB + c * RB + first * QB, 16), count * QB)]

        def both(self, name, up, down):
            for (v, first, count), peer in ((up, to_xp), (down, to_xm)):
                cp.start(self.at(v, first, count), peer, self.sem[name], self.send)

        def share(self, name, *blocks):
            for v, first, count in blocks:
                cp.start(self.at(v, first, count), to_pair, self.sem[name], self.send)

        def arrived(self, name, quarters):
            cp.arrived(self.buf.at[0 : quarters * QB], self.sem[name])

        def oa(self):
            self.both("a", (x, 0, 1), (x, 2, 1))

        def ob(self):
            self.both("b", (x, 1, 1), (x, 3, 1))
            self.share("d", (x, 0, 4))

        def oc(self):
            self.both("c", (x, 2, 2), (x, 0, 2))

        def ra(self):
            self.arrived("a", 2)
            self.both("ra", (xm, 0, 1), (xp, 2, 1))
            self.share("near", (xm, 0, 1), (xp, 2, 1))

        def rb(self):
            self.arrived("b", 2)
            self.both("rb", (xm, 1, 1), (xp, 3, 1))
            self.share("near", (xm, 1, 1), (xp, 3, 1))

        def nr(self):
            self.arrived("c", 4)
            self.share("near", (xm, 2, 2), (xp, 0, 2))

        def nw(self):
            self.arrived("near", 8)

        def fa(self):
            self.arrived("ra", 2)
            self.share("far", (xf, 0, 1), (xf, 2, 1))

        def fb(self):
            self.arrived("rb", 2)
            self.share("far", (xf, 1, 1), (xf, 3, 1))

        def fw(self):
            self.arrived("far", 4)

        def own_wait(self):
            self.arrived("d", 4)

    class Weights:
        def __init__(self, buf):
            self.buf, self.deep = buf, buf.shape[3]
            self.sem = [cp.take() for _ in range(6)]
            rows = 30 * buf.shape[3] * buf.shape[4] // D
            self.send = cp.take_send(x1.at[0:rows])

        def four(self, sem, plan):
            for ref, peer in plan:
                cp.start(ref, peer, self.sem[sem], self.send)

        def s0(self):
            half = self.deep // 2
            parts = pl.ds(0, half), pl.ds(half, half)
            for turn in range(2):
                lo, hi = parts[turn], parts[1 - turn]
                plan = (
                    (self.buf.at[0, z, y, lo], to_yp),
                    (self.buf.at[1, z, y, lo], to_zp),
                    (self.buf.at[0, z, y, hi], to_ym),
                    (self.buf.at[1, z, y, hi], to_zm),
                )
                self.four(turn, plan)

        def s1(self):
            half = self.deep // 2
            lo, hi = pl.ds(0, half), pl.ds(half, half)
            plan = (
                (self.buf.at[0, z, ym, lo], to_yp),
                (self.buf.at[1, zm, y, lo], to_zp),
                (self.buf.at[0, z, yp, hi], to_ym),
                (self.buf.at[1, zp, y, hi], to_zm),
            )
            cp.arrived(self.buf.at[0, 0, 0:2], self.sem[0])
            self.four(2, plan)

        def s2(self):
            cp.arrived(self.buf.at[0, 0, 0:2], self.sem[1])
            cp.arrived(self.buf.at[0, 0, 0:2], self.sem[2])
            parts = pl.ds(0, 2), pl.ds(2, 2)
            for turn in range(2):
                lo, hi = parts[turn], parts[1 - turn]
                plan = (
                    (self.buf.at[0, z, lo], to_zp),
                    (self.buf.at[1, lo, y], to_yp),
                    (self.buf.at[0, z, hi], to_zm),
                    (self.buf.at[1, hi, y], to_ym),
                )
                self.four(3 + turn, plan)

        def s3(self):
            lo, hi = pl.ds(0, 2), pl.ds(2, 2)
            plan = (
                (self.buf.at[0, zm, lo], to_zp),
                (self.buf.at[1, lo, ym], to_yp),
                (self.buf.at[0, zp, hi], to_zm),
                (self.buf.at[1, hi, yp], to_ym),
            )
            cp.arrived(self.buf.at[0, 0:2], self.sem[3])
            self.four(5, plan)

        def s4(self):
            cp.arrived(self.buf.at[0, 0:2], self.sem[4])
            cp.arrived(self.buf.at[0, 0:2], self.sem[5])

    ring1, ring2 = Ring(x1), Ring(x2)
    gv, gp, gu, gd = Weights(vg), Weights(pp), Weights(uu), Weights(dd)

    steps = {}

    def step_named(name):
        def keep(body):
            steps[name] = body
            return body

        return keep

    for name, chain in (("V", gv), ("P", gp), ("U", gu), ("D", gd)):
        for part in ("s0", "s1", "s2", "s3", "s4"):
            steps[name + "." + part] = getattr(chain, part)
    for name, chain in (("R1", ring1), ("R2", ring2)):
        for part in ("oa", "ob", "oc", "ra", "rb", "nr", "nw", "fa", "fb", "fw"):
            steps[name + "." + part] = getattr(chain, part)

    point_sem, point_send = [cp.take() for _ in range(2)], cp.take_send(x1.at[0:48])

    def send_point(turn, v, first, count, peer):
        ref = pp.at[v // 2, z, y, pl.ds(pl.multiple_of((v % 2) * 256 + first, 128), count)]
        cp.start(ref, peer, point_sem[turn], point_send)

    @step_named("px.0")
    def _():
        send_point(0, x, 0, 256, to_xp)
        send_point(0, x, 0, 256, to_xm)

    @step_named("px.1")
    def _():
        cp.arrived(pp.at[0, 0, 0], point_sem[0])
        send_point(1, xm, 0, 128, to_xp)
        send_point(1, xp, 128, 128, to_xm)

    steps["px.2"] = lambda: cp.arrived(pp.at[0, 0, 0, 0:256], point_sem[1])

    @step_named("c.ld")
    def _():
        for i in (13, 14, 11):
            loads[i].wait()
        for half in range(2):
            uu[half, z, y] = w_up[:, half * 512 : half * 512 + 512].astype(BF)
            dd[half, z, y] = (w_down[half * 512 : half * 512 + 512, :] * down_scale[...]).astype(BF)

    @step_named("c.n1")
    def _():
        loads[0].wait()
        loads[1].wait()
        norm_rows(resid, gain1, x1, tp * RB)

    @step_named("c.init")
    def _():
        glu[0:HALO, :] = jnp.zeros((HALO, CW), BF)
        glu[HALO + SEQ : HALO + SEQ + HALO, :] = jnp.zeros((HALO, CW), BF)
        st[...] = jnp.zeros(st.shape, F32)
        for i in (4, 5, 6, 7, 10, 12):
            loads[i].wait()

    own_cols = pl.ds(pl.multiple_of(tp * CW, CW), CW)

    def gated(v):
        rows = pl.multiple_of(v * CB, CB)
        block = x1[pl.ds(rows, CB), :]
        value = dot(block, vg[0].reshape(D, CW)) * value_scale[:, own_cols]
        gate = dot(block, vg[1].reshape(D, CW)) * gate_scale[:, own_cols]
        glu[pl.ds(pl.multiple_of(rows + HALO, 16), CB), :] = (value * jax.nn.sigmoid(gate)).astype(BF)

    @step_named("c.gx")
    def _():
        ring1.own_wait()
        gated(x)

    steps["c.gp"] = lambda: gated(xp)

    glu_sem = {name: cp.take() for name in ("gp", "gm", "end", "far", "two")}
    glu_send = cp.take_send(x1.at[0:208])

    def send_glu(name, v, first, count, peer):
        rows = pl.ds(pl.multiple_of(v * CB + first, 16), count)
        cp.copy(glu.at[rows], cin.at[x, pl.ds(first, count)], peer, glu_sem[name], glu_send).start()

    def send_far(first, slot, peer):
        rows = pl.ds(pl.multiple_of(xf * CB + first, 16), FAR)
        cp.copy(glu.at[rows], far_in.at[slot], peer, glu_sem["far"], glu_send).start()

    def glu_arrived(name, rows):
        cp.arrived(glu.at[0:rows], glu_sem[name])

    steps["c.sp"] = lambda: send_glu("gp", xp, 0, CB + HALO, to_xp)

    @step_named("c.gm")
    def _():
        gated(xm)
        send_glu("gm", xm, HALO, CB + HALO, to_xm)

    @step_named("c.gf")
    def _():
        gated(xf)
        send_far(0, 0, to_xp)
        send_far(FAR, 1, to_xm)
        send_glu("end", xp, CB + HALO, HALO, to_xp)
        send_glu("end", xm, 0, HALO, to_xm)

    def convolve(v):
        def step(i, carry):
            part, chunk = i % 2, i // 2
            lane = pl.multiple_of(part * 128, 128)
            row = pl.multiple_of(chunk * 64, 64)
            col = pl.multiple_of((2 * v + c) * CW + part * 128, 128)
            data = cin[v, pl.ds(row, 96), pl.ds(lane, 128)].astype(F32)
            total = jnp.zeros((64, 128), F32)
            for b in range(8):
                turned = data if b == 0 else pltpu.roll(data, 96 - b, 0)
                for a in range(4):
                    k = 8 * a + b
                    if k:
                        tap = taps[k - 1 : k, pl.ds(col, 128)]
                        total = total + tap * turned[8 * a : 8 * a + 64]
            cv[v, pl.ds(row, 64), pl.ds(lane, 128)] = total
            st[0, pl.ds(row, 64), :] += total
            st[1, pl.ds(row, 64), :] += total * total
            return carry

        lax.fori_loop(0, 12, step, 0)

    @step_named("c.cx")
    def _():
        cin[x] = glu[pl.ds(pl.multiple_of(x * CB, CB), CB + 2 * HALO), :]
        convolve(x)

    @step_named("c.fr")
    def _():
        glu_arrived("far", 2 * FAR)
        for slot, v, peer in ((0, xm, to_xp), (1, xp, to_xm)):
            there = cin.at[v, pl.ds(slot * FAR, FAR)]
            cp.copy(far_in.at[slot], there, peer, glu_sem["two"], glu_send).start()

    @step_named("c.cm")
    def _():
        glu_arrived("gp", CB + HALO)
        glu_arrived("end", 2 * HALO)
        convolve(xm)

    @step_named("c.cp")
    def _():
        glu_arrived("gm", CB + HALO)
        convolve(xp)

    @step_named("c.cf")
    def _():
        glu_arrived("two", 2 * FAR)
        convolve(xf)

    st_sem, st_send = cp.take(), cp.take_send(st)

    @step_named("c.st")
    def _():
        for kind in range(2):
            total = st[kind]
            for shift in (4, 8, 16, 32, 64):
                total = total + pltpu.roll(total, shift, 1)
            st[kind] = total
        cp.copy(st, st_in, to_pair, st_sem, st_send).start()

    def activate(i, carry):
        rows = pl.ds(pl.multiple_of(i * 32, 32), 32)
        gmean = (st[0, rows, :] + st_in[0, rows, :]) / GROUP_WIDTH
        gsquare = (st[1, rows, :] + st_in[1, rows, :]) / GROUP_WIDTH
        inv = lax.rsqrt(gsquare - gmean * gmean + 1e-05)
        for v in range(4):
            for part in range(2):
                col = pl.multiple_of((2 * v + c) * CW + part * 128, 128)
                lane = part * 128
                s = (cv[v, rows, lane : lane + 128] - gmean) * inv * conv_gain[:, pl.ds(col, 128)]
                act[rows, v * CW + lane : v * CW + lane + 128] = (s / (1.0 + jnp.exp(-s))).astype(BF)
        return carry

    @step_named("c.ac")
    def _():
        cp.arrived(st, st_sem)
        lax.fori_loop(0, CB // 32, activate, 0)

    pair_rows = pl.ds(pl.multiple_of((1 - c) * RB, RB), RB)
    own_rows = pl.ds(pl.multiple_of(c * RB, RB), RB)
    mix_sem, mix_send = cp.take(), cp.take_send(mix_out)

    def columns(buf, n):
        halves = []
        for half in range(2):
            two = buf[half, n // 2, pl.ds((n % 2) * 2, 2)]
            halves.append(jnp.concatenate([two[0], two[1]], axis=1))
        return jnp.concatenate(halves, axis=0)

    def point(n, carry):
        rows = jnp.concatenate([act[pair_rows, :], act[own_rows, :]], axis=0)
        both = dot(rows, columns(pp, n))
        mix_out[n] = both[:RB].astype(BF)
        cp.copy(mix_out.at[n], mix_in.at[n], to_pair, mix_sem, mix_send).start()
        mix[:, pl.ds(pl.multiple_of(n * 256, 256), 256)] = both[RB:]
        return carry

    steps["c.pt"] = lambda: lax.fori_loop(0, 8, point, 0)

    def add_mixed(n, carry):
        cols = pl.ds(pl.multiple_of(n * 256, 256), 256)
        mixed = mix[:, cols] + mix_in[n].astype(F32)
        mid[:, cols] = (resid[:, cols].astype(F32) + mixed).astype(BF)
        return carry

    @step_named("c.nm")
    def _():
        cp.arrived(mix_in, mix_sem)
        lax.fori_loop(0, 8, add_mixed, 0)
        norm_rows(mid, gain2, x2, tp * RB)

    def up(v):
        rows = pl.ds(pl.multiple_of(v * CB, CB), CB)

        def step(n, carry):
            weight = uu[n // 2, :, :, :, pl.ds(pl.multiple_of((n % 2) * 256, 256), 256)].reshape(D, 256)
            cols = pl.ds(pl.multiple_of(n * 256, 256), 256)
            upper = jnp.maximum(dot(x2[rows, :], weight) * up_scale[:, cols], 0.0)
            hid[rows, cols] = (upper * upper).astype(BF)
            return carry

        lax.fori_loop(0, 4, step, 0)

    @step_named("c.ux")
    def _():
        ring2.own_wait()
        up(x)

    steps["c.up"] = lambda: up(xp)
    steps["c.um"] = lambda: up(xm)
    steps["c.uf"] = lambda: up(xf)

    pair_sem = {"f": cp.take(8), "pl": cp.take(4), "la": cp.take(4), "x": cp.take()}
    relay_sem, end_sem = cp.take(4), cp.take(4)
    pair_send, ring_send = cp.take_send(par_out), cp.take_send(par.at[0:3])

    def down(v, n, sem):
        pair_rows = pl.ds(pl.multiple_of(v * CB + (1 - c) * RB, RB), RB)
        own_rows = pl.ds(pl.multiple_of(v * CB + c * RB, RB), RB)
        rows = jnp.concatenate([hid[pair_rows, :], hid[own_rows, :]], axis=0)
        both = dot(rows, columns(dd, n))
        par_out[v, n] = both[:RB].astype(BF)
        cp.copy(par_out.at[v, n], par_in.at[v, n], to_pair, sem, pair_send).start()
        par[v, n] = both[RB:].astype(BF)

    def pair_arrived(sem, count):
        cp.arrived(par_in.at[0, 0:count], sem)

    def add_pair(v, n):
        par[v, n] = (par[v, n].astype(F32) + par_in[v, n].astype(F32)).astype(BF)

    def relay(side, k):
        n = k + 4 * side
        cp.copy(par.at[xf, n], rel_in.at[side, k], to_xm if side else to_xp, relay_sem + k, ring_send).start()

    def plain(side, k):
        n = k + 4 * (1 - side)
        to, peer = (xm, to_xm) if side else (xp, to_xp)
        cp.copy(par.at[to, n], fin_in.at[side, n], peer, end_sem + k, ring_send).start()

    def last(side, k):
        n = k + 4 * side
        to, peer = (xm, to_xm) if side else (xp, to_xp)
        cp.copy(par.at[to, n], fin_in.at[side, n], peer, end_sem + k, ring_send).start()

    def each(count, body):
        def step(i, carry):
            body(i)
            return carry

        lax.fori_loop(0, count, step, 0)

    def relay_chunk(j):
        n = (j % 2) * 4 + j // 2
        pair_arrived(pair_sem["f"] + n, 1)
        add_pair(xf, n)

        @pl.when(j % 2 == 0)
        def _():
            relay(0, j // 2)

        @pl.when(j % 2 == 1)
        def _():
            relay(1, j // 2)

    @step_named("d.fa")
    def _():
        def far_step(i):
            n = (i % 2) * 4 + i // 2
            down(xf, n, pair_sem["f"] + n)

            @pl.when(i >= 3)
            def _():
                relay_chunk(i - 3)

        each(8, far_step)
        each(3, lambda i: relay_chunk(i + 5))

    @step_named("d.pl")
    def _():
        def plain_chunk(k):
            pair_arrived(pair_sem["pl"] + k, 2)
            add_pair(xp, k + 4)
            plain(0, k)
            add_pair(xm, k)
            plain(1, k)

        def near_step(k):
            down(xp, k + 4, pair_sem["pl"] + k)
            down(xm, k, pair_sem["pl"] + k)

            @pl.when(k >= 1)
            def _():
                plain_chunk(k - 1)

        each(4, near_step)
        plain_chunk(3)

    @step_named("d.la")
    def _():
        def last_step(k):
            down(xp, k, pair_sem["la"] + k)
            down(xm, k + 4, pair_sem["la"] + k)

        each(4, last_step)

    @step_named("d.sl")
    def _():
        def send_last(k):
            pair_arrived(pair_sem["la"] + k, 2)
            cp.arrived(rel_in.at[0, 0:2], relay_sem + k)
            for side, v in ((0, xp), (1, xm)):
                n = k + 4 * side
                total = par[v, n].astype(F32) + par_in[v, n].astype(F32) + rel_in[side, k].astype(F32)
                par[v, n] = total.astype(BF)
                last(side, k)

        each(4, send_last)

    @step_named("d.xx")
    def _():
        each(8, lambda n: down(x, n, pair_sem["x"]))
        pair_arrived(pair_sem["x"], 8)

        def own_step(n):
            cols = pl.ds(pl.multiple_of(n * 256, 256), 256)
            mix[:, cols] = mid[:, cols].astype(F32) + (par[x, n].astype(F32) + par_in[x, n].astype(F32))

        each(8, own_step)

    def out_copy(n):
        cols = pl.ds(pl.multiple_of(n * 256, 256), 256)
        return pltpu.make_async_copy(out_buf.at[n], out.at[:, cols], out_sem.at[0])

    def finish(k):
        cp.arrived(fin_in.at[0, 0:4], end_sem + k)
        for n in (k, k + 4):
            cols = pl.ds(pl.multiple_of(n * 256, 256), 256)
            total = fin_in[0, n].astype(F32) + fin_in[1, n].astype(F32)
            out_buf[n] = (mix[:, cols] + total).astype(BF)
            out_copy(n).start()

    steps["d.fn"] = lambda: each(4, finish)
    pl.semaphore_wait(barrier, 7)
    for name in ORDER:
        with jax.named_scope(name):
            steps[name]()
    assert len(ORDER) == len(set(ORDER)) == len(steps)
    cp.finish()
    pltpu.make_async_copy(resid, out, out_sem.at[0]).wait()


SCRATCH = (
    ((SEQ, D), BF),
    ((SEQ, D), BF),
    ((2, 4, 4, 128, 256), BF),
    ((2, 4, 4, 512, 128), BF),
    ((2, 4, 4, 128, 512), BF),
    ((2, 4, 4, 512, 128), BF),
    ((SEQ + 2 * HALO, CW), BF),
    ((4, CB + 2 * HALO, CW), BF),
    ((4, CB, CW), F32),
    ((2, CB, 128), F32),
    ((2, CB, 128), F32),
    ((CB, 4 * CW), BF),
    ((8, RB, 256), BF),
    ((8, RB, 256), BF),
    ((RB, D), F32),
    ((RB, D), BF),
    ((SEQ, 1024), BF),
    ((4, 8, RB, 256), BF),
    ((4, 8, RB, 256), BF),
    ((4, 8, RB, 256), BF),
    ((2, 4, RB, 256), BF),
    ((2, 8, RB, 256), BF),
    ((2, FAR, CW), BF),
    ((8, RB, 256), BF),
)


def shards(*arrays):
    flat = [a.reshape(1, -1) if a.ndim == 1 else a for a in arrays]
    return pl.pallas_call(
        kernel,
        out_shape=jax.ShapeDtypeStruct((RB, D), BF),
        in_specs=[pl.BlockSpec(memory_space=pltpu.HBM)] * len(flat),
        out_specs=pl.BlockSpec(memory_space=pl.ANY),
        scratch_shapes=[pltpu.VMEM(a.shape, a.dtype) for a in flat]
        + [pltpu.VMEM(shape, kind) for shape, kind in SCRATCH]
        + [pltpu.SemaphoreType.DMA((count,)) for count in (N_SEND, N_RECV, len(flat), 1)],
        compiler_params=pltpu.CompilerParams(
            collective_id=0, has_side_effects=True, vmem_limit_bytes=66 * 1000 * 1000
        ),
        name="layer",
    )(*flat)


def solution(mesh):
    in_specs = (
        P(("fs", "tp"), None),
        P(),
        P("fs", "tp"),
        P("fs", "tp"),
        P(),
        P(),
        P(),
        P(),
        P("tp", "fs"),
        P("fs"),
        P(),
        P("fs", "tp"),
        P("tp"),
        P("tp", "fs"),
        P("fs"),
    )
    out_specs = P(("fs", "tp"), None)
    return jax.shard_map(shards, mesh=mesh, in_specs=in_specs, out_specs=out_specs, check_vma=False)
```

```python
import functools

import jax
import jax.numpy as jnp
from jax import lax
from jax.experimental import pallas as pl
from jax.experimental.pallas import tpu as pltpu
from jax.sharding import PartitionSpec as P

BF = jnp.bfloat16
F32 = jnp.float32
MESH = pl.DeviceIdType.MESH

RB = 192
QB = 48
CB = 384
SEQ = 1536
D = 2048
CW = 256
HALO = 16
FAR = 208
KERNEL = 31
GROUP_WIDTH = 512.0
N_SEND, N_RECV = 12, 96

ORDER = (
    "V.s0", "px.0", "c.n1", "R1.oa", "c.ld", "R1.ob", "D.s0", "px.1", "V.s1", "U.s0", "V.s2", "c.init",
    "R1.oc", "px.2", "P.s0", "V.s3", "P.s1", "R1.ra", "R1.rb", "V.s4", "R1.nr", "U.s1", "P.s2", "R1.nw",
    "c.gx", "c.gp", "c.sp", "R1.fa", "c.gm", "D.s1", "R1.fb", "R1.fw", "c.gf", "c.cx", "P.s3", "c.fr", "c.cm",
    "U.s2", "c.cp", "c.cf", "c.st", "c.a0", "P.s4", "c.p0", "c.m0", "R2.oa", "U.s3", "c.a1", "c.p1", "D.s2",
    "c.m1", "R2.ob", "R2.ra", "U.s4", "R2.rb", "D.s3", "c.ux", "R2.nr", "R2.nw", "c.up", "c.um", "D.s4",
    "R2.fa", "d.ep", "D.s5", "d.sp", "R2.fb", "d.pl", "R2.fw", "c.uf", "d.ef", "d.sf", "d.fa", "d.la", "d.sl",
    "d.xx", "d.fn",
)


def dot(a, b):
    return jnp.dot(a, b, preferred_element_type=F32)


class Copies:
    def __init__(self, send, recv, peer):
        self.send, self.recv, self.peer = send, recv, peer
        self.sends, self.recvs, self.finals = 0, 0, []

    def take(self, count=1):
        at = self.recvs
        self.recvs += count
        assert self.recvs <= N_RECV
        return at

    def take_send(self, total):
        at = self.sends
        self.sends += 1
        assert self.sends <= N_SEND
        self.finals.append((total, at))
        return at

    def copy(self, src, dst, device, recv, send):
        return pltpu.make_async_remote_copy(
            src_ref=src,
            dst_ref=dst,
            send_sem=self.send.at[send],
            recv_sem=self.recv.at[recv],
            device_id=device,
            device_id_type=MESH,
        )

    def start(self, ref, device, recv, send):
        self.copy(ref, ref, device, recv, send).start()

    def arrived(self, total, recv):
        self.copy(total, total, self.peer, recv, 0).wait_recv()

    def finish(self):
        for total, at in self.finals:
            self.copy(total, total, self.peer, 0, at).wait_send()


def kernel(*refs):
    hbm, out, local, refs = refs[:15], refs[15], refs[16:31], refs[31:]
    x1, x2, vg, pp, uu, dd, glu, cin, cv, st, st_in, act, mix_out, mix_in, mix, mid, hid = refs[:17]
    par_out, par_in, par, rel_in, fin_in, far_in, out_buf, send_sem, recv_sem, load_sem, out_sem = refs[17:]
    resid, gain1, w_value, w_gate, value_scale, gate_scale, taps, conv_gain = local[:8]
    w_point, point_scale, gain2, w_up, up_scale, w_down, down_scale = local[8:]

    fs = lax.axis_index("fs")
    tp = lax.axis_index("tp")
    z, y = fs // 4, fs % 4
    x, c = tp // 2, tp % 2
    xp, xm, xf = (x + 1) % 4, (x + 3) % 4, (x + 2) % 4
    yp, ym = (y + 1) % 4, (y + 3) % 4
    zp, zm = (z + 1) % 4, (z + 3) % 4
    to_xp, to_xm = ({"tp": v * 2 + c} for v in (xp, xm))
    to_pair = {"tp": x * 2 + 1 - c}
    to_yp, to_ym = ({"fs": z * 4 + v} for v in (yp, ym))
    to_zp, to_zm = ({"fs": v * 4 + y} for v in (zp, zm))
    cp = Copies(send_sem, recv_sem, to_pair)

    barrier = pltpu.get_barrier_semaphore()
    for peer in (to_pair, to_xp, to_xm, to_yp, to_ym, to_zp, to_zm):
        pl.semaphore_signal(barrier, inc=1, device_id=peer, device_id_type=MESH)

    loads = [pltpu.make_async_copy(a, b, load_sem.at[i]) for i, (a, b) in enumerate(zip(hbm, local))]
    for i in (2, 3, 8, 9, 0, 1, 13, 14, 11, 4, 5, 6, 7, 10, 12):
        loads[i].start()

    for i in (2, 3, 8, 9):
        loads[i].wait()
    vg[0, z, y] = w_value[...].astype(BF)
    vg[1, z, y] = w_gate[...].astype(BF)
    own_point = pp.at[x // 2, z, y, pl.ds(pl.multiple_of((x % 2) * 256, 256), 256)]
    own_point[...] = (w_point[...] * point_scale[...]).astype(BF)

    def norm_rows(source, gain, target, base, first=0, count=RB // 16):
        def step(i, carry):
            rows = pl.multiple_of(i * 16, 16)
            v = source[pl.ds(rows, 16), :].astype(F32)
            scale = lax.rsqrt(jnp.mean(v * v, axis=-1, keepdims=True) + 1e-06)
            at = pl.multiple_of(base + i * 16, 16)
            target[pl.ds(at, 16), :] = (v * scale * gain[...]).astype(BF)
            return carry

        lax.fori_loop(first, first + count, step, 0)

    class Ring:
        def __init__(self, buf):
            self.buf = buf
            self.sem = {name: cp.take() for name in ("a", "b", "c", "d", "ra", "rb", "near", "far")}
            self.send = cp.take_send(buf.at[0 : 28 * QB])

        def at(self, v, first, count):
            return self.buf.at[pl.ds(pl.multiple_of(v * CB + c * RB + first * QB, 16), count * QB)]

        def both(self, name, up, down):
            for (v, first, count), peer in ((up, to_xp), (down, to_xm)):
                cp.start(self.at(v, first, count), peer, self.sem[name], self.send)

        def share(self, name, *blocks):
            for v, first, count in blocks:
                cp.start(self.at(v, first, count), to_pair, self.sem[name], self.send)

        def arrived(self, name, quarters):
            cp.arrived(self.buf.at[0 : quarters * QB], self.sem[name])

        def oa(self):
            self.both("a", (x, 0, 1), (x, 2, 1))

        def ob(self):
            self.both("b", (x, 1, 1), (x, 3, 1))
            self.share("d", (x, 0, 4))

        def oc(self):
            self.both("c", (x, 2, 2), (x, 0, 2))

        def ra(self):
            self.arrived("a", 2)
            self.both("ra", (xm, 0, 1), (xp, 2, 1))
            self.share("near", (xm, 0, 1), (xp, 2, 1))

        def rb(self):
            self.arrived("b", 2)
            self.both("rb", (xm, 1, 1), (xp, 3, 1))
            self.share("near", (xm, 1, 1), (xp, 3, 1))

        def nr(self):
            self.arrived("c", 4)
            self.share("near", (xm, 2, 2), (xp, 0, 2))

        def nw(self):
            self.arrived("near", 8)

        def fa(self):
            self.arrived("ra", 2)
            self.share("far", (xf, 0, 1), (xf, 2, 1))

        def fb(self):
            self.arrived("rb", 2)
            self.share("far", (xf, 1, 1), (xf, 3, 1))

        def fw(self):
            self.arrived("far", 4)

        def own_wait(self):
            self.arrived("d", 4)

    class LateRing(Ring):
        def __init__(self, buf):
            super().__init__(buf)
            self.rc = cp.take()

        def oa(self):
            self.both("a", (x, 0, 2), (x, 0, 2))

        def ob(self):
            self.both("b", (x, 2, 1), (x, 2, 1))
            self.both("c", (x, 3, 1), (x, 3, 1))
            self.share("d", (x, 0, 4))

        def ra(self):
            self.arrived("a", 4)
            cp.start(self.at(xm, 0, 2), to_xp, self.sem["ra"], self.send)
            self.share("near", (xm, 0, 2), (xp, 0, 2))

        def rb(self):
            self.arrived("b", 2)
            cp.start(self.at(xp, 2, 1), to_xm, self.sem["rb"], self.send)
            self.share("near", (xm, 2, 1), (xp, 2, 1))

        def nr(self):
            self.arrived("c", 2)
            cp.start(self.at(xp, 3, 1), to_xm, self.rc, self.send)
            self.share("near", (xm, 3, 1), (xp, 3, 1))

        def fa(self):
            self.arrived("rb", 1)
            self.share("far", (xf, 2, 1))

        def fb(self):
            self.arrived("ra", 2)
            self.share("far", (xf, 0, 2))
            cp.arrived(self.buf.at[0:QB], self.rc)
            self.share("far", (xf, 3, 1))

    class Weights:
        def __init__(self, buf):
            self.buf, self.deep = buf, buf.shape[3]
            self.sem = [cp.take() for _ in range(6)]
            rows = 30 * buf.shape[3] * buf.shape[4] // D
            self.send = cp.take_send(x1.at[0:rows])

        def four(self, sem, plan):
            for ref, peer in plan:
                cp.start(ref, peer, self.sem[sem], self.send)

        def s0(self):
            half = self.deep // 2
            parts = pl.ds(0, half), pl.ds(half, half)
            for turn in range(2):
                lo, hi = parts[turn], parts[1 - turn]
                plan = (
                    (self.buf.at[0, z, y, lo], to_yp),
                    (self.buf.at[1, z, y, lo], to_zp),
                    (self.buf.at[0, z, y, hi], to_ym),
                    (self.buf.at[1, z, y, hi], to_zm),
                )
                self.four(turn, plan)

        def s1(self):
            half = self.deep // 2
            lo, hi = pl.ds(0, half), pl.ds(half, half)
            plan = (
                (self.buf.at[0, z, ym, lo], to_yp),
                (self.buf.at[1, zm, y, lo], to_zp),
                (self.buf.at[0, z, yp, hi], to_ym),
                (self.buf.at[1, zp, y, hi], to_zm),
            )
            cp.arrived(self.buf.at[0, 0, 0:2], self.sem[0])
            self.four(2, plan)

        def s2(self):
            cp.arrived(self.buf.at[0, 0, 0:2], self.sem[1])
            cp.arrived(self.buf.at[0, 0, 0:2], self.sem[2])
            parts = pl.ds(0, 2), pl.ds(2, 2)
            for turn in range(2):
                lo, hi = parts[turn], parts[1 - turn]
                plan = (
                    (self.buf.at[0, z, lo], to_zp),
                    (self.buf.at[1, lo, y], to_yp),
                    (self.buf.at[0, z, hi], to_zm),
                    (self.buf.at[1, hi, y], to_ym),
                )
                self.four(3 + turn, plan)

        def s3(self):
            lo, hi = pl.ds(0, 2), pl.ds(2, 2)
            plan = (
                (self.buf.at[0, zm, lo], to_zp),
                (self.buf.at[1, lo, ym], to_yp),
                (self.buf.at[0, zp, hi], to_zm),
                (self.buf.at[1, hi, yp], to_ym),
            )
            cp.arrived(self.buf.at[0, 0:2], self.sem[3])
            self.four(5, plan)

        def s4(self):
            cp.arrived(self.buf.at[0, 0:2], self.sem[4])
            cp.arrived(self.buf.at[0, 0:2], self.sem[5])

    ring1, ring2 = Ring(x1), LateRing(x2)
    gv, gp, gu, gd = Weights(vg), Weights(pp), Weights(uu), Weights(dd)

    steps = {}

    def step_named(name):
        def keep(body):
            steps[name] = body
            return body

        return keep

    for name, chain in (("V", gv), ("P", gp), ("U", gu), ("D", gd)):
        for part in ("s0", "s1", "s2", "s3", "s4"):
            steps[name + "." + part] = getattr(chain, part)
    steps["D.s4"] = lambda: cp.arrived(dd.at[0, 0:2], gd.sem[4])
    steps["D.s5"] = lambda: cp.arrived(dd.at[0, 0:2], gd.sem[5])
    steps["R1.oc"] = ring1.oc
    for name, chain in (("R1", ring1), ("R2", ring2)):
        for part in ("oa", "ob", "ra", "rb", "nr", "nw", "fa", "fb", "fw"):
            steps[name + "." + part] = getattr(chain, part)

    point_sem, point_send = [cp.take() for _ in range(2)], cp.take_send(x1.at[0:48])

    def send_point(turn, v, first, count, peer):
        ref = pp.at[v // 2, z, y, pl.ds(pl.multiple_of((v % 2) * 256 + first, 128), count)]
        cp.start(ref, peer, point_sem[turn], point_send)

    @step_named("px.0")
    def _():
        send_point(0, x, 0, 256, to_xp)
        send_point(0, x, 0, 256, to_xm)

    @step_named("px.1")
    def _():
        cp.arrived(pp.at[0, 0, 0], point_sem[0])
        send_point(1, xm, 0, 128, to_xp)
        send_point(1, xp, 128, 128, to_xm)

    steps["px.2"] = lambda: cp.arrived(pp.at[0, 0, 0, 0:256], point_sem[1])

    @step_named("c.ld")
    def _():
        for i in (13, 14, 11):
            loads[i].wait()
        for half in range(2):
            uu[half, z, y] = w_up[:, half * 512 : half * 512 + 512].astype(BF)
            dd[half, z, y] = (w_down[half * 512 : half * 512 + 512, :] * down_scale[...]).astype(BF)

    @step_named("c.n1")
    def _():
        loads[0].wait()
        loads[1].wait()
        norm_rows(resid, gain1, x1, tp * RB)

    @step_named("c.init")
    def _():
        glu[0:HALO, :] = jnp.zeros((HALO, CW), BF)
        glu[HALO + SEQ : HALO + SEQ + HALO, :] = jnp.zeros((HALO, CW), BF)
        st[...] = jnp.zeros(st.shape, F32)
        for i in (4, 5, 6, 7, 10, 12):
            loads[i].wait()

    own_cols = pl.ds(pl.multiple_of(tp * CW, CW), CW)

    def gated(v):
        rows = pl.multiple_of(v * CB, CB)
        block = x1[pl.ds(rows, CB), :]
        value = dot(block, vg[0].reshape(D, CW)) * value_scale[:, own_cols]
        gate = dot(block, vg[1].reshape(D, CW)) * gate_scale[:, own_cols]
        glu[pl.ds(pl.multiple_of(rows + HALO, 16), CB), :] = (value * jax.nn.sigmoid(gate)).astype(BF)

    @step_named("c.gx")
    def _():
        ring1.own_wait()
        gated(x)

    steps["c.gp"] = lambda: gated(xp)

    glu_sem = {name: cp.take() for name in ("gp", "gm", "end", "far", "two")}
    glu_send = cp.take_send(x1.at[0:208])

    def send_glu(name, v, first, count, peer):
        rows = pl.ds(pl.multiple_of(v * CB + first, 16), count)
        cp.copy(glu.at[rows], cin.at[x, pl.ds(first, count)], peer, glu_sem[name], glu_send).start()

    def send_far(first, slot, peer):
        rows = pl.ds(pl.multiple_of(xf * CB + first, 16), FAR)
        cp.copy(glu.at[rows], far_in.at[slot], peer, glu_sem["far"], glu_send).start()

    def glu_arrived(name, rows):
        cp.arrived(glu.at[0:rows], glu_sem[name])

    steps["c.sp"] = lambda: send_glu("gp", xp, 0, CB + HALO, to_xp)

    @step_named("c.gm")
    def _():
        gated(xm)
        send_glu("gm", xm, HALO, CB + HALO, to_xm)

    @step_named("c.gf")
    def _():
        gated(xf)
        send_far(0, 0, to_xp)
        send_far(FAR, 1, to_xm)
        send_glu("end", xp, CB + HALO, HALO, to_xp)
        send_glu("end", xm, 0, HALO, to_xm)

    def convolve(v):
        def step(i, carry):
            part, chunk = i % 2, i // 2
            lane = pl.multiple_of(part * 128, 128)
            row = pl.multiple_of(chunk * 64, 64)
            col = pl.multiple_of((2 * v + c) * CW + part * 128, 128)
            data = cin[v, pl.ds(row, 96), pl.ds(lane, 128)].astype(F32)
            total = jnp.zeros((64, 128), F32)
            for b in range(8):
                turned = data if b == 0 else pltpu.roll(data, 96 - b, 0)
                for a in range(4):
                    k = 8 * a + b
                    if k:
                        tap = taps[k - 1 : k, pl.ds(col, 128)]
                        total = total + tap * turned[8 * a : 8 * a + 64]
            cv[v, pl.ds(row, 64), pl.ds(lane, 128)] = total
            st[0, pl.ds(row, 64), :] += total
            st[1, pl.ds(row, 64), :] += total * total
            return carry

        lax.fori_loop(0, 12, step, 0)

    @step_named("c.cx")
    def _():
        cin[x] = glu[pl.ds(pl.multiple_of(x * CB, CB), CB + 2 * HALO), :]
        convolve(x)

    @step_named("c.fr")
    def _():
        glu_arrived("far", 2 * FAR)
        for slot, v, peer in ((0, xm, to_xp), (1, xp, to_xm)):
            there = cin.at[v, pl.ds(slot * FAR, FAR)]
            cp.copy(far_in.at[slot], there, peer, glu_sem["two"], glu_send).start()

    @step_named("c.cm")
    def _():
        glu_arrived("gp", CB + HALO)
        glu_arrived("end", 2 * HALO)
        convolve(xm)

    @step_named("c.cp")
    def _():
        glu_arrived("gm", CB + HALO)
        convolve(xp)

    @step_named("c.cf")
    def _():
        glu_arrived("two", 2 * FAR)
        convolve(xf)

    st_sem, st_send = cp.take(), cp.take_send(st)

    @step_named("c.st")
    def _():
        for kind in range(2):
            total = st[kind]
            for shift in (4, 8, 16, 32, 64):
                total = total + pltpu.roll(total, shift, 1)
            st[kind] = total
        cp.copy(st, st_in, to_pair, st_sem, st_send).start()

    def activate(i, carry):
        rows = pl.ds(pl.multiple_of((i // 3) * 96 + (i % 3) * 32, 32), 32)
        gmean = (st[0, rows, :] + st_in[0, rows, :]) / GROUP_WIDTH
        gsquare = (st[1, rows, :] + st_in[1, rows, :]) / GROUP_WIDTH
        inv = lax.rsqrt(gsquare - gmean * gmean + 1e-05)
        for v in range(4):
            for part in range(2):
                col = pl.multiple_of((2 * v + c) * CW + part * 128, 128)
                lane = part * 128
                s = (cv[v, rows, lane : lane + 128] - gmean) * inv * conv_gain[:, pl.ds(col, 128)]
                act[rows, v * CW + lane : v * CW + lane + 128] = (s / (1.0 + jnp.exp(-s))).astype(BF)
        return carry

    def activate_half(half):
        lax.fori_loop(3 * half, 3 * half + 3, activate, 0)
        lax.fori_loop(3 * half + 6, 3 * half + 9, activate, 0)

    @step_named("c.a0")
    def _():
        cp.arrived(st, st_sem)
        activate_half(0)

    steps["c.a1"] = lambda: activate_half(1)
    mix_sem, mix_send = cp.take(2), cp.take_send(mix_out)

    def columns(buf, n):
        halves = []
        for half in range(2):
            two = buf[half, n // 2, pl.ds((n % 2) * 2, 2)]
            halves.append(jnp.concatenate([two[0], two[1]], axis=1))
        return jnp.concatenate(halves, axis=0)

    def half_rows(core, half):
        return pl.ds(pl.multiple_of(core * RB + half * 96, 32), 96)

    def point(half):
        def step(n, carry):
            rows = jnp.concatenate([act[half_rows(1 - c, half), :], act[half_rows(c, half), :]], axis=0)
            weight = jnp.concatenate([columns(pp, 2 * n), columns(pp, 2 * n + 1)], axis=1)
            both = dot(rows, weight)
            mix_out[half, n] = both[:96].astype(BF)
            cp.copy(mix_out.at[half, n], mix_in.at[half, n], to_pair, mix_sem + half, mix_send).start()
            mix[half * 96 : half * 96 + 96, pl.ds(pl.multiple_of(n * 512, 512), 512)] = both[96:]
            return carry

        lax.fori_loop(0, 4, step, 0)

    def middle(half):
        def step(n, carry):
            rows = slice(half * 96, half * 96 + 96)
            cols = pl.ds(pl.multiple_of(n * 512, 512), 512)
            mixed = mix[rows, cols] + mix_in[half, n].astype(F32)
            mid[rows, cols] = (resid[rows, cols].astype(F32) + mixed).astype(BF)
            return carry

        cp.arrived(mix_in.at[half], mix_sem + half)
        lax.fori_loop(0, 4, step, 0)
        norm_rows(mid, gain2, x2, tp * RB, 6 * half, 6)

    steps["c.p0"], steps["c.p1"] = (lambda: point(0)), (lambda: point(1))
    steps["c.m0"], steps["c.m1"] = (lambda: middle(0)), (lambda: middle(1))

    def up(v):
        rows = pl.ds(pl.multiple_of(v * CB, CB), CB)

        def step(n, carry):
            weight = uu[n].reshape(D, 512)
            cols = pl.ds(pl.multiple_of(n * 512, 512), 512)
            upper = jnp.maximum(dot(x2[rows, :], weight) * up_scale[:, cols], 0.0)
            hid[rows, cols] = (upper * upper).astype(BF)
            return carry

        lax.fori_loop(0, 2, step, 0)

    @step_named("c.ux")
    def _():
        ring2.own_wait()
        up(x)

    steps["c.up"] = lambda: up(xp)
    steps["c.um"] = lambda: up(xm)
    steps["c.uf"] = lambda: up(xf)

    pair_sem = {"f": cp.take(8), "pl": cp.take(4), "la": cp.take(4), "x": cp.take()}
    relay_sem, end_sem = cp.take(4), cp.take(4)
    pair_send, ring_send = cp.take_send(par_out), cp.take_send(par.at[0:3])

    def place(i):
        dz = (i % 4 + 3 * (i // 4)) % 4
        turn = (dz // 2 + i // 4) % 2
        return ((z + dz) % 4) * 2 + (y // 2 + turn) % 2

    def down(*chunks):
        done = []
        for v, i, _ in chunks:
            pair_rows = pl.ds(pl.multiple_of(v * CB + (1 - c) * RB, RB), RB)
            own_rows = pl.ds(pl.multiple_of(v * CB + c * RB, RB), RB)
            rows = jnp.concatenate([hid[pair_rows, :], hid[own_rows, :]], axis=0)
            done.append(dot(rows, columns(dd, place(i))))
        for (v, i, _), both in zip(chunks, done):
            par_out[v, i] = both[:RB].astype(BF)
            par[v, i] = both[RB:].astype(BF)
        for v, i, sem in chunks:
            cp.copy(par_out.at[v, i], par_in.at[v, i], to_pair, sem, pair_send).start()

    def pair_arrived(sem, count):
        cp.arrived(par_in.at[0, 0:count], sem)

    def add_pair(v, n):
        par[v, n] = (par[v, n].astype(F32) + par_in[v, n].astype(F32)).astype(BF)

    def relay(side, k):
        n = k + 4 * side
        cp.copy(par.at[xf, n], rel_in.at[side, k], to_xm if side else to_xp, relay_sem + k, ring_send).start()

    def plain(side, k):
        n = k + 4 * (1 - side)
        to, peer = (xm, to_xm) if side else (xp, to_xp)
        cp.copy(par.at[to, n], fin_in.at[side, n], peer, end_sem + k, ring_send).start()

    def last(side, k):
        n = k + 4 * side
        to, peer = (xm, to_xm) if side else (xp, to_xp)
        cp.copy(par.at[to, n], fin_in.at[side, n], peer, end_sem + k, ring_send).start()

    def each(count, body):
        def step(i, carry):
            body(i)
            return carry

        lax.fori_loop(0, count, step, 0)

    def relay_chunk(side, k):
        n = side * 4 + k
        pair_arrived(pair_sem["f"] + n, 1)
        add_pair(xf, n)
        relay(side, k)

    def plain_chunk(k):
        pair_arrived(pair_sem["pl"] + k, 2)
        add_pair(xp, k + 4)
        plain(0, k)
        add_pair(xm, k)
        plain(1, k)

    def far_two(k):
        down((xf, k, pair_sem["f"] + k), (xf, k + 4, pair_sem["f"] + k + 4))

    def near_two(k):
        down((xp, k + 4, pair_sem["pl"] + k), (xm, k, pair_sem["pl"] + k))

    steps["d.ep"] = lambda: near_two(0)

    @step_named("d.ef")
    def _():
        far_two(0)
        down((xf, 1, pair_sem["f"] + 1))

    steps["d.sp"] = lambda: plain_chunk(0)

    @step_named("d.sf")
    def _():
        relay_chunk(0, 0)
        relay_chunk(1, 0)
        relay_chunk(0, 1)

    @step_named("d.fa")
    def _():
        down((xf, 5, pair_sem["f"] + 5), (xf, 2, pair_sem["f"] + 2))

        down((xf, 6, pair_sem["f"] + 6), (xf, 3, pair_sem["f"] + 3))
        relay_chunk(1, 1)
        relay_chunk(0, 2)
        down((xf, 7, pair_sem["f"] + 7))
        relay_chunk(1, 2)
        relay_chunk(0, 3)
        relay_chunk(1, 3)

    @step_named("d.pl")
    def _():
        def near_step(k):
            near_two(k)

            @pl.when(k >= 2)
            def _():
                plain_chunk(k - 1)

        each(3, lambda k: near_step(k + 1))
        plain_chunk(3)

    @step_named("d.la")
    def _():
        each(4, lambda k: down((xp, k, pair_sem["la"] + k), (xm, k + 4, pair_sem["la"] + k)))

    @step_named("d.sl")
    def _():
        def send_last(k):
            pair_arrived(pair_sem["la"] + k, 2)
            cp.arrived(rel_in.at[0, 0:2], relay_sem + k)
            for side, v in ((0, xp), (1, xm)):
                n = k + 4 * side
                total = par[v, n].astype(F32) + par_in[v, n].astype(F32) + rel_in[side, k].astype(F32)
                par[v, n] = total.astype(BF)
                last(side, k)

        each(4, send_last)

    @step_named("d.xx")
    def _():
        each(4, lambda k: down((x, k, pair_sem["x"]), (x, k + 4, pair_sem["x"])))
        pair_arrived(pair_sem["x"], 8)

        def own_step(n):
            cols = pl.ds(pl.multiple_of(place(n) * 256, 256), 256)
            mix[:, cols] = mid[:, cols].astype(F32) + (par[x, n].astype(F32) + par_in[x, n].astype(F32))

        each(8, own_step)

    def out_copy(n):
        cols = pl.ds(pl.multiple_of(place(n) * 256, 256), 256)
        return pltpu.make_async_copy(out_buf.at[n], out.at[:, cols], out_sem.at[0])

    def finish(k):
        cp.arrived(fin_in.at[0, 0:4], end_sem + k)
        for n in (k, k + 4):
            cols = pl.ds(pl.multiple_of(place(n) * 256, 256), 256)
            total = fin_in[0, n].astype(F32) + fin_in[1, n].astype(F32)
            out_buf[n] = (mix[:, cols] + total).astype(BF)
            out_copy(n).start()

    steps["d.fn"] = lambda: each(4, finish)
    pl.semaphore_wait(barrier, 7)
    for name in ORDER:
        with jax.named_scope(name):
            steps[name]()
    assert len(ORDER) == len(set(ORDER)) == len(steps)
    cp.finish()
    pltpu.make_async_copy(resid, out, out_sem.at[0]).wait()


SCRATCH = (
    ((SEQ, D), BF),
    ((SEQ, D), BF),
    ((2, 4, 4, 128, 256), BF),
    ((2, 4, 4, 512, 128), BF),
    ((2, 4, 4, 128, 512), BF),
    ((2, 4, 4, 512, 128), BF),
    ((SEQ + 2 * HALO, CW), BF),
    ((4, CB + 2 * HALO, CW), BF),
    ((4, CB, CW), F32),
    ((2, CB, 128), F32),
    ((2, CB, 128), F32),
    ((CB, 4 * CW), BF),
    ((2, 4, 96, 512), BF),
    ((2, 4, 96, 512), BF),
    ((RB, D), F32),
    ((RB, D), BF),
    ((SEQ, 1024), BF),
    ((4, 8, RB, 256), BF),
    ((4, 8, RB, 256), BF),
    ((4, 8, RB, 256), BF),
    ((2, 4, RB, 256), BF),
    ((2, 8, RB, 256), BF),
    ((2, FAR, CW), BF),
    ((8, RB, 256), BF),
)


def shards(*arrays):
    flat = [a.reshape(1, -1) if a.ndim == 1 else a for a in arrays]
    return pl.pallas_call(
        kernel,
        out_shape=jax.ShapeDtypeStruct((RB, D), BF),
        in_specs=[pl.BlockSpec(memory_space=pltpu.HBM)] * len(flat),
        out_specs=pl.BlockSpec(memory_space=pl.ANY),
        scratch_shapes=[pltpu.VMEM(a.shape, a.dtype) for a in flat]
        + [pltpu.VMEM(shape, kind) for shape, kind in SCRATCH]
        + [pltpu.SemaphoreType.DMA((count,)) for count in (N_SEND, N_RECV, len(flat), 1)],
        compiler_params=pltpu.CompilerParams(
            collective_id=0, has_side_effects=True, vmem_limit_bytes=66 * 1000 * 1000
        ),
        name="layer",
    )(*flat)


def solution(mesh):
    in_specs = (
        P(("fs", "tp"), None),
        P(),
        P("fs", "tp"),
        P("fs", "tp"),
        P(),
        P(),
        P(),
        P(),
        P("tp", "fs"),
        P("fs"),
        P(),
        P("fs", "tp"),
        P("tp"),
        P("tp", "fs"),
        P("fs"),
    )
    out_specs = P(("fs", "tp"), None)
    return jax.shard_map(shards, mesh=mesh, in_specs=in_specs, out_specs=out_specs, check_vma=False)
```

```python
import functools

import jax
import jax.numpy as jnp
from jax import lax
from jax.experimental import pallas as pl
from jax.experimental.pallas import tpu as pltpu
from jax.sharding import PartitionSpec as P

BF = jnp.bfloat16
F32 = jnp.float32
MESH = pl.DeviceIdType.MESH

RB = 192
QB = 48
CB = 384
SEQ = 1536
D = 2048
CW = 256
HALO = 16
FAR = 208
KERNEL = 31
GROUP_WIDTH = 512.0
N_SEND, N_RECV = 12, 96

ORDER = (
    "c.ld", "V.s0", "px.0", "U.s0", "c.n1", "R1.oa", "px.1", "V.s1", "D.s0", "R1.ob", "V.s2", "px.2", "P.s0",
    "c.init", "U.s1", "R1.oc", "R1.ra", "R1.rb", "P.s1", "V.s3", "R1.nr", "P.s2", "R1.nw", "R1.fa", "V.s4",
    "c.gx", "c.gp", "c.sp", "c.gm", "R1.fb", "c.g0", "R1.fw", "c.gf", "c.cx", "P.s3", "D.s1", "c.f0", "c.f1",
    "c.f2", "c.cm", "U.s2", "c.cp", "c.cf", "c.a0", "P.s4", "c.p0", "c.a1", "c.m0", "R2.oa", "c.p1", "U.s3",
    "c.m1", "D.s2", "R2.ob", "R2.ra", "U.s4", "c.ux", "R2.rb", "D.s3", "R2.nr", "R2.nw", "c.up", "c.um",
    "R2.fa", "D.s4", "d.ep", "d.sp", "R2.fb", "R2.fw", "c.uf", "d.ef", "d.sf", "D.s5", "d.pl", "d.fa", "d.la",
    "d.sl", "d.xx", "d.fn",
)


CHUNKS = (
    ((0, 0), (0, 1)),
    ((1, 0), (1, 1)),
    ((2, 0), (2, 1)),
    ((2, 2), (2, 3)),
    ((3, 0), (3, 1)),
    ((0, 3), (1, 3)),
    ((0, 2), (1, 2)),
    ((3, 2), (3, 3)),
)


def dot(a, b):
    return jnp.dot(a, b, preferred_element_type=F32)


class Copies:
    def __init__(self, send, recv, peer):
        self.send, self.recv, self.peer = send, recv, peer
        self.sends, self.recvs, self.finals = 0, 0, []

    def take(self, count=1):
        at = self.recvs
        self.recvs += count
        assert self.recvs <= N_RECV
        return at

    def take_send(self, total):
        at = self.sends
        self.sends += 1
        assert self.sends <= N_SEND
        self.finals.append((total, at))
        return at

    def copy(self, src, dst, device, recv, send):
        return pltpu.make_async_remote_copy(
            src_ref=src,
            dst_ref=dst,
            send_sem=self.send.at[send],
            recv_sem=self.recv.at[recv],
            device_id=device,
            device_id_type=MESH,
        )

    def start(self, ref, device, recv, send):
        self.copy(ref, ref, device, recv, send).start()

    def arrived(self, total, recv):
        self.copy(total, total, self.peer, recv, 0).wait_recv()

    def finish(self):
        for total, at in self.finals:
            self.copy(total, total, self.peer, 0, at).wait_send()


def kernel(*refs):
    hbm, out, local, refs = refs[:15], refs[15], refs[16:31], refs[31:]
    x1, x2, vg, pp, uu, dd, glu, cin, cv, st, st_in, act, mix_out, mix_in, mix, mid, hid = refs[:17]
    par_out, par_in, par, rel_in, fin_in, far_in, out_buf, send_sem, recv_sem, load_sem, out_sem = refs[17:]
    resid, gain1, w_value, w_gate, value_scale, gate_scale, taps, conv_gain = local[:8]
    w_point, point_scale, gain2, w_up, up_scale, w_down, down_scale = local[8:]

    fs = lax.axis_index("fs")
    tp = lax.axis_index("tp")
    z, y = fs // 4, fs % 4
    x, c = tp // 2, tp % 2
    xp, xm, xf = (x + 1) % 4, (x + 3) % 4, (x + 2) % 4
    yp, ym = (y + 1) % 4, (y + 3) % 4
    zp, zm = (z + 1) % 4, (z + 3) % 4
    to_xp, to_xm = ({"tp": v * 2 + c} for v in (xp, xm))
    to_pair = {"tp": x * 2 + 1 - c}
    to_yp, to_ym = ({"fs": z * 4 + v} for v in (yp, ym))
    to_zp, to_zm = ({"fs": v * 4 + y} for v in (zp, zm))
    cp = Copies(send_sem, recv_sem, to_pair)

    barrier = pltpu.get_barrier_semaphore()
    for peer in (to_pair, to_xp, to_xm, to_yp, to_ym, to_zp, to_zm):
        pl.semaphore_signal(barrier, inc=1, device_id=peer, device_id_type=MESH)

    loads = [pltpu.make_async_copy(a, b, load_sem.at[i]) for i, (a, b) in enumerate(zip(hbm, local))]
    for i in (2, 3, 8, 9, 0, 1, 13, 14, 11, 4, 5, 6, 7, 10, 12):
        loads[i].start()

    for i in (2, 3, 8, 9):
        loads[i].wait()
    vg[0, z, y] = w_value[...].astype(BF)
    vg[1, z, y] = w_gate[...].astype(BF)
    own_point = pp.at[x // 2, z, y, pl.ds(pl.multiple_of((x % 2) * 256, 256), 256)]
    own_point[...] = (w_point[...] * point_scale[...]).astype(BF)

    def norm_rows(source, gain, target, base):
        def step(i, carry):
            rows = pl.multiple_of(i * 16, 16)
            v = source[pl.ds(rows, 16), :].astype(F32)
            scale = lax.rsqrt(jnp.mean(v * v, axis=-1, keepdims=True) + 1e-06)
            at = pl.multiple_of(base + i * 16, 16)
            target[pl.ds(at, 16), :] = (v * scale * gain[...]).astype(BF)
            return carry

        lax.fori_loop(0, RB // 16, step, 0)

    class Ring:
        def __init__(self, buf):
            self.buf = buf
            self.sem = {name: cp.take() for name in ("a", "b", "c", "d", "ra", "rb", "near", "far")}
            self.send = cp.take_send(buf.at[0 : 28 * QB])

        def at(self, v, first, count):
            return self.buf.at[pl.ds(pl.multiple_of(v * CB + c * RB + first * QB, 16), count * QB)]

        def both(self, name, up, down):
            for (v, first, count), peer in ((up, to_xp), (down, to_xm)):
                cp.start(self.at(v, first, count), peer, self.sem[name], self.send)

        def share(self, name, *blocks):
            for v, first, count in blocks:
                cp.start(self.at(v, first, count), to_pair, self.sem[name], self.send)

        def arrived(self, name, quarters):
            cp.arrived(self.buf.at[0 : quarters * QB], self.sem[name])

        def oa(self):
            self.both("a", (x, 0, 1), (x, 2, 1))

        def ob(self):
            self.both("b", (x, 1, 1), (x, 3, 1))
            self.share("d", (x, 0, 4))

        def oc(self):
            self.both("c", (x, 2, 2), (x, 0, 2))

        def ra(self):
            self.arrived("a", 2)
            self.both("ra", (xm, 0, 1), (xp, 2, 1))
            self.share("near", (xm, 0, 1), (xp, 2, 1))

        def rb(self):
            self.arrived("b", 2)
            self.both("rb", (xm, 1, 1), (xp, 3, 1))
            self.share("near", (xm, 1, 1), (xp, 3, 1))

        def nr(self):
            self.arrived("c", 4)
            self.share("near", (xm, 2, 2), (xp, 0, 2))

        def nw(self):
            self.arrived("near", 8)

        def fa(self):
            self.arrived("ra", 2)
            self.share("far", (xf, 0, 1), (xf, 2, 1))

        def fb(self):
            self.arrived("rb", 2)
            self.share("far", (xf, 1, 1), (xf, 3, 1))

        def fw(self):
            self.arrived("far", 4)

        def own_wait(self):
            self.arrived("d", 4)

    class LateRing(Ring):
        def __init__(self, buf):
            super().__init__(buf)
            self.rc = cp.take()

        def oa(self):
            self.both("a", (x, 0, 2), (x, 0, 2))

        def ob(self):
            self.both("b", (x, 2, 1), (x, 2, 1))
            self.both("c", (x, 3, 1), (x, 3, 1))
            self.share("d", (x, 0, 4))

        def ra(self):
            self.arrived("a", 4)
            cp.start(self.at(xm, 0, 2), to_xp, self.sem["ra"], self.send)
            self.share("near", (xm, 0, 2), (xp, 0, 2))

        def rb(self):
            self.arrived("b", 2)
            cp.start(self.at(xp, 2, 1), to_xm, self.sem["rb"], self.send)
            self.share("near", (xm, 2, 1), (xp, 2, 1))

        def nr(self):
            self.arrived("c", 2)
            cp.start(self.at(xp, 3, 1), to_xm, self.rc, self.send)
            self.share("near", (xm, 3, 1), (xp, 3, 1))

        def fa(self):
            self.arrived("rb", 1)
            self.share("far", (xf, 2, 1))

        def fb(self):
            self.arrived("ra", 2)
            self.share("far", (xf, 0, 2))
            cp.arrived(self.buf.at[0:QB], self.rc)
            self.share("far", (xf, 3, 1))

    class Weights:
        def __init__(self, buf):
            self.buf, self.deep = buf, buf.shape[3]
            self.sem = [cp.take() for _ in range(6)]
            rows = 30 * buf.shape[3] * buf.shape[4] // D
            self.send = cp.take_send(x1.at[0:rows])

        def four(self, sem, plan):
            for ref, peer in plan:
                cp.start(ref, peer, self.sem[sem], self.send)

        def s0(self):
            half = self.deep // 2
            parts = pl.ds(0, half), pl.ds(half, half)
            for turn in range(2):
                lo, hi = parts[turn], parts[1 - turn]
                plan = (
                    (self.buf.at[0, z, y, lo], to_yp),
                    (self.buf.at[1, z, y, lo], to_zp),
                    (self.buf.at[0, z, y, hi], to_ym),
                    (self.buf.at[1, z, y, hi], to_zm),
                )
                self.four(turn, plan)

        def s1(self):
            half = self.deep // 2
            lo, hi = pl.ds(0, half), pl.ds(half, half)
            plan = (
                (self.buf.at[0, z, ym, lo], to_yp),
                (self.buf.at[1, zm, y, lo], to_zp),
                (self.buf.at[0, z, yp, hi], to_ym),
                (self.buf.at[1, zp, y, hi], to_zm),
            )
            cp.arrived(self.buf.at[0, 0, 0:2], self.sem[0])
            self.four(2, plan)

        def s2(self):
            cp.arrived(self.buf.at[0, 0, 0:2], self.sem[1])
            cp.arrived(self.buf.at[0, 0, 0:2], self.sem[2])
            parts = pl.ds(0, 2), pl.ds(2, 2)
            for turn in range(2):
                lo, hi = parts[turn], parts[1 - turn]
                plan = (
                    (self.buf.at[0, z, lo], to_zp),
                    (self.buf.at[1, lo, y], to_yp),
                    (self.buf.at[0, z, hi], to_zm),
                    (self.buf.at[1, hi, y], to_ym),
                )
                self.four(3 + turn, plan)

        def s3(self):
            lo, hi = pl.ds(0, 2), pl.ds(2, 2)
            plan = (
                (self.buf.at[0, zm, lo], to_zp),
                (self.buf.at[1, lo, ym], to_yp),
                (self.buf.at[0, zp, hi], to_zm),
                (self.buf.at[1, hi, yp], to_ym),
            )
            cp.arrived(self.buf.at[0, 0:2], self.sem[3])
            self.four(5, plan)

        def s4(self):
            cp.arrived(self.buf.at[0, 0:2], self.sem[4])
            cp.arrived(self.buf.at[0, 0:2], self.sem[5])

    ring1, ring2 = Ring(x1), LateRing(x2)
    gv, gp, gu, gd = Weights(vg), Weights(pp), Weights(uu), Weights(dd)

    steps = {}

    def step_named(name):
        def keep(body):
            steps[name] = body
            return body

        return keep

    for name, chain in (("V", gv), ("P", gp), ("U", gu), ("D", gd)):
        for part in ("s0", "s1", "s2", "s3", "s4"):
            steps[name + "." + part] = getattr(chain, part)
    steps["D.s4"] = lambda: cp.arrived(dd.at[0, 0:2], gd.sem[4])
    steps["D.s5"] = lambda: cp.arrived(dd.at[0, 0:2], gd.sem[5])
    steps["R1.oc"] = ring1.oc
    for name, chain in (("R1", ring1), ("R2", ring2)):
        for part in ("oa", "ob", "ra", "rb", "nr", "nw", "fa", "fb", "fw"):
            steps[name + "." + part] = getattr(chain, part)

    point_sem, point_send = [cp.take() for _ in range(2)], cp.take_send(x1.at[0:48])

    def send_point(turn, v, first, count, peer):
        ref = pp.at[v // 2, z, y, pl.ds(pl.multiple_of((v % 2) * 256 + first, 128), count)]
        cp.start(ref, peer, point_sem[turn], point_send)

    @step_named("px.0")
    def _():
        send_point(0, x, 0, 256, to_xp)
        send_point(0, x, 0, 256, to_xm)

    @step_named("px.1")
    def _():
        cp.arrived(pp.at[0, 0, 0], point_sem[0])
        send_point(1, xm, 0, 128, to_xp)
        send_point(1, xp, 128, 128, to_xm)

    steps["px.2"] = lambda: cp.arrived(pp.at[0, 0, 0, 0:256], point_sem[1])

    @step_named("c.ld")
    def _():
        for i in (13, 14, 11):
            loads[i].wait()
        for half in range(2):
            uu[half, z, y] = w_up[:, half * 512 : half * 512 + 512].astype(BF)
            dd[half, z, y] = (w_down[half * 512 : half * 512 + 512, :] * down_scale[...]).astype(BF)

    @step_named("c.n1")
    def _():
        loads[0].wait()
        loads[1].wait()
        norm_rows(resid, gain1, x1, tp * RB)

    @step_named("c.init")
    def _():
        glu[0:HALO, :] = jnp.zeros((HALO, CW), BF)
        glu[HALO + SEQ : HALO + SEQ + HALO, :] = jnp.zeros((HALO, CW), BF)
        st[...] = jnp.zeros(st.shape, F32)
        for i in (4, 5, 6, 7, 10, 12):
            loads[i].wait()

    own_cols = pl.ds(pl.multiple_of(tp * CW, CW), CW)

    def gated_rows(first, count):
        rows = pl.multiple_of(first, 64)
        block = x1[pl.ds(rows, count), :]
        value = dot(block, vg[0].reshape(D, CW)) * value_scale[:, own_cols]
        gate = dot(block, vg[1].reshape(D, CW)) * gate_scale[:, own_cols]
        glu[pl.ds(pl.multiple_of(rows + HALO, 16), count), :] = (value * jax.nn.sigmoid(gate)).astype(BF)

    def gated(v):
        gated_rows(v * CB, CB)

    @step_named("c.gx")
    def _():
        ring1.own_wait()
        gated(x)

    steps["c.gp"] = lambda: gated(xp)

    glu_sem = {name: cp.take() for name in ("gp", "gm", "end", "fo", "f1", "f2", "two")}
    glu_send = cp.take_send(x1.at[0:208])

    def send_glu(name, v, first, count, peer):
        rows = pl.ds(pl.multiple_of(v * CB + first, 16), count)
        cp.copy(glu.at[rows], cin.at[x, pl.ds(first, count)], peer, glu_sem[name], glu_send).start()

    def send_far(name, slot, at, count):
        rows = pl.ds(pl.multiple_of(xf * CB + slot * FAR + at, 16), count)
        there = far_in.at[slot, pl.ds(at, count)]
        peer = {"tp": ((x + 1 + 2 * slot) % 4) * 2 + c}
        cp.copy(glu.at[rows], there, peer, glu_sem[name], glu_send).start()

    def relay_far(name, slot, at, count):
        glu_arrived(name, count)
        there = cin.at[(x + 3 + 2 * slot) % 4, pl.ds(pl.multiple_of(slot * FAR + at, 16), count)]
        peer = {"tp": ((x + 1 + 2 * slot) % 4) * 2 + c}
        cp.copy(far_in.at[slot, pl.ds(at, count)], there, peer, glu_sem["two"], glu_send).start()

    def glu_arrived(name, rows):
        cp.arrived(glu.at[0:rows], glu_sem[name])

    steps["c.sp"] = lambda: send_glu("gp", xp, 0, CB + HALO, to_xp)

    @step_named("c.gm")
    def _():
        gated(xm)
        send_glu("gm", xm, HALO, CB + HALO, to_xm)

    @step_named("c.g0")
    def _():
        gated_rows(xf * CB + c * RB, RB)
        send_far("fo", c, 0, FAR)

    @step_named("c.gf")
    def _():
        gated_rows(xf * CB + (1 - c) * RB, RB)
        send_far("f1", 1 - c, 0, 112)
        send_far("f2", 1 - c, 112, 96)
        send_glu("end", xp, CB + HALO, HALO, to_xp)
        send_glu("end", xm, 0, HALO, to_xm)

    def convolve(v, first=0, count=8):
        def step(i, carry):
            part, chunk = i % 2, i // 2
            half, slot = chunk // 2, chunk % 2
            lane = pl.multiple_of(part * 128, 128)
            row = pl.multiple_of(slot * RB + half * 96, 32)
            col = pl.multiple_of((2 * v + c) * CW + part * 128, 128)
            data = cin[v, pl.ds(row, 128), pl.ds(lane, 128)].astype(F32)
            total = jnp.zeros((96, 128), F32)
            for b in range(8):
                turned = data if b == 0 else pltpu.roll(data, 128 - b, 0)
                for a in range(4):
                    k = 8 * a + b
                    if k:
                        tap = taps[k - 1 : k, pl.ds(col, 128)]
                        total = total + tap * turned[8 * a : 8 * a + 96]
            cv[v, pl.ds(row, 96), pl.ds(lane, 128)] = total
            there = pl.ds(pl.multiple_of(slot * 96, 32), 96)
            st[half, 0, there, :] += total
            st[half, 1, there, :] += total * total
            return carry

        lax.fori_loop(first, first + count, step, 0)

    @step_named("c.cx")
    def _():
        cin[x] = glu[pl.ds(pl.multiple_of(x * CB, CB), CB + 2 * HALO), :]
        convolve(x)

    steps["c.f0"] = lambda: relay_far("fo", c, 0, FAR)
    steps["c.f1"] = lambda: relay_far("f1", 1 - c, 0, 112)
    steps["c.f2"] = lambda: relay_far("f2", 1 - c, 112, 96)

    @step_named("c.cm")
    def _():
        glu_arrived("gp", CB + HALO)
        glu_arrived("end", 2 * HALO)
        convolve(xm)

    @step_named("c.cp")
    def _():
        glu_arrived("gm", CB + HALO)
        convolve(xp)

    st_sem, st_send = cp.take(2), cp.take_send(st)

    def finish_stats(half):
        for kind in range(2):
            total = st[half, kind]
            for shift in (4, 8, 16, 32, 64):
                total = total + pltpu.roll(total, shift, 1)
            st[half, kind] = total
        cp.copy(st.at[half], st_in.at[half], to_pair, st_sem + half, st_send).start()

    @step_named("c.cf")
    def _():
        glu_arrived("two", 2 * FAR)
        for half in range(2):
            convolve(xf, 4 * half, 4)
            finish_stats(half)

    def activate(i, carry):
        rows = pl.ds(pl.multiple_of((i // 3) * 96 + (i % 3) * 32, 32), 32)
        half = (i // 3) % 2
        there = pl.ds(pl.multiple_of((i // 6) * 96 + (i % 3) * 32, 32), 32)
        gmean = (st[half, 0, there, :] + st_in[half, 0, there, :]) / GROUP_WIDTH
        gsquare = (st[half, 1, there, :] + st_in[half, 1, there, :]) / GROUP_WIDTH
        inv = lax.rsqrt(gsquare - gmean * gmean + 1e-05)
        for v in range(4):
            for part in range(2):
                col = pl.multiple_of((2 * v + c) * CW + part * 128, 128)
                lane = part * 128
                s = (cv[v, rows, lane : lane + 128] - gmean) * inv * conv_gain[:, pl.ds(col, 128)]
                act[rows, v * CW + lane : v * CW + lane + 128] = (s / (1.0 + jnp.exp(-s))).astype(BF)
        return carry

    def activate_half(half):
        lax.fori_loop(3 * half, 3 * half + 3, activate, 0)
        lax.fori_loop(3 * half + 6, 3 * half + 9, activate, 0)

    @step_named("c.a0")
    def _():
        cp.arrived(st.at[0], st_sem)
        activate_half(0)

    @step_named("c.a1")
    def _():
        cp.arrived(st.at[1], st_sem + 1)
        activate_half(1)

    mix_sem, mix_send = cp.take(2), cp.take_send(mix_out)

    def columns(buf, n):
        halves = []
        for half in range(2):
            two = buf[half, n // 2, pl.ds((n % 2) * 2, 2)]
            halves.append(jnp.concatenate([two[0], two[1]], axis=1))
        return jnp.concatenate(halves, axis=0)

    def half_rows(core, half):
        return pl.ds(pl.multiple_of(core * RB + half * 96, 32), 96)

    def point(half):
        def step(n, carry):
            rows = jnp.concatenate([act[half_rows(1 - c, half), :], act[half_rows(c, half), :]], axis=0)
            weight = jnp.concatenate([columns(pp, 2 * n), columns(pp, 2 * n + 1)], axis=1)
            both = dot(rows, weight)
            mix_out[half, n] = both[:96].astype(BF)
            cp.copy(mix_out.at[half, n], mix_in.at[half, n], to_pair, mix_sem + half, mix_send).start()
            mix[half * 96 : half * 96 + 96, pl.ds(pl.multiple_of(n * 512, 512), 512)] = both[96:]
            return carry

        lax.fori_loop(0, 4, step, 0)

    def middle(half):
        def step(i, carry):
            here = pl.ds(pl.multiple_of(i * 16, 16), 16)
            rows = pl.ds(pl.multiple_of(half * 96 + i * 16, 16), 16)
            mixed = mix[rows, :] + jnp.concatenate([mix_in[half, n, here, :] for n in range(4)], axis=1).astype(F32)
            data = (resid[rows, :].astype(F32) + mixed).astype(BF)
            mid[rows, :] = data
            v = data.astype(F32)
            scale = lax.rsqrt(jnp.mean(v * v, axis=-1, keepdims=True) + 1e-06)
            at = pl.multiple_of(tp * RB + half * 96 + i * 16, 16)
            x2[pl.ds(at, 16), :] = (v * scale * gain2[...]).astype(BF)
            return carry

        cp.arrived(mix_in.at[half], mix_sem + half)
        lax.fori_loop(0, 6, step, 0)

    steps["c.p0"], steps["c.p1"] = (lambda: point(0)), (lambda: point(1))
    steps["c.m0"], steps["c.m1"] = (lambda: middle(0)), (lambda: middle(1))

    def up(v):
        rows = pl.ds(pl.multiple_of(v * CB, CB), CB)

        def step(n, carry):
            weight = uu[n].reshape(D, 512)
            cols = pl.ds(pl.multiple_of(n * 512, 512), 512)
            upper = jnp.maximum(dot(x2[rows, :], weight) * up_scale[:, cols], 0.0)
            hid[rows, cols] = (upper * upper).astype(BF)
            return carry

        lax.fori_loop(0, 2, step, 0)

    @step_named("c.ux")
    def _():
        ring2.own_wait()
        up(x)

    steps["c.up"] = lambda: up(xp)
    steps["c.um"] = lambda: up(xm)
    steps["c.uf"] = lambda: up(xf)

    pair_sem = {"f": cp.take(8), "pl": cp.take(8), "la": cp.take(4), "x": cp.take()}
    relay_sem, end_sem = cp.take(4), cp.take(4)
    pair_send, ring_send = cp.take_send(par_out), cp.take_send(par.at[0:3])

    def blocks(i):
        return [((z + dz) % 4, (y + dy) % 4) for dz, dy in CHUNKS[i]]

    def block_columns(owner):
        return pl.ds(pl.multiple_of((owner[0] * 4 + owner[1]) * 128, 128), 128)

    def down_columns(i):
        (za, ya), (zb, yb) = blocks(i)
        halves = [jnp.concatenate([dd[half, za, ya], dd[half, zb, yb]], axis=1) for half in range(2)]
        return jnp.concatenate(halves, axis=0)

    def down(*chunks):
        done = []
        for v, i, _ in chunks:
            pair_rows = pl.ds(pl.multiple_of(v * CB + (1 - c) * RB, RB), RB)
            own_rows = pl.ds(pl.multiple_of(v * CB + c * RB, RB), RB)
            rows = jnp.concatenate([hid[pair_rows, :], hid[own_rows, :]], axis=0)
            done.append(dot(rows, down_columns(i)))
        for (v, i, _), both in zip(chunks, done):
            par_out[v, i] = both[:RB].astype(BF)
            par[v, i] = both[RB:].astype(BF)
        for v, i, sem in chunks:
            cp.copy(par_out.at[v, i], par_in.at[v, i], to_pair, sem, pair_send).start()

    def pair_arrived(sem, count):
        cp.arrived(par_in.at[0, 0:count], sem)

    def add_pair(v, n):
        par[v, n] = (par[v, n].astype(F32) + par_in[v, n].astype(F32)).astype(BF)

    def relay(side, k):
        n = k + 4 * side
        cp.copy(par.at[xf, n], rel_in.at[side, k], to_xm if side else to_xp, relay_sem + k, ring_send).start()

    def plain(side, k):
        n = k + 4 * (1 - side)
        to, peer = (xm, to_xm) if side else (xp, to_xp)
        cp.copy(par.at[to, n], fin_in.at[side, n], peer, end_sem + k, ring_send).start()

    def last(side, k):
        n = k + 4 * side
        to, peer = (xm, to_xm) if side else (xp, to_xp)
        cp.copy(par.at[to, n], fin_in.at[side, n], peer, end_sem + k, ring_send).start()

    def each(count, body):
        for i in range(count):
            body(i)

    def relay_chunk(side, k):
        n = side * 4 + k
        pair_arrived(pair_sem["f"] + n, 1)
        add_pair(xf, n)
        relay(side, k)

    def plain_chunk(side, k):
        pair_arrived(pair_sem["pl"] + 4 * side + k, 1)
        add_pair(xm if side else xp, k if side else k + 4)
        plain(side, k)

    def far(i):
        return xf, i, pair_sem["f"] + i

    def near(side, k):
        return xm if side else xp, k if side else k + 4, pair_sem["pl"] + 4 * side + k

    @step_named("d.ep")
    def _():
        down(near(0, 0), near(1, 0))
        down(near(0, 1), near(1, 1))

    @step_named("d.ef")
    def _():
        down(far(0), far(4))
        down(far(1), far(5))

    @step_named("d.sp")
    def _():
        for k in range(2):
            for side in range(2):
                plain_chunk(side, k)

    @step_named("d.sf")
    def _():
        for k in range(2):
            for side in range(2):
                relay_chunk(side, k)

    @step_named("d.fa")
    def _():
        down(far(2), far(6))
        down(far(3), far(7))
        for k in range(2, 4):
            for side in range(2):
                relay_chunk(side, k)

    @step_named("d.pl")
    def _():
        down(near(0, 2), near(1, 2))
        down(near(0, 3), near(1, 3))
        for k in range(2, 4):
            for side in range(2):
                plain_chunk(side, k)

    @step_named("d.la")
    def _():
        each(4, lambda k: down((xp, k, pair_sem["la"] + k), (xm, k + 4, pair_sem["la"] + k)))

    @step_named("d.sl")
    def _():
        def send_last(k):
            pair_arrived(pair_sem["la"] + k, 2)
            cp.arrived(rel_in.at[0, 0:2], relay_sem + k)
            for side, v in ((0, xp), (1, xm)):
                n = k + 4 * side
                total = par[v, n].astype(F32) + par_in[v, n].astype(F32) + rel_in[side, k].astype(F32)
                par[v, n] = total.astype(BF)
                last(side, k)

        each(4, send_last)

    @step_named("d.xx")
    def _():
        each(4, lambda k: down((x, k, pair_sem["x"]), (x, k + 4, pair_sem["x"])))
        pair_arrived(pair_sem["x"], 8)

        def own_step(i):
            for part, owner in enumerate(blocks(i)):
                lane, cols = slice(part * 128, part * 128 + 128), block_columns(owner)
                own = par[x, i, :, lane].astype(F32) + par_in[x, i, :, lane].astype(F32)
                mix[:, cols] = mid[:, cols].astype(F32) + own

        each(8, own_step)

    def finish(k):
        cp.arrived(fin_in.at[0, 0:4], end_sem + k)
        for i in (k, k + 4):
            total = fin_in[0, i].astype(F32) + fin_in[1, i].astype(F32)
            for part, owner in enumerate(blocks(i)):
                lane, cols = slice(part * 128, part * 128 + 128), block_columns(owner)
                out_buf[i, part] = (mix[:, cols] + total[:, lane]).astype(BF)
                pltpu.make_async_copy(out_buf.at[i, part], out.at[:, cols], out_sem.at[0]).start()

    steps["d.fn"] = lambda: each(4, finish)
    pl.semaphore_wait(barrier, 7)
    for name in ORDER:
        with jax.named_scope(name):
            steps[name]()
    assert len(ORDER) == len(set(ORDER)) == len(steps)
    cp.finish()
    pltpu.make_async_copy(resid, out, out_sem.at[0]).wait()


SCRATCH = (
    ((SEQ, D), BF),
    ((SEQ, D), BF),
    ((2, 4, 4, 128, 256), BF),
    ((2, 4, 4, 512, 128), BF),
    ((2, 4, 4, 128, 512), BF),
    ((2, 4, 4, 512, 128), BF),
    ((SEQ + 2 * HALO, CW), BF),
    ((4, CB + 2 * HALO, CW), BF),
    ((4, CB, CW), F32),
    ((2, 2, RB, 128), F32),
    ((2, 2, RB, 128), F32),
    ((CB, 4 * CW), BF),
    ((2, 4, 96, 512), BF),
    ((2, 4, 96, 512), BF),
    ((RB, D), F32),
    ((RB, D), BF),
    ((SEQ, 1024), BF),
    ((4, 8, RB, 256), BF),
    ((4, 8, RB, 256), BF),
    ((4, 8, RB, 256), BF),
    ((2, 4, RB, 256), BF),
    ((2, 8, RB, 256), BF),
    ((2, FAR, CW), BF),
    ((8, 2, RB, 128), BF),
)


def shards(*arrays):
    flat = [a.reshape(1, -1) if a.ndim == 1 else a for a in arrays]
    return pl.pallas_call(
        kernel,
        out_shape=jax.ShapeDtypeStruct((RB, D), BF),
        in_specs=[pl.BlockSpec(memory_space=pltpu.HBM)] * len(flat),
        out_specs=pl.BlockSpec(memory_space=pl.ANY),
        scratch_shapes=[pltpu.VMEM(a.shape, a.dtype) for a in flat]
        + [pltpu.VMEM(shape, kind) for shape, kind in SCRATCH]
        + [pltpu.SemaphoreType.DMA((count,)) for count in (N_SEND, N_RECV, len(flat), 1)],
        compiler_params=pltpu.CompilerParams(
            collective_id=0, has_side_effects=True, vmem_limit_bytes=66 * 1000 * 1000
        ),
        name="layer",
    )(*flat)


def solution(mesh):
    in_specs = (
        P(("fs", "tp"), None),
        P(),
        P("fs", "tp"),
        P("fs", "tp"),
        P(),
        P(),
        P(),
        P(),
        P("tp", "fs"),
        P("fs"),
        P(),
        P("fs", "tp"),
        P("tp"),
        P("tp", "fs"),
        P("fs"),
    )
    out_specs = P(("fs", "tp"), None)
    return jax.shard_map(shards, mesh=mesh, in_specs=in_specs, out_specs=out_specs, check_vma=False)
```

```python
import functools

import jax
import jax.numpy as jnp
from jax import lax
from jax.experimental import pallas as pl
from jax.experimental.pallas import tpu as pltpu
from jax.sharding import PartitionSpec as P

BF = jnp.bfloat16
F32 = jnp.float32
MESH = pl.DeviceIdType.MESH

RB = 192
QB = 48
CB = 384
SEQ = 1536
D = 2048
CW = 256
HALO = 16
FAR = 208
KERNEL = 31
GROUP_WIDTH = 512.0
N_SEND, N_RECV = 12, 96

ORDER = (
    "c.ld", "V.s0", "px.0", "U.s0", "D.s0", "c.n1", "R1.oa", "px.1", "V.s1", "U.s1", "R1.ob", "R1.oc", "D.s1",
    "px.2", "P.s0", "V.s2", "c.init", "R1.ra", "R1.rb", "P.s1", "V.s3", "R1.nr", "P.s2", "R1.nw", "V.s4",
    "c.gx", "c.gp", "c.sp", "R1.fa", "c.gm", "R1.fb", "c.g0", "R1.fw", "c.gf", "c.cx", "P.s3", "c.f0", "c.f1",
    "c.f2", "c.cm", "U.s2", "c.cp", "c.cf", "c.a0", "P.s4", "c.p0", "c.a1", "c.m0", "R2.oa", "c.p1", "U.s3",
    "c.m1", "D.s2", "R2.ob", "R2.ra", "U.s4", "c.ux", "R2.rb", "R2.nr", "D.s3", "R2.nw", "c.up", "c.um",
    "R2.fa", "D.s4", "d.e0", "d.e1", "d.s0", "d.s1", "R2.fb", "c.u0", "R2.fw", "c.uf", "d.ef", "d.sf", "D.s5",
    "d.pl", "d.fa", "d.la", "d.sl", "d.xx", "d.fn",
)


CHUNKS = (
    ((0, 0), (0, 1)),
    ((1, 0), (1, 1)),
    ((2, 0), (2, 1)),
    ((2, 2), (2, 3)),
    ((3, 0), (3, 1)),
    ((0, 3), (1, 3)),
    ((0, 2), (1, 2)),
    ((3, 2), (3, 3)),
)


def dot(a, b):
    return jnp.dot(a, b, preferred_element_type=F32)


class Copies:
    def __init__(self, send, recv, peer):
        self.send, self.recv, self.peer = send, recv, peer
        self.sends, self.recvs, self.finals = 0, 0, []

    def take(self, count=1):
        at = self.recvs
        self.recvs += count
        assert self.recvs <= N_RECV
        return at

    def take_send(self, total):
        at = self.sends
        self.sends += 1
        assert self.sends <= N_SEND
        self.finals.append((total, at))
        return at

    def copy(self, src, dst, device, recv, send):
        return pltpu.make_async_remote_copy(
            src_ref=src,
            dst_ref=dst,
            send_sem=self.send.at[send],
            recv_sem=self.recv.at[recv],
            device_id=device,
            device_id_type=MESH,
        )

    def start(self, ref, device, recv, send):
        self.copy(ref, ref, device, recv, send).start()

    def arrived(self, total, recv):
        self.copy(total, total, self.peer, recv, 0).wait_recv()

    def finish(self):
        for total, at in self.finals:
            self.copy(total, total, self.peer, 0, at).wait_send()


def kernel(*refs):
    hbm, out, local, refs = refs[:15], refs[15], refs[16:31], refs[31:]
    x1, x2, vg, pp, uu, dd, glu, cin, cv, st, st_in, act, mix_out, mix_in, mix, mid, hid = refs[:17]
    par_out, par_in, par, rel_in, fin_in, far_in, out_buf, send_sem, recv_sem, load_sem, out_sem = refs[17:]
    resid, gain1, w_value, w_gate, value_scale, gate_scale, taps, conv_gain = local[:8]
    w_point, point_scale, gain2, w_up, up_scale, w_down, down_scale = local[8:]

    fs = lax.axis_index("fs")
    tp = lax.axis_index("tp")
    z, y = fs // 4, fs % 4
    x, c = tp // 2, tp % 2
    xp, xm, xf = (x + 1) % 4, (x + 3) % 4, (x + 2) % 4
    yp, ym = (y + 1) % 4, (y + 3) % 4
    zp, zm = (z + 1) % 4, (z + 3) % 4
    to_xp, to_xm = ({"tp": v * 2 + c} for v in (xp, xm))
    to_pair = {"tp": x * 2 + 1 - c}
    to_yp, to_ym = ({"fs": z * 4 + v} for v in (yp, ym))
    to_zp, to_zm = ({"fs": v * 4 + y} for v in (zp, zm))
    cp = Copies(send_sem, recv_sem, to_pair)

    barrier = pltpu.get_barrier_semaphore()
    for peer in (to_pair, to_xp, to_xm, to_yp, to_ym, to_zp, to_zm):
        pl.semaphore_signal(barrier, inc=1, device_id=peer, device_id_type=MESH)

    loads = [pltpu.make_async_copy(a, b, load_sem.at[i]) for i, (a, b) in enumerate(zip(hbm, local))]
    for i in (2, 3, 8, 9, 0, 1, 13, 14, 11, 4, 5, 6, 7, 10, 12):
        loads[i].start()

    for i in (2, 3, 8, 9):
        loads[i].wait()
    vg[0, z, y] = w_value[...].astype(BF)
    vg[1, z, y] = w_gate[...].astype(BF)
    own_point = pp.at[x // 2, z, y, pl.ds(pl.multiple_of((x % 2) * 256, 256), 256)]
    own_point[...] = (w_point[...] * point_scale[...]).astype(BF)

    def norm_rows(source, gain, target, base):
        def step(i, carry):
            rows = pl.multiple_of(i * 16, 16)
            v = source[pl.ds(rows, 16), :].astype(F32)
            scale = lax.rsqrt(jnp.mean(v * v, axis=-1, keepdims=True) + 1e-06)
            at = pl.multiple_of(base + i * 16, 16)
            target[pl.ds(at, 16), :] = (v * scale * gain[...]).astype(BF)
            return carry

        lax.fori_loop(0, RB // 16, step, 0)

    class Ring:
        def __init__(self, buf):
            self.buf = buf
            self.sem = {name: cp.take() for name in ("a", "b", "c", "d", "ra", "rb", "near", "far")}
            self.send = cp.take_send(buf.at[0 : 28 * QB])

        def at(self, v, first, count):
            return self.buf.at[pl.ds(pl.multiple_of(v * CB + c * RB + first * QB, 16), count * QB)]

        def both(self, name, up, down):
            for (v, first, count), peer in ((up, to_xp), (down, to_xm)):
                cp.start(self.at(v, first, count), peer, self.sem[name], self.send)

        def share(self, name, *blocks):
            for v, first, count in blocks:
                cp.start(self.at(v, first, count), to_pair, self.sem[name], self.send)

        def arrived(self, name, quarters):
            cp.arrived(self.buf.at[0 : quarters * QB], self.sem[name])

        def oa(self):
            self.both("a", (x, 0, 1), (x, 2, 1))

        def ob(self):
            self.both("b", (x, 1, 1), (x, 3, 1))
            self.share("d", (x, 0, 4))

        def oc(self):
            self.both("c", (x, 2, 2), (x, 0, 2))

        def ra(self):
            self.arrived("a", 2)
            self.both("ra", (xm, 0, 1), (xp, 2, 1))
            self.share("near", (xm, 0, 1), (xp, 2, 1))

        def rb(self):
            self.arrived("b", 2)
            self.both("rb", (xm, 1, 1), (xp, 3, 1))
            self.share("near", (xm, 1, 1), (xp, 3, 1))

        def nr(self):
            self.arrived("c", 4)
            self.share("near", (xm, 2, 2), (xp, 0, 2))

        def nw(self):
            self.arrived("near", 8)

        def fa(self):
            self.arrived("ra", 2)
            self.share("far", (xf, 0, 1), (xf, 2, 1))

        def fb(self):
            self.arrived("rb", 2)
            self.share("far", (xf, 1, 1), (xf, 3, 1))

        def fw(self):
            self.arrived("far", 4)

        def own_wait(self):
            self.arrived("d", 4)

    class LateRing(Ring):
        def __init__(self, buf):
            super().__init__(buf)
            self.rc = cp.take()

        def oa(self):
            self.both("a", (x, 0, 2), (x, 0, 2))

        def ob(self):
            self.both("b", (x, 2, 1), (x, 2, 1))
            self.both("c", (x, 3, 1), (x, 3, 1))
            self.share("d", (x, 0, 4))

        def ra(self):
            self.arrived("a", 4)
            cp.start(self.at(xm, 0, 2), to_xp, self.sem["ra"], self.send)
            self.share("near", (xm, 0, 2), (xp, 0, 2))

        def rb(self):
            self.arrived("b", 2)
            cp.start(self.at(xp, 2, 1), to_xm, self.sem["rb"], self.send)
            self.share("near", (xm, 2, 1), (xp, 2, 1))

        def nr(self):
            self.arrived("c", 2)
            cp.start(self.at(xp, 3, 1), to_xm, self.rc, self.send)
            self.share("near", (xm, 3, 1), (xp, 3, 1))

        def fa(self):
            self.arrived("rb", 1)
            self.share("far", (xf, 2, 1))

        def fb(self):
            self.arrived("ra", 2)
            self.share("far", (xf, 0, 2))
            cp.arrived(self.buf.at[0:QB], self.rc)
            self.share("far", (xf, 3, 1))

    class Weights:
        def __init__(self, buf):
            self.buf, self.deep = buf, buf.shape[3]
            self.sem = [cp.take() for _ in range(6)]
            rows = 30 * buf.shape[3] * buf.shape[4] // D
            self.send = cp.take_send(x1.at[0:rows])

        def four(self, sem, plan):
            for ref, peer in plan:
                cp.start(ref, peer, self.sem[sem], self.send)

        def s0(self):
            half = self.deep // 2
            parts = pl.ds(0, half), pl.ds(half, half)
            for turn in range(2):
                lo, hi = parts[turn], parts[1 - turn]
                plan = (
                    (self.buf.at[0, z, y, lo], to_yp),
                    (self.buf.at[1, z, y, lo], to_zp),
                    (self.buf.at[0, z, y, hi], to_ym),
                    (self.buf.at[1, z, y, hi], to_zm),
                )
                self.four(turn, plan)

        def s1(self):
            half = self.deep // 2
            lo, hi = pl.ds(0, half), pl.ds(half, half)
            plan = (
                (self.buf.at[0, z, ym, lo], to_yp),
                (self.buf.at[1, zm, y, lo], to_zp),
                (self.buf.at[0, z, yp, hi], to_ym),
                (self.buf.at[1, zp, y, hi], to_zm),
            )
            cp.arrived(self.buf.at[0, 0, 0:2], self.sem[0])
            self.four(2, plan)

        def s2(self):
            cp.arrived(self.buf.at[0, 0, 0:2], self.sem[1])
            cp.arrived(self.buf.at[0, 0, 0:2], self.sem[2])
            parts = pl.ds(0, 2), pl.ds(2, 2)
            for turn in range(2):
                lo, hi = parts[turn], parts[1 - turn]
                plan = (
                    (self.buf.at[0, z, lo], to_zp),
                    (self.buf.at[1, lo, y], to_yp),
                    (self.buf.at[0, z, hi], to_zm),
                    (self.buf.at[1, hi, y], to_ym),
                )
                self.four(3 + turn, plan)

        def s3(self):
            lo, hi = pl.ds(0, 2), pl.ds(2, 2)
            plan = (
                (self.buf.at[0, zm, lo], to_zp),
                (self.buf.at[1, lo, ym], to_yp),
                (self.buf.at[0, zp, hi], to_zm),
                (self.buf.at[1, hi, yp], to_ym),
            )
            cp.arrived(self.buf.at[0, 0:2], self.sem[3])
            self.four(5, plan)

        def s4(self):
            cp.arrived(self.buf.at[0, 0:2], self.sem[4])
            cp.arrived(self.buf.at[0, 0:2], self.sem[5])

    ring1, ring2 = Ring(x1), LateRing(x2)
    gv, gp, gu, gd = Weights(vg), Weights(pp), Weights(uu), Weights(dd)

    steps = {}

    def step_named(name):
        def keep(body):
            steps[name] = body
            return body

        return keep

    for name, chain in (("V", gv), ("P", gp), ("U", gu), ("D", gd)):
        for part in ("s0", "s1", "s2", "s3", "s4"):
            steps[name + "." + part] = getattr(chain, part)
    steps["D.s4"] = lambda: cp.arrived(dd.at[0, 0:2], gd.sem[4])
    steps["D.s5"] = lambda: cp.arrived(dd.at[0, 0:2], gd.sem[5])
    steps["R1.oc"] = ring1.oc
    for name, chain in (("R1", ring1), ("R2", ring2)):
        for part in ("oa", "ob", "ra", "rb", "nr", "nw", "fa", "fb", "fw"):
            steps[name + "." + part] = getattr(chain, part)

    point_sem, point_send = [cp.take() for _ in range(2)], cp.take_send(x1.at[0:48])

    def send_point(turn, v, first, count, peer):
        ref = pp.at[v // 2, z, y, pl.ds(pl.multiple_of((v % 2) * 256 + first, 128), count)]
        cp.start(ref, peer, point_sem[turn], point_send)

    @step_named("px.0")
    def _():
        send_point(0, x, 0, 256, to_xp)
        send_point(0, x, 0, 256, to_xm)

    @step_named("px.1")
    def _():
        cp.arrived(pp.at[0, 0, 0], point_sem[0])
        send_point(1, xm, 0, 128, to_xp)
        send_point(1, xp, 128, 128, to_xm)

    steps["px.2"] = lambda: cp.arrived(pp.at[0, 0, 0, 0:256], point_sem[1])

    @step_named("c.ld")
    def _():
        for i in (13, 14, 11):
            loads[i].wait()
        for half in range(2):
            uu[half, z, y] = w_up[:, half * 512 : half * 512 + 512].astype(BF)
            dd[half, z, y] = (w_down[half * 512 : half * 512 + 512, :] * down_scale[...]).astype(BF)

    @step_named("c.n1")
    def _():
        loads[0].wait()
        loads[1].wait()
        norm_rows(resid, gain1, x1, tp * RB)

    @step_named("c.init")
    def _():
        glu[0:HALO, :] = jnp.zeros((HALO, CW), BF)
        glu[HALO + SEQ : HALO + SEQ + HALO, :] = jnp.zeros((HALO, CW), BF)
        st[...] = jnp.zeros(st.shape, F32)
        for i in (4, 5, 6, 7, 10, 12):
            loads[i].wait()

    own_cols = pl.ds(pl.multiple_of(tp * CW, CW), CW)

    def gated_rows(first, count):
        rows = pl.multiple_of(first, 64)
        block = x1[pl.ds(rows, count), :]
        value = dot(block, vg[0].reshape(D, CW)) * value_scale[:, own_cols]
        gate = dot(block, vg[1].reshape(D, CW)) * gate_scale[:, own_cols]
        glu[pl.ds(pl.multiple_of(rows + HALO, 16), count), :] = (value * jax.nn.sigmoid(gate)).astype(BF)

    def gated(v):
        gated_rows(v * CB, CB)

    @step_named("c.gx")
    def _():
        ring1.own_wait()
        gated(x)

    steps["c.gp"] = lambda: gated(xp)

    glu_sem = {name: cp.take() for name in ("gp", "gm", "end", "fo", "f1", "f2", "two")}
    glu_send = cp.take_send(x1.at[0:208])

    def send_glu(name, v, first, count, peer):
        rows = pl.ds(pl.multiple_of(v * CB + first, 16), count)
        cp.copy(glu.at[rows], cin.at[x, pl.ds(first, count)], peer, glu_sem[name], glu_send).start()

    def send_far(name, slot, at, count):
        rows = pl.ds(pl.multiple_of(xf * CB + slot * FAR + at, 16), count)
        there = far_in.at[slot, pl.ds(at, count)]
        peer = {"tp": ((x + 1 + 2 * slot) % 4) * 2 + c}
        cp.copy(glu.at[rows], there, peer, glu_sem[name], glu_send).start()

    def relay_far(name, slot, at, count):
        glu_arrived(name, count)
        there = cin.at[(x + 3 + 2 * slot) % 4, pl.ds(pl.multiple_of(slot * FAR + at, 16), count)]
        peer = {"tp": ((x + 1 + 2 * slot) % 4) * 2 + c}
        cp.copy(far_in.at[slot, pl.ds(at, count)], there, peer, glu_sem["two"], glu_send).start()

    def glu_arrived(name, rows):
        cp.arrived(glu.at[0:rows], glu_sem[name])

    steps["c.sp"] = lambda: send_glu("gp", xp, 0, CB + HALO, to_xp)

    @step_named("c.gm")
    def _():
        gated(xm)
        send_glu("gm", xm, HALO, CB + HALO, to_xm)

    @step_named("c.g0")
    def _():
        gated_rows(xf * CB + c * RB, RB)
        send_far("fo", c, 0, FAR)

    @step_named("c.gf")
    def _():
        gated_rows(xf * CB + (1 - c) * RB, RB)
        send_far("f1", 1 - c, 0, 112)
        send_far("f2", 1 - c, 112, 96)
        send_glu("end", xp, CB + HALO, HALO, to_xp)
        send_glu("end", xm, 0, HALO, to_xm)

    def convolve(v, first=0, count=8):
        def step(i, carry):
            part, chunk = i % 2, i // 2
            half, slot = chunk // 2, chunk % 2
            lane = pl.multiple_of(part * 128, 128)
            row = pl.multiple_of(slot * RB + half * 96, 32)
            col = pl.multiple_of((2 * v + c) * CW + part * 128, 128)
            data = cin[v, pl.ds(row, 128), pl.ds(lane, 128)].astype(F32)
            total = jnp.zeros((96, 128), F32)
            for b in range(8):
                turned = data if b == 0 else pltpu.roll(data, 128 - b, 0)
                for a in range(4):
                    k = 8 * a + b
                    if k:
                        tap = taps[k - 1 : k, pl.ds(col, 128)]
                        total = total + tap * turned[8 * a : 8 * a + 96]
            cv[v, pl.ds(row, 96), pl.ds(lane, 128)] = total
            there = pl.ds(pl.multiple_of(slot * 96, 32), 96)
            st[half, 0, there, :] += total
            st[half, 1, there, :] += total * total
            return carry

        lax.fori_loop(first, first + count, step, 0)

    @step_named("c.cx")
    def _():
        cin[x] = glu[pl.ds(pl.multiple_of(x * CB, CB), CB + 2 * HALO), :]
        convolve(x)

    steps["c.f0"] = lambda: relay_far("fo", c, 0, FAR)
    steps["c.f1"] = lambda: relay_far("f1", 1 - c, 0, 112)
    steps["c.f2"] = lambda: relay_far("f2", 1 - c, 112, 96)

    @step_named("c.cm")
    def _():
        glu_arrived("gp", CB + HALO)
        glu_arrived("end", 2 * HALO)
        convolve(xm)

    @step_named("c.cp")
    def _():
        glu_arrived("gm", CB + HALO)
        convolve(xp)

    st_sem, st_send = cp.take(2), cp.take_send(st)

    def finish_stats(half):
        for kind in range(2):
            total = st[half, kind]
            for shift in (4, 8, 16, 32, 64):
                total = total + pltpu.roll(total, shift, 1)
            st[half, kind] = total
        cp.copy(st.at[half], st_in.at[half], to_pair, st_sem + half, st_send).start()

    @step_named("c.cf")
    def _():
        glu_arrived("two", 2 * FAR)
        for half in range(2):
            convolve(xf, 4 * half, 4)
            finish_stats(half)

    def activate(i, carry):
        rows = pl.ds(pl.multiple_of((i // 3) * 96 + (i % 3) * 32, 32), 32)
        half = (i // 3) % 2
        there = pl.ds(pl.multiple_of((i // 6) * 96 + (i % 3) * 32, 32), 32)
        gmean = (st[half, 0, there, :] + st_in[half, 0, there, :]) / GROUP_WIDTH
        gsquare = (st[half, 1, there, :] + st_in[half, 1, there, :]) / GROUP_WIDTH
        inv = lax.rsqrt(gsquare - gmean * gmean + 1e-05)
        for v in range(4):
            for part in range(2):
                col = pl.multiple_of((2 * v + c) * CW + part * 128, 128)
                lane = part * 128
                s = (cv[v, rows, lane : lane + 128] - gmean) * inv * conv_gain[:, pl.ds(col, 128)]
                act[rows, v * CW + lane : v * CW + lane + 128] = (s / (1.0 + jnp.exp(-s))).astype(BF)
        return carry

    def activate_half(half):
        lax.fori_loop(3 * half, 3 * half + 3, activate, 0)
        lax.fori_loop(3 * half + 6, 3 * half + 9, activate, 0)

    @step_named("c.a0")
    def _():
        cp.arrived(st.at[0], st_sem)
        activate_half(0)

    @step_named("c.a1")
    def _():
        cp.arrived(st.at[1], st_sem + 1)
        activate_half(1)

    mix_sem, mix_send = cp.take(2), cp.take_send(mix_out)

    def columns(buf, n):
        halves = []
        for half in range(2):
            two = buf[half, n // 2, pl.ds((n % 2) * 2, 2)]
            halves.append(jnp.concatenate([two[0], two[1]], axis=1))
        return jnp.concatenate(halves, axis=0)

    def half_rows(core, half):
        return pl.ds(pl.multiple_of(core * RB + half * 96, 32), 96)

    def point(half):
        def step(n, carry):
            rows = jnp.concatenate([act[half_rows(1 - c, half), :], act[half_rows(c, half), :]], axis=0)
            weight = jnp.concatenate([columns(pp, 2 * n), columns(pp, 2 * n + 1)], axis=1)
            both = dot(rows, weight)
            mix_out[half, n] = both[:96].astype(BF)
            cp.copy(mix_out.at[half, n], mix_in.at[half, n], to_pair, mix_sem + half, mix_send).start()
            mix[half * 96 : half * 96 + 96, pl.ds(pl.multiple_of(n * 512, 512), 512)] = both[96:]
            return carry

        for n in range(4):
            step(n, 0)

    def middle(half):
        def step(i, carry):
            here = pl.ds(pl.multiple_of(i * 16, 16), 16)
            rows = pl.ds(pl.multiple_of(half * 96 + i * 16, 16), 16)
            mixed = mix[rows, :] + jnp.concatenate([mix_in[half, n, here, :] for n in range(4)], axis=1).astype(F32)
            data = (resid[rows, :].astype(F32) + mixed).astype(BF)
            mid[rows, :] = data
            v = data.astype(F32)
            scale = lax.rsqrt(jnp.mean(v * v, axis=-1, keepdims=True) + 1e-06)
            at = pl.multiple_of(tp * RB + half * 96 + i * 16, 16)
            x2[pl.ds(at, 16), :] = (v * scale * gain2[...]).astype(BF)
            return carry

        cp.arrived(mix_in.at[half], mix_sem + half)
        lax.fori_loop(0, 6, step, 0)

    steps["c.p0"], steps["c.p1"] = (lambda: point(0)), (lambda: point(1))
    steps["c.m0"], steps["c.m1"] = (lambda: middle(0)), (lambda: middle(1))

    def up(v):
        up_rows(v * CB, CB)

    def up_rows(first, count):
        rows = pl.ds(pl.multiple_of(first, 64), count)

        def step(n, carry):
            weight = uu[n].reshape(D, 512)
            cols = pl.ds(pl.multiple_of(n * 512, 512), 512)
            upper = jnp.maximum(dot(x2[rows, :], weight) * up_scale[:, cols], 0.0)
            hid[rows, cols] = (upper * upper).astype(BF)
            return carry

        for n in range(2):
            step(n, 0)

    @step_named("c.ux")
    def _():
        ring2.own_wait()
        up(x)

    steps["c.up"] = lambda: up(xp)
    steps["c.um"] = lambda: up(xm)
    steps["c.u0"] = lambda: up_rows(xf * CB + c * RB, RB)
    steps["c.uf"] = lambda: up_rows(xf * CB + (1 - c) * RB, RB)

    pair_sem = {"f": cp.take(8), "pl": cp.take(8), "la": cp.take(4), "x": cp.take()}
    relay_sem, end_sem = cp.take(4), cp.take(4)
    pair_send, ring_send = cp.take_send(par_out), cp.take_send(par.at[0:3])

    def blocks(i):
        return [((z + dz) % 4, (y + dy) % 4) for dz, dy in CHUNKS[i]]

    def block_columns(owner):
        return pl.ds(pl.multiple_of((owner[0] * 4 + owner[1]) * 128, 128), 128)

    def down_columns(i):
        (za, ya), (zb, yb) = blocks(i)
        halves = [jnp.concatenate([dd[half, za, ya], dd[half, zb, yb]], axis=1) for half in range(2)]
        return jnp.concatenate(halves, axis=0)

    def down(*chunks):
        done = []
        for v, i, _ in chunks:
            pair_rows = pl.ds(pl.multiple_of(v * CB + (1 - c) * RB, RB), RB)
            own_rows = pl.ds(pl.multiple_of(v * CB + c * RB, RB), RB)
            rows = jnp.concatenate([hid[pair_rows, :], hid[own_rows, :]], axis=0)
            done.append(dot(rows, down_columns(i)))
        for (v, i, _), both in zip(chunks, done):
            par_out[v, i] = both[:RB].astype(BF)
            par[v, i] = both[RB:].astype(BF)
        for v, i, sem in chunks:
            cp.copy(par_out.at[v, i], par_in.at[v, i], to_pair, sem, pair_send).start()

    def pair_arrived(sem, count):
        cp.arrived(par_in.at[0, 0:count], sem)

    def add_pair(v, n):
        par[v, n] = (par[v, n].astype(F32) + par_in[v, n].astype(F32)).astype(BF)

    def relay(side, k):
        n = k + 4 * side
        cp.copy(par.at[xf, n], rel_in.at[side, k], to_xm if side else to_xp, relay_sem + k, ring_send).start()

    def plain(side, k):
        n = k + 4 * (1 - side)
        to, peer = (xm, to_xm) if side else (xp, to_xp)
        cp.copy(par.at[to, n], fin_in.at[side, n], peer, end_sem + k, ring_send).start()

    def last(side, k):
        n = k + 4 * side
        to, peer = (xm, to_xm) if side else (xp, to_xp)
        cp.copy(par.at[to, n], fin_in.at[side, n], peer, end_sem + k, ring_send).start()

    def each(count, body):
        for i in range(count):
            body(i)

    def relay_chunk(side, k):
        n = side * 4 + k
        pair_arrived(pair_sem["f"] + n, 1)
        add_pair(xf, n)
        relay(side, k)

    def plain_chunk(side, k):
        pair_arrived(pair_sem["pl"] + 4 * side + k, 1)
        add_pair(xm if side else xp, k if side else k + 4)
        plain(side, k)

    def far(i):
        return xf, i, pair_sem["f"] + i

    def near(side, k):
        return xm if side else xp, k if side else k + 4, pair_sem["pl"] + 4 * side + k

    for side in range(2):
        steps[f"d.e{side}"] = lambda side=side: down(near(side, 0), near(side, 1))

    @step_named("d.ef")
    def _():
        down(far(0), far(4))
        down(far(1), far(5))

    def send_plain(side):
        plain_chunk(side, 0)
        plain_chunk(side, 1)

    for side in range(2):
        steps[f"d.s{side}"] = lambda side=side: send_plain(side)

    @step_named("d.sf")
    def _():
        for k in range(2):
            for side in range(2):
                relay_chunk(side, k)

    @step_named("d.fa")
    def _():
        down(far(2), far(6))
        down(far(3), far(7))
        for k in range(2, 4):
            for side in range(2):
                relay_chunk(side, k)

    @step_named("d.pl")
    def _():
        down(near(0, 2), near(1, 2))
        down(near(0, 3), near(1, 3))
        for k in range(2, 4):
            for side in range(2):
                plain_chunk(side, k)

    @step_named("d.la")
    def _():
        each(4, lambda k: down((xp, k, pair_sem["la"] + k), (xm, k + 4, pair_sem["la"] + k)))

    @step_named("d.sl")
    def _():
        def send_last(k):
            pair_arrived(pair_sem["la"] + k, 2)
            cp.arrived(rel_in.at[0, 0:2], relay_sem + k)
            for side, v in ((0, xp), (1, xm)):
                n = k + 4 * side
                total = par[v, n].astype(F32) + par_in[v, n].astype(F32) + rel_in[side, k].astype(F32)
                par[v, n] = total.astype(BF)
                last(side, k)

        each(4, send_last)

    @step_named("d.xx")
    def _():
        each(4, lambda k: down((x, k, pair_sem["x"]), (x, k + 4, pair_sem["x"])))
        pair_arrived(pair_sem["x"], 8)

        def own_step(i):
            for part, owner in enumerate(blocks(i)):
                lane, cols = slice(part * 128, part * 128 + 128), block_columns(owner)
                own = par[x, i, :, lane].astype(F32) + par_in[x, i, :, lane].astype(F32)
                mix[:, cols] = mid[:, cols].astype(F32) + own

        each(8, own_step)

    def finish(k):
        cp.arrived(fin_in.at[0, 0:4], end_sem + k)
        for i in (k, k + 4):
            total = fin_in[0, i].astype(F32) + fin_in[1, i].astype(F32)
            for part, owner in enumerate(blocks(i)):
                lane, cols = slice(part * 128, part * 128 + 128), block_columns(owner)
                out_buf[i, part] = (mix[:, cols] + total[:, lane]).astype(BF)
                pltpu.make_async_copy(out_buf.at[i, part], out.at[:, cols], out_sem.at[0]).start()

    steps["d.fn"] = lambda: each(4, finish)
    pl.semaphore_wait(barrier, 7)
    for name in ORDER:
        with jax.named_scope(name):
            steps[name]()
    assert len(ORDER) == len(set(ORDER)) == len(steps)
    cp.finish()
    pltpu.make_async_copy(resid, out, out_sem.at[0]).wait()


SCRATCH = (
    ((SEQ, D), BF),
    ((SEQ, D), BF),
    ((2, 4, 4, 128, 256), BF),
    ((2, 4, 4, 512, 128), BF),
    ((2, 4, 4, 128, 512), BF),
    ((2, 4, 4, 512, 128), BF),
    ((SEQ + 2 * HALO, CW), BF),
    ((4, CB + 2 * HALO, CW), BF),
    ((4, CB, CW), F32),
    ((2, 2, RB, 128), F32),
    ((2, 2, RB, 128), F32),
    ((CB, 4 * CW), BF),
    ((2, 4, 96, 512), BF),
    ((2, 4, 96, 512), BF),
    ((RB, D), F32),
    ((RB, D), BF),
    ((SEQ, 1024), BF),
    ((4, 8, RB, 256), BF),
    ((4, 8, RB, 256), BF),
    ((4, 8, RB, 256), BF),
    ((2, 4, RB, 256), BF),
    ((2, 8, RB, 256), BF),
    ((2, FAR, CW), BF),
    ((8, 2, RB, 128), BF),
)


def shards(*arrays):
    flat = [a.reshape(1, -1) if a.ndim == 1 else a for a in arrays]
    return pl.pallas_call(
        kernel,
        out_shape=jax.ShapeDtypeStruct((RB, D), BF),
        in_specs=[pl.BlockSpec(memory_space=pltpu.HBM)] * len(flat),
        out_specs=pl.BlockSpec(memory_space=pl.ANY),
        scratch_shapes=[pltpu.VMEM(a.shape, a.dtype) for a in flat]
        + [pltpu.VMEM(shape, kind) for shape, kind in SCRATCH]
        + [pltpu.SemaphoreType.DMA((count,)) for count in (N_SEND, N_RECV, len(flat), 1)],
        compiler_params=pltpu.CompilerParams(
            collective_id=0, has_side_effects=True, vmem_limit_bytes=66 * 1000 * 1000
        ),
        name="layer",
    )(*flat)


def solution(mesh):
    in_specs = (
        P(("fs", "tp"), None),
        P(),
        P("fs", "tp"),
        P("fs", "tp"),
        P(),
        P(),
        P(),
        P(),
        P("tp", "fs"),
        P("fs"),
        P(),
        P("fs", "tp"),
        P("tp"),
        P("tp", "fs"),
        P("fs"),
    )
    out_specs = P(("fs", "tp"), None)
    return jax.shard_map(shards, mesh=mesh, in_specs=in_specs, out_specs=out_specs, check_vma=False)
```

```python
import functools

import jax
import jax.numpy as jnp
from jax import lax
from jax.experimental import pallas as pl
from jax.experimental.pallas import tpu as pltpu
from jax.sharding import PartitionSpec as P

BF = jnp.bfloat16
F32 = jnp.float32
MESH = pl.DeviceIdType.MESH

RB = 192
QB = 48
CB = 384
SEQ = 1536
D = 2048
CW = 256
HALO = 16
FAR = 208
KERNEL = 31
GROUP_WIDTH = 512.0
N_SEND, N_RECV = 12, 77

ORDER = (
    "c.ld", "V.s0", "px.0", "U.s0", "D.s0", "c.n1", "R1.oa", "px.1", "R1.ob", "R1.oc", "V.s1", "U.s1", "D.s1",
    "px.2", "P.s0", "V.s2", "c.init", "R1.ra", "R1.rb", "P.s1", "V.s3", "R1.nr", "P.s2", "R1.nw", "V.s4",
    "c.gx", "c.gp", "c.sp", "R1.fa", "c.gm", "R1.fb", "c.g0", "R1.fw", "c.gf", "c.cx", "P.s3", "c.f0", "c.f1",
    "c.f2", "c.cm", "U.s2", "c.cp", "c.cf", "c.a0", "P.s4", "c.p0", "c.a1", "c.m0", "R2.oa", "c.p1", "U.s3",
    "c.m1", "D.s2", "R2.ob", "R2.ra", "U.s4", "c.ux", "R2.rb", "R2.nr", "D.s3", "R2.nw", "c.up", "c.um",
    "R2.fa", "D.s4", "d.e0", "d.e1", "d.s0", "d.s1", "R2.fb", "c.u0", "R2.fw", "c.uf", "d.ef", "d.sf", "D.s5",
    "d.pl", "d.fa", "d.la", "d.sl", "d.xx", "d.fn",
)


CHUNKS = (
    ((0, 0), (0, 1)),
    ((1, 0), (1, 1)),
    ((2, 0), (2, 1)),
    ((2, 2), (2, 3)),
    ((3, 0), (3, 1)),
    ((0, 3), (1, 3)),
    ((0, 2), (1, 2)),
    ((3, 2), (3, 3)),
)


def dot(a, b):
    return jnp.dot(a, b, preferred_element_type=F32)


class Copies:
    def __init__(self, send, recv, peer):
        self.send, self.recv, self.peer = send, recv, peer
        self.sends, self.recvs, self.finals = 0, 0, []

    def take(self, count=1):
        at = self.recvs
        self.recvs += count
        assert self.recvs <= N_RECV
        return at

    def take_send(self, total):
        at = self.sends
        self.sends += 1
        assert self.sends <= N_SEND
        self.finals.append((total, at))
        return at

    def copy(self, src, dst, device, recv, send):
        return pltpu.make_async_remote_copy(
            src_ref=src,
            dst_ref=dst,
            send_sem=self.send.at[send],
            recv_sem=self.recv.at[recv],
            device_id=device,
            device_id_type=MESH,
        )

    def start(self, ref, device, recv, send):
        self.copy(ref, ref, device, recv, send).start()

    def arrived(self, total, recv):
        self.copy(total, total, self.peer, recv, 0).wait_recv()

    def finish(self):
        for total, at in self.finals:
            self.copy(total, total, self.peer, 0, at).wait_send()


def kernel(*refs):
    hbm, out, local, refs = refs[:15], refs[15], refs[16:31], refs[31:]
    x1, x2, vg, pp, uu, dd, glu, cin, cv, st, st_in, act, mix_out, mix_in, mix, mid, hid = refs[:17]
    par_out, par_in, par, rel_in, fin_in, far_in, out_buf, send_sem, recv_sem, load_sem, out_sem = refs[17:]
    resid, gain1, w_value, w_gate, value_scale, gate_scale, taps, conv_gain = local[:8]
    w_point, point_scale, gain2, w_up, up_scale, w_down, down_scale = local[8:]

    fs = lax.axis_index("fs")
    tp = lax.axis_index("tp")
    z, y = fs // 4, fs % 4
    x, c = tp // 2, tp % 2
    xp, xm, xf = (x + 1) % 4, (x + 3) % 4, (x + 2) % 4
    yp, ym = (y + 1) % 4, (y + 3) % 4
    zp, zm = (z + 1) % 4, (z + 3) % 4
    to_xp, to_xm = ({"tp": v * 2 + c} for v in (xp, xm))
    to_pair = {"tp": x * 2 + 1 - c}
    to_yp, to_ym = ({"fs": z * 4 + v} for v in (yp, ym))
    to_zp, to_zm = ({"fs": v * 4 + y} for v in (zp, zm))
    cp = Copies(send_sem, recv_sem, to_pair)

    barrier = pltpu.get_barrier_semaphore()
    for peer in (to_pair, to_xp, to_xm, to_yp, to_ym, to_zp, to_zm):
        pl.semaphore_signal(barrier, inc=1, device_id=peer, device_id_type=MESH)

    loads = [pltpu.make_async_copy(a, b, load_sem.at[i]) for i, (a, b) in enumerate(zip(hbm, local))]
    for i in (2, 3, 8, 9, 0, 1, 13, 14, 11, 4, 5, 6, 7, 10, 12):
        loads[i].start()

    for i in (2, 3, 8, 9):
        loads[i].wait()
    vg[0, z, y] = w_value[...].astype(BF)
    vg[1, z, y] = w_gate[...].astype(BF)
    own_point = pp.at[x // 2, z, y, pl.ds(pl.multiple_of((x % 2) * 256, 256), 256)]
    own_point[...] = (w_point[...] * point_scale[...]).astype(BF)

    def norm_rows(source, gain, target, base):
        def step(i, carry):
            rows = pl.multiple_of(i * 16, 16)
            v = source[pl.ds(rows, 16), :].astype(F32)
            scale = lax.rsqrt(jnp.mean(v * v, axis=-1, keepdims=True) + 1e-06)
            at = pl.multiple_of(base + i * 16, 16)
            target[pl.ds(at, 16), :] = (v * scale * gain[...]).astype(BF)
            return carry

        lax.fori_loop(0, RB // 16, step, 0)

    class Ring:
        def __init__(self, buf):
            self.buf = buf
            self.sem = {name: cp.take() for name in ("a", "b", "c", "d", "ra", "rb", "near", "far")}
            self.send = cp.take_send(buf.at[0 : 28 * QB])

        def at(self, v, first, count):
            return self.buf.at[pl.ds(pl.multiple_of(v * CB + c * RB + first * QB, 16), count * QB)]

        def both(self, name, up, down):
            for (v, first, count), peer in ((up, to_xp), (down, to_xm)):
                cp.start(self.at(v, first, count), peer, self.sem[name], self.send)

        def share(self, name, *blocks):
            for v, first, count in blocks:
                cp.start(self.at(v, first, count), to_pair, self.sem[name], self.send)

        def arrived(self, name, quarters):
            cp.arrived(self.buf.at[0 : quarters * QB], self.sem[name])

        def oa(self):
            self.both("a", (x, 0, 1), (x, 2, 1))

        def ob(self):
            self.both("b", (x, 1, 1), (x, 3, 1))
            self.share("d", (x, 0, 4))

        def oc(self):
            self.both("c", (x, 2, 2), (x, 0, 2))

        def ra(self):
            self.arrived("a", 2)
            self.both("ra", (xm, 0, 1), (xp, 2, 1))
            self.share("near", (xm, 0, 1), (xp, 2, 1))

        def rb(self):
            self.arrived("b", 2)
            self.both("rb", (xm, 1, 1), (xp, 3, 1))
            self.share("near", (xm, 1, 1), (xp, 3, 1))

        def nr(self):
            self.arrived("c", 4)
            self.share("near", (xm, 2, 2), (xp, 0, 2))

        def nw(self):
            self.arrived("near", 8)

        def fa(self):
            self.arrived("ra", 2)
            self.share("far", (xf, 0, 1), (xf, 2, 1))

        def fb(self):
            self.arrived("rb", 2)
            self.share("far", (xf, 1, 1), (xf, 3, 1))

        def fw(self):
            self.arrived("far", 4)

        def own_wait(self):
            self.arrived("d", 4)

    class LateRing(Ring):
        def __init__(self, buf):
            super().__init__(buf)
            self.rc = cp.take()

        def oa(self):
            self.both("a", (x, 0, 2), (x, 0, 2))

        def ob(self):
            self.both("b", (x, 2, 1), (x, 2, 1))
            self.both("c", (x, 3, 1), (x, 3, 1))
            self.share("d", (x, 0, 4))

        def ra(self):
            self.arrived("a", 4)
            cp.start(self.at(xm, 0, 2), to_xp, self.sem["ra"], self.send)
            self.share("near", (xm, 0, 2), (xp, 0, 2))

        def rb(self):
            self.arrived("b", 2)
            cp.start(self.at(xp, 2, 1), to_xm, self.sem["rb"], self.send)
            self.share("near", (xm, 2, 1), (xp, 2, 1))

        def nr(self):
            self.arrived("c", 2)
            cp.start(self.at(xp, 3, 1), to_xm, self.rc, self.send)
            self.share("near", (xm, 3, 1), (xp, 3, 1))

        def fa(self):
            self.arrived("rb", 1)
            self.share("far", (xf, 2, 1))

        def fb(self):
            self.arrived("ra", 2)
            self.share("far", (xf, 0, 2))
            cp.arrived(self.buf.at[0:QB], self.rc)
            self.share("far", (xf, 3, 1))

    class Weights:
        def __init__(self, buf, apart=0):
            self.buf, self.deep, self.apart = buf, buf.shape[3], apart
            self.sem = [cp.take() for _ in range(4 + apart)]
            rows = 30 * buf.shape[3] * buf.shape[4] // D
            self.send = cp.take_send(x1.at[0:rows])

        def four(self, sem, plan):
            for ref, peer in plan:
                cp.start(ref, peer, self.sem[sem], self.send)

        def s0(self):
            half = self.deep // 2
            parts = pl.ds(0, half), pl.ds(half, half)
            for turn in range(2):
                lo, hi = parts[turn], parts[1 - turn]
                plan = (
                    (self.buf.at[0, z, y, lo], to_yp),
                    (self.buf.at[1, z, y, lo], to_zp),
                    (self.buf.at[0, z, y, hi], to_ym),
                    (self.buf.at[1, z, y, hi], to_zm),
                )
                self.four(turn, plan)

        def s1(self):
            half = self.deep // 2
            lo, hi = pl.ds(0, half), pl.ds(half, half)
            plan = (
                (self.buf.at[0, z, ym, lo], to_yp),
                (self.buf.at[1, zm, y, lo], to_zp),
                (self.buf.at[0, z, yp, hi], to_ym),
                (self.buf.at[1, zp, y, hi], to_zm),
            )
            cp.arrived(self.buf.at[0, 0, 0:2], self.sem[0])
            self.four(1, plan)

        def s2(self):
            cp.arrived(self.buf.at[0, 0], self.sem[1])
            parts = pl.ds(0, 2), pl.ds(2, 2)
            for turn in range(2):
                lo, hi = parts[turn], parts[1 - turn]
                plan = (
                    (self.buf.at[0, z, lo], to_zp),
                    (self.buf.at[1, lo, y], to_yp),
                    (self.buf.at[0, z, hi], to_zm),
                    (self.buf.at[1, hi, y], to_ym),
                )
                self.four(2 + turn, plan)

        def s3(self):
            lo, hi = pl.ds(0, 2), pl.ds(2, 2)
            plan = (
                (self.buf.at[0, zm, lo], to_zp),
                (self.buf.at[1, lo, ym], to_yp),
                (self.buf.at[0, zp, hi], to_zm),
                (self.buf.at[1, hi, yp], to_ym),
            )
            cp.arrived(self.buf.at[0, 0:2], self.sem[2])
            self.four(3 + self.apart, plan)

        def s4(self):
            cp.arrived(self.buf.at[0], self.sem[3])

    ring1, ring2 = Ring(x1), LateRing(x2)
    gv, gp, gu, gd = Weights(vg), Weights(pp), Weights(uu), Weights(dd, 1)

    steps = {}

    def step_named(name):
        def keep(body):
            steps[name] = body
            return body

        return keep

    for name, chain in (("V", gv), ("P", gp), ("U", gu), ("D", gd)):
        for part in ("s0", "s1", "s2", "s3", "s4"):
            steps[name + "." + part] = getattr(chain, part)
    steps["D.s4"] = lambda: cp.arrived(dd.at[0, 0:2], gd.sem[3])
    steps["D.s5"] = lambda: cp.arrived(dd.at[0, 0:2], gd.sem[4])
    steps["R1.oc"] = ring1.oc
    for name, chain in (("R1", ring1), ("R2", ring2)):
        for part in ("oa", "ob", "ra", "rb", "nr", "nw", "fa", "fb", "fw"):
            steps[name + "." + part] = getattr(chain, part)

    point_sem, point_send = [cp.take() for _ in range(2)], cp.take_send(x1.at[0:48])

    def send_point(turn, v, first, count, peer):
        ref = pp.at[v // 2, z, y, pl.ds(pl.multiple_of((v % 2) * 256 + first, 128), count)]
        cp.start(ref, peer, point_sem[turn], point_send)

    @step_named("px.0")
    def _():
        send_point(0, x, 0, 256, to_xp)
        send_point(0, x, 0, 256, to_xm)

    @step_named("px.1")
    def _():
        cp.arrived(pp.at[0, 0, 0], point_sem[0])
        send_point(1, xm, 0, 128, to_xp)
        send_point(1, xp, 128, 128, to_xm)

    steps["px.2"] = lambda: cp.arrived(pp.at[0, 0, 0, 0:256], point_sem[1])

    @step_named("c.ld")
    def _():
        for i in (13, 14, 11):
            loads[i].wait()
        for half in range(2):
            uu[half, z, y] = w_up[:, half * 512 : half * 512 + 512].astype(BF)
            dd[half, z, y] = (w_down[half * 512 : half * 512 + 512, :] * down_scale[...]).astype(BF)

    @step_named("c.n1")
    def _():
        loads[0].wait()
        loads[1].wait()
        norm_rows(resid, gain1, x1, tp * RB)

    @step_named("c.init")
    def _():
        glu[0:HALO, :] = jnp.zeros((HALO, CW), BF)
        glu[HALO + SEQ : HALO + SEQ + HALO, :] = jnp.zeros((HALO, CW), BF)
        st[...] = jnp.zeros(st.shape, F32)
        for i in (4, 5, 6, 7, 10, 12):
            loads[i].wait()

    own_cols = pl.ds(pl.multiple_of(tp * CW, CW), CW)

    def gated_rows(first, count):
        rows = pl.multiple_of(first, 64)
        block = x1[pl.ds(rows, count), :]
        value = dot(block, vg[0].reshape(D, CW)) * value_scale[:, own_cols]
        gate = dot(block, vg[1].reshape(D, CW)) * gate_scale[:, own_cols]
        glu[pl.ds(pl.multiple_of(rows + HALO, 16), count), :] = (value * jax.nn.sigmoid(gate)).astype(BF)

    def gated(v):
        gated_rows(v * CB, CB)

    @step_named("c.gx")
    def _():
        ring1.own_wait()
        gated(x)

    steps["c.gp"] = lambda: gated(xp)

    glu_sem = {name: cp.take() for name in ("gp", "gm", "end", "fo", "f1", "f2", "two")}
    glu_send = cp.take_send(x1.at[0:208])

    def send_glu(name, v, first, count, peer):
        rows = pl.ds(pl.multiple_of(v * CB + first, 16), count)
        cp.copy(glu.at[rows], cin.at[x, pl.ds(first, count)], peer, glu_sem[name], glu_send).start()

    def send_far(name, slot, at, count):
        rows = pl.ds(pl.multiple_of(xf * CB + slot * FAR + at, 16), count)
        there = far_in.at[slot, pl.ds(at, count)]
        peer = {"tp": ((x + 1 + 2 * slot) % 4) * 2 + c}
        cp.copy(glu.at[rows], there, peer, glu_sem[name], glu_send).start()

    def relay_far(name, slot, at, count):
        glu_arrived(name, count)
        there = cin.at[(x + 3 + 2 * slot) % 4, pl.ds(pl.multiple_of(slot * FAR + at, 16), count)]
        peer = {"tp": ((x + 1 + 2 * slot) % 4) * 2 + c}
        cp.copy(far_in.at[slot, pl.ds(at, count)], there, peer, glu_sem["two"], glu_send).start()

    def glu_arrived(name, rows):
        cp.arrived(glu.at[0:rows], glu_sem[name])

    steps["c.sp"] = lambda: send_glu("gp", xp, 0, CB + HALO, to_xp)

    @step_named("c.gm")
    def _():
        gated(xm)
        send_glu("gm", xm, HALO, CB + HALO, to_xm)

    @step_named("c.g0")
    def _():
        gated_rows(xf * CB + c * RB, RB)
        send_far("fo", c, 0, FAR)

    @step_named("c.gf")
    def _():
        gated_rows(xf * CB + (1 - c) * RB, RB)
        send_far("f1", 1 - c, 0, 112)
        send_far("f2", 1 - c, 112, 96)
        send_glu("end", xp, CB + HALO, HALO, to_xp)
        send_glu("end", xm, 0, HALO, to_xm)

    def convolve(v, first=0, count=8):
        def step(i, carry):
            part, chunk = i % 2, i // 2
            half, slot = chunk // 2, chunk % 2
            lane = pl.multiple_of(part * 128, 128)
            row = pl.multiple_of(slot * RB + half * 96, 32)
            col = pl.multiple_of((2 * v + c) * CW + part * 128, 128)
            data = cin[v, pl.ds(row, 128), pl.ds(lane, 128)].astype(F32)
            total = jnp.zeros((96, 128), F32)
            for b in range(8):
                turned = data if b == 0 else pltpu.roll(data, 128 - b, 0)
                for a in range(4):
                    k = 8 * a + b
                    if k:
                        tap = taps[k - 1 : k, pl.ds(col, 128)]
                        total = total + tap * turned[8 * a : 8 * a + 96]
            cv[v, pl.ds(row, 96), pl.ds(lane, 128)] = total
            there = pl.ds(pl.multiple_of(slot * 96, 32), 96)
            st[half, 0, there, :] += total
            st[half, 1, there, :] += total * total
            return carry

        lax.fori_loop(first, first + count, step, 0)

    @step_named("c.cx")
    def _():
        cin[x] = glu[pl.ds(pl.multiple_of(x * CB, CB), CB + 2 * HALO), :]
        convolve(x)

    steps["c.f0"] = lambda: relay_far("fo", c, 0, FAR)
    steps["c.f1"] = lambda: relay_far("f1", 1 - c, 0, 112)
    steps["c.f2"] = lambda: relay_far("f2", 1 - c, 112, 96)

    @step_named("c.cm")
    def _():
        glu_arrived("gp", CB + HALO)
        glu_arrived("end", 2 * HALO)
        convolve(xm)

    @step_named("c.cp")
    def _():
        glu_arrived("gm", CB + HALO)
        convolve(xp)

    st_sem, st_send = cp.take(2), cp.take_send(st)

    def finish_stats(half):
        for kind in range(2):
            total = st[half, kind]
            for shift in (4, 8, 16, 32, 64):
                total = total + pltpu.roll(total, shift, 1)
            st[half, kind] = total
        cp.copy(st.at[half], st_in.at[half], to_pair, st_sem + half, st_send).start()

    @step_named("c.cf")
    def _():
        glu_arrived("two", 2 * FAR)
        for half in range(2):
            convolve(xf, 4 * half, 4)
            finish_stats(half)

    def activate(i, carry):
        rows = pl.ds(pl.multiple_of((i // 3) * 96 + (i % 3) * 32, 32), 32)
        half = (i // 3) % 2
        there = pl.ds(pl.multiple_of((i // 6) * 96 + (i % 3) * 32, 32), 32)
        gmean = (st[half, 0, there, :] + st_in[half, 0, there, :]) / GROUP_WIDTH
        gsquare = (st[half, 1, there, :] + st_in[half, 1, there, :]) / GROUP_WIDTH
        inv = lax.rsqrt(gsquare - gmean * gmean + 1e-05)
        for v in range(4):
            for part in range(2):
                col = pl.multiple_of((2 * v + c) * CW + part * 128, 128)
                lane = part * 128
                s = (cv[v, rows, lane : lane + 128] - gmean) * inv * conv_gain[:, pl.ds(col, 128)]
                act[rows, v * CW + lane : v * CW + lane + 128] = (s / (1.0 + jnp.exp(-s))).astype(BF)
        return carry

    def activate_half(half):
        lax.fori_loop(3 * half, 3 * half + 3, activate, 0)
        lax.fori_loop(3 * half + 6, 3 * half + 9, activate, 0)

    @step_named("c.a0")
    def _():
        cp.arrived(st.at[0], st_sem)
        activate_half(0)

    @step_named("c.a1")
    def _():
        cp.arrived(st.at[1], st_sem + 1)
        activate_half(1)

    mix_sem, mix_send = cp.take(2), cp.take_send(mix_out)

    def columns(buf, n):
        halves = []
        for half in range(2):
            two = buf[half, n // 2, pl.ds((n % 2) * 2, 2)]
            halves.append(jnp.concatenate([two[0], two[1]], axis=1))
        return jnp.concatenate(halves, axis=0)

    def half_rows(core, half):
        return pl.ds(pl.multiple_of(core * RB + half * 96, 32), 96)

    def point(half):
        def step(n, carry):
            rows = jnp.concatenate([act[half_rows(1 - c, half), :], act[half_rows(c, half), :]], axis=0)
            weight = jnp.concatenate([columns(pp, 2 * n), columns(pp, 2 * n + 1)], axis=1)
            both = dot(rows, weight)
            mix_out[half, n] = both[:96].astype(BF)
            cp.copy(mix_out.at[half, n], mix_in.at[half, n], to_pair, mix_sem + half, mix_send).start()
            mix[half * 96 : half * 96 + 96, pl.ds(pl.multiple_of(n * 512, 512), 512)] = both[96:]
            return carry

        for n in range(4):
            step(n, 0)

    def middle(half):
        def step(i, carry):
            here = pl.ds(pl.multiple_of(i * 16, 16), 16)
            rows = pl.ds(pl.multiple_of(half * 96 + i * 16, 16), 16)
            mixed = mix[rows, :] + jnp.concatenate([mix_in[half, n, here, :] for n in range(4)], axis=1).astype(F32)
            data = (resid[rows, :].astype(F32) + mixed).astype(BF)
            mid[rows, :] = data
            v = data.astype(F32)
            scale = lax.rsqrt(jnp.mean(v * v, axis=-1, keepdims=True) + 1e-06)
            at = pl.multiple_of(tp * RB + half * 96 + i * 16, 16)
            x2[pl.ds(at, 16), :] = (v * scale * gain2[...]).astype(BF)
            return carry

        cp.arrived(mix_in.at[half], mix_sem + half)
        lax.fori_loop(0, 6, step, 0)

    steps["c.p0"], steps["c.p1"] = (lambda: point(0)), (lambda: point(1))
    steps["c.m0"], steps["c.m1"] = (lambda: middle(0)), (lambda: middle(1))

    def up(v):
        up_rows(v * CB, CB)

    def up_rows(first, count):
        rows = pl.ds(pl.multiple_of(first, 64), count)

        def step(n, carry):
            weight = uu[n].reshape(D, 512)
            cols = pl.ds(pl.multiple_of(n * 512, 512), 512)
            upper = jnp.maximum(dot(x2[rows, :], weight) * up_scale[:, cols], 0.0)
            hid[rows, cols] = (upper * upper).astype(BF)
            return carry

        for n in range(2):
            step(n, 0)

    @step_named("c.ux")
    def _():
        ring2.own_wait()
        up(x)

    steps["c.up"] = lambda: up(xp)
    steps["c.um"] = lambda: up(xm)
    steps["c.u0"] = lambda: up_rows(xf * CB + c * RB, RB)
    steps["c.uf"] = lambda: up_rows(xf * CB + (1 - c) * RB, RB)

    pair_sem = {"f": cp.take(8), "pl": cp.take(8), "la": cp.take(4), "x": cp.take()}
    relay_sem, end_sem = cp.take(4), cp.take(4)
    pair_send, ring_send = cp.take_send(par_out), cp.take_send(par.at[0:3])

    def blocks(i):
        return [((z + dz) % 4, (y + dy) % 4) for dz, dy in CHUNKS[i]]

    def block_columns(owner):
        return pl.ds(pl.multiple_of((owner[0] * 4 + owner[1]) * 128, 128), 128)

    def down_columns(i):
        (za, ya), (zb, yb) = blocks(i)
        halves = [jnp.concatenate([dd[half, za, ya], dd[half, zb, yb]], axis=1) for half in range(2)]
        return jnp.concatenate(halves, axis=0)

    def down(*chunks):
        done = []
        for v, i, _ in chunks:
            pair_rows = pl.ds(pl.multiple_of(v * CB + (1 - c) * RB, RB), RB)
            own_rows = pl.ds(pl.multiple_of(v * CB + c * RB, RB), RB)
            rows = jnp.concatenate([hid[pair_rows, :], hid[own_rows, :]], axis=0)
            done.append(dot(rows, down_columns(i)))
        for (v, i, _), both in zip(chunks, done):
            par_out[v, i] = both[:RB].astype(BF)
            par[v, i] = both[RB:].astype(BF)
        for v, i, sem in chunks:
            cp.copy(par_out.at[v, i], par_in.at[v, i], to_pair, sem, pair_send).start()

    def pair_arrived(sem, count):
        cp.arrived(par_in.at[0, 0:count], sem)

    def add_pair(v, n):
        par[v, n] = (par[v, n].astype(F32) + par_in[v, n].astype(F32)).astype(BF)

    def relay(side, k):
        n = k + 4 * side
        cp.copy(par.at[xf, n], rel_in.at[side, k], to_xm if side else to_xp, relay_sem + k, ring_send).start()

    def plain(side, k):
        n = k + 4 * (1 - side)
        to, peer = (xm, to_xm) if side else (xp, to_xp)
        cp.copy(par.at[to, n], fin_in.at[side, n], peer, end_sem + k, ring_send).start()

    def last(side, k):
        n = k + 4 * side
        to, peer = (xm, to_xm) if side else (xp, to_xp)
        cp.copy(par.at[to, n], fin_in.at[side, n], peer, end_sem + k, ring_send).start()

    def each(count, body):
        for i in range(count):
            body(i)

    def relay_chunk(side, k):
        n = side * 4 + k
        pair_arrived(pair_sem["f"] + n, 1)
        add_pair(xf, n)
        relay(side, k)

    def plain_chunk(side, k):
        pair_arrived(pair_sem["pl"] + 4 * side + k, 1)
        add_pair(xm if side else xp, k if side else k + 4)
        plain(side, k)

    def far(i):
        return xf, i, pair_sem["f"] + i

    def near(side, k):
        return xm if side else xp, k if side else k + 4, pair_sem["pl"] + 4 * side + k

    for side in range(2):
        steps[f"d.e{side}"] = lambda side=side: down(near(side, 0), near(side, 1))

    @step_named("d.ef")
    def _():
        down(far(0), far(4))
        down(far(1), far(5))

    def send_plain(side):
        plain_chunk(side, 0)
        plain_chunk(side, 1)

    for side in range(2):
        steps[f"d.s{side}"] = lambda side=side: send_plain(side)

    @step_named("d.sf")
    def _():
        for k in range(2):
            for side in range(2):
                relay_chunk(side, k)

    @step_named("d.fa")
    def _():
        down(far(2), far(6))
        down(far(3), far(7))
        for k in range(2, 4):
            for side in range(2):
                relay_chunk(side, k)

    @step_named("d.pl")
    def _():
        down(near(0, 2), near(1, 2))
        down(near(0, 3), near(1, 3))
        for k in range(2, 4):
            for side in range(2):
                plain_chunk(side, k)

    @step_named("d.la")
    def _():
        each(4, lambda k: down((xp, k, pair_sem["la"] + k), (xm, k + 4, pair_sem["la"] + k)))

    @step_named("d.sl")
    def _():
        def send_last(k):
            pair_arrived(pair_sem["la"] + k, 2)
            cp.arrived(rel_in.at[0, 0:2], relay_sem + k)
            for side, v in ((0, xp), (1, xm)):
                n = k + 4 * side
                total = par[v, n].astype(F32) + par_in[v, n].astype(F32) + rel_in[side, k].astype(F32)
                par[v, n] = total.astype(BF)
                last(side, k)

        each(4, send_last)

    @step_named("d.xx")
    def _():
        each(4, lambda k: down((x, k, pair_sem["x"]), (x, k + 4, pair_sem["x"])))
        pair_arrived(pair_sem["x"], 8)

        def own_step(i):
            for part, owner in enumerate(blocks(i)):
                lane, cols = slice(part * 128, part * 128 + 128), block_columns(owner)
                own = par[x, i, :, lane].astype(F32) + par_in[x, i, :, lane].astype(F32)
                mix[:, cols] = mid[:, cols].astype(F32) + own

        each(8, own_step)

    def finish(k):
        cp.arrived(fin_in.at[0, 0:4], end_sem + k)
        for i in (k, k + 4):
            total = fin_in[0, i].astype(F32) + fin_in[1, i].astype(F32)
            for part, owner in enumerate(blocks(i)):
                lane, cols = slice(part * 128, part * 128 + 128), block_columns(owner)
                out_buf[i, part] = (mix[:, cols] + total[:, lane]).astype(BF)
                pltpu.make_async_copy(out_buf.at[i, part], out.at[:, cols], out_sem.at[0]).start()

    steps["d.fn"] = lambda: each(4, finish)
    pl.semaphore_wait(barrier, 7)
    for name in ORDER:
        with jax.named_scope(name):
            steps[name]()
    assert len(ORDER) == len(set(ORDER)) == len(steps)
    cp.finish()
    pltpu.make_async_copy(resid, out, out_sem.at[0]).wait()


SCRATCH = (
    ((SEQ, D), BF),
    ((SEQ, D), BF),
    ((2, 4, 4, 128, 256), BF),
    ((2, 4, 4, 512, 128), BF),
    ((2, 4, 4, 128, 512), BF),
    ((2, 4, 4, 512, 128), BF),
    ((SEQ + 2 * HALO, CW), BF),
    ((4, CB + 2 * HALO, CW), BF),
    ((4, CB, CW), F32),
    ((2, 2, RB, 128), F32),
    ((2, 2, RB, 128), F32),
    ((CB, 4 * CW), BF),
    ((2, 4, 96, 512), BF),
    ((2, 4, 96, 512), BF),
    ((RB, D), F32),
    ((RB, D), BF),
    ((SEQ, 1024), BF),
    ((4, 8, RB, 256), BF),
    ((4, 8, RB, 256), BF),
    ((4, 8, RB, 256), BF),
    ((2, 4, RB, 256), BF),
    ((2, 8, RB, 256), BF),
    ((2, FAR, CW), BF),
    ((8, 2, RB, 128), BF),
)


def shards(*arrays):
    flat = [a.reshape(1, -1) if a.ndim == 1 else a for a in arrays]
    return pl.pallas_call(
        kernel,
        out_shape=jax.ShapeDtypeStruct((RB, D), BF),
        in_specs=[pl.BlockSpec(memory_space=pltpu.HBM)] * len(flat),
        out_specs=pl.BlockSpec(memory_space=pl.ANY),
        scratch_shapes=[pltpu.VMEM(a.shape, a.dtype) for a in flat]
        + [pltpu.VMEM(shape, kind) for shape, kind in SCRATCH]
        + [pltpu.SemaphoreType.DMA((count,)) for count in (N_SEND, N_RECV, len(flat), 1)],
        compiler_params=pltpu.CompilerParams(
            collective_id=0, has_side_effects=True, vmem_limit_bytes=66 * 1000 * 1000
        ),
        name="layer",
    )(*flat)


def solution(mesh):
    in_specs = (
        P(("fs", "tp"), None),
        P(),
        P("fs", "tp"),
        P("fs", "tp"),
        P(),
        P(),
        P(),
        P(),
        P("tp", "fs"),
        P("fs"),
        P(),
        P("fs", "tp"),
        P("tp"),
        P("tp", "fs"),
        P("fs"),
    )
    out_specs = P(("fs", "tp"), None)
    return jax.shard_map(shards, mesh=mesh, in_specs=in_specs, out_specs=out_specs, check_vma=False)
```
